512 devices in a mesh: sp: 32 (over z, core), tp: 16 (over y, x).
Axes of the slice: x: 4, y: 4, z: 16, core: 2. Of those that a mesh axis runs over, the one named last changes fastest.
Arguments:
- resid: bfloat16 [8192, 2048], P('sp'), may hold values from -18 to 18
- narrow_head_input: bfloat16 [8192, 1024], P('sp', 'tp'), may hold values from -6 to 6
- wide_head_input: bfloat16 [8192, 2048], P('sp', 'tp'), may hold values from -6 to 6
- key_group_input: bfloat16 [8192, 512], P('sp'), may hold values from -6 to 6
- query_group_input: bfloat16 [8192, 512], P('sp'), may hold values from -6 to 6
- narrow_output_gate: bfloat16 [8192, 1024], P('sp', 'tp'), may hold values from -6 to 6
- wide_output_gate: bfloat16 [8192, 2048], P('sp', 'tp'), may hold values from -6 to 6
- step_input_rows: bfloat16 [8192, 2, 16], P('sp', None, 'tp'), may hold values from -4 to 4
- head_decay_logarithm: float32 [2, 16], P(None, 'tp'), may hold values from -14 to -2
- position_log_decay: float32 [8192, 2, 16], P('sp', None, 'tp'), may hold values from -1.4 to 0
- direct_input_weight: float32 [2, 16], P(None, 'tp'), may hold values from 0.5 to 2
- narrow_conv_taps: float32 [4, 1024], P(None, 'tp'), may hold values from -3 to 3
- wide_conv_taps: float32 [4, 2048], P(None, 'tp'), may hold values from -3 to 3
- key_conv_taps: float32 [4, 512], replicated, may hold values from -3 to 3
- query_conv_taps: float32 [4, 512], replicated, may hold values from -3 to 3
- narrow_norm_gain: float32 [1024], P('tp'), may hold values from 0.1 to 1.9
- wide_norm_gain: float32 [2048], P('tp'), may hold values from 0.1 to 1.9
- narrow_output_rows: bfloat16 [1024, 2048], P('tp'), may hold values from -0.109375 to 0.109375
- wide_output_rows: bfloat16 [2048, 2048], P('tp'), may hold values from -0.109375 to 0.109375
- feedforward_norm_gain: float32 [2048], replicated, may hold values from 0.1 to 1.9
- routes: int32 [8192, 3], P('sp'), may hold values from 0 to 31, all different within a row; in each aligned block of 256 rows (0 to 255, 256 to 511, ...) at most 32 rows name the same one
- routing_weight_values: float32 [8192, 3], P('sp'), may hold values from 0.1 to 1
- expert_gate_matrix: bfloat16 [32, 2048, 2048], P('sp', None, 'tp'), may hold values from -1 to 1
- expert_up_matrix: bfloat16 [32, 2048, 2048], P('sp', None, 'tp'), may hold values from -1 to 1
- expert_down_matrix: bfloat16 [32, 2048, 2048], P('sp', 'tp'), may hold values from -0.015625 to 0.015625
Outputs:
- layer_out: bfloat16 [8192, 2048], P('sp', 'tp')
The draws below stay inside these ranges and needn't reach their ends.
Inputs may be any that keep to these rules, and one draw needn't show every extreme that they name: `routes`: each token names 3 different experts. Among the tokens of one index of sp (aligned blocks of 256 rows) no expert is named by more than 32 of them, and in some blocks one is named by exactly 32.
All inputs are finite; a program needn't handle non-finite values.
Results may differ from the reference program's by a relative error of at most 0.015.
Values may be sent and summed in bfloat16 or wider, within the bound.
A program may use at most 64 MiB of HBM per device.

```python
import math
import jax
import jax.numpy as jnp
import numpy as np
from jax import lax

D = 2048
HEADS = 16
NARROW_HEAD_DIM = 64
WIDE_HEAD_DIM = 128
STATE = 128
GROUPS = 4
CONV_W = 4
BLOCK = 128
FF = 2048
TOPK = 3
TOK_SP = 256
TOKENS = 8192
EXPERTS = 32
CAP = 32
N_SP = 32
N_TP = 16


def draw_resid(key, part):
    key_base, key_rows = jax.random.split(jax.random.fold_in(key, 3), 2)
    row_scales = jnp.exp(jax.random.uniform(key_rows, (TOKENS, 1), jnp.float32, math.log(0.3), math.log(3.0)))
    base = jnp.clip(jax.random.normal(key_base, (TOKENS, D), jnp.float32), -6.0, 6.0)
    return jnp.clip(base * row_scales, -18.0, 18.0).astype(jnp.bfloat16)


def draw_step_input_rows(key, part):
    key_base, key_shift = jax.random.split(jax.random.fold_in(key, 5))
    block_total = TOKENS // TOK_SP
    shifts = jax.random.uniform(key_shift, (block_total, 1, 1, 1), jnp.float32, -1.0, 1.0)
    base = jax.random.normal(key_base, (block_total, TOK_SP, 2, HEADS), jnp.float32)
    return jnp.clip(base + shifts, -4.0, 4.0).reshape(TOKENS, 2, HEADS).astype(jnp.bfloat16)


def draw_head_decay_logarithm(key, part):
    key_kind, key_slow, key_fast = jax.random.split(jax.random.fold_in(key, 7), 3)
    slow_share = 0.5
    slow_heads = jax.random.uniform(key_kind, (2, HEADS), jnp.float32) < slow_share
    slow_rate = jnp.exp(jax.random.uniform(key_slow, (2, HEADS), jnp.float32, math.log(0.1), math.log(0.6))) / TOKENS
    fast_rate = jnp.exp(jax.random.uniform(key_fast, (2, HEADS), jnp.float32, math.log(1.0 / 60.0), math.log(1.0 / 20.0)))
    return jnp.clip(jnp.log(jnp.where(slow_heads, slow_rate, fast_rate)), -14.0, -2.0).astype(jnp.float32)


def draw_position_log_decay(key, part):
    key_spots, key_depth = jax.random.split(jax.random.fold_in(key, 9))
    spots = jax.random.randint(key_spots, (3,), 0, TOKENS)
    depth = jax.random.uniform(key_depth, (3, 2, HEADS), jnp.float32, math.log(0.5), math.log(0.8))
    hits = (jnp.arange(TOKENS)[:, None] == spots[None, :]).astype(jnp.float32)
    return jnp.clip(jnp.einsum('tk,khd->thd', hits, depth), -1.4, 0.0).astype(jnp.float32)


def draw_expert_gate_matrix(key, part):
    key_base, key_cols = jax.random.split(jax.random.fold_in(key, 11))
    column_scales = jnp.exp(jax.random.uniform(key_cols, (EXPERTS, 1, FF), jnp.float32, math.log(0.5), math.log(8.0)))
    base = jax.random.normal(key_base, (EXPERTS, D, FF), jnp.float32)
    return jnp.clip(base * column_scales / math.sqrt(D), -1.0, 1.0).astype(jnp.bfloat16)


def draw_expert_up_matrix(key, part):
    key_base, key_cols = jax.random.split(jax.random.fold_in(key, 13))
    column_scales = jnp.exp(jax.random.uniform(key_cols, (EXPERTS, 1, FF), jnp.float32, math.log(0.5), math.log(8.0)))
    base = jax.random.normal(key_base, (EXPERTS, D, FF), jnp.float32)
    return jnp.clip(base * column_scales / math.sqrt(D), -1.0, 1.0).astype(jnp.bfloat16)


def level_of(own_key, dims, shards, least, high):
    def one(dim, blocks):
        draws = jax.random.uniform(jax.random.fold_in(jax.random.fold_in(own_key, 6), dim), (blocks,), jnp.float32, least / len(shards), high / len(shards))
        return jnp.repeat(jnp.exp(draws), dims[dim] // blocks).reshape((-1,) + (1,) * (len(dims) - dim - 1))

    gain = one(*shards[0])
    for cut in shards[1:]:
        gain = gain * one(*cut)
    return gain


def shared_out(rng, own, number, rows, amount, top, limit, lean):
    sequence = jax.random.permutation(rng, amount)
    crowded, common = portions_of(amount, rows * top, limit, lean, True), portions_of(amount, rows * top, limit, lean, False)
    places = jnp.arange(amount)

    def named(tallies, offset_by):
        used = int((tallies > 0).sum())
        fixed = max(1, used // 4)
        moved = fixed + (places - fixed + offset_by * (used - fixed)) % max(1, amount - fixed)
        return jnp.zeros((amount,), jnp.int32).at[sequence[jnp.where(places < fixed, places, moved)]].set(jnp.asarray(tallies, jnp.int32))

    tallies = jnp.where(number % 4 == 0, named(crowded, number // 4), named(common, number - number // 4 - 1))
    mixed = jax.random.permutation(jax.random.fold_in(own, 3), amount)
    giver, sink = mixed[0:amount // 2 * 2:2], mixed[1:amount // 2 * 2:2]
    margin = jnp.minimum(tallies[giver] - 1, limit - tallies[sink]) // 2
    margin = jnp.where((giver == sequence[0]) | (sink == sequence[0]) | (tallies[sink] == 0), 0, jnp.maximum(margin, 0))
    moved = jax.random.randint(jax.random.fold_in(own, 4), (amount // 2,), 0, 1 << 20) % (margin + 1)
    tallies = tallies.at[giver].add(-moved).at[sink].add(moved)
    members = jnp.searchsorted(jnp.cumsum(tallies), jnp.arange(rows * top), side="right").astype(jnp.int32)
    listing = members.reshape(top, rows).T
    listing = listing[jax.random.permutation(jax.random.fold_in(own, 1), rows)]
    offset_by = jax.random.randint(jax.random.fold_in(own, 2), (rows, 1), 0, top)
    return jnp.take_along_axis(listing, (jnp.arange(top)[None, :] + offset_by) % top, axis=1)


def portions_of(number_of, total, bound, lean, full):
    portions = [(1 << 20) // math.isqrt(standing ** lean) + 1 for standing in range(1, number_of + 1)]
    largest = bound if full else min(bound, max(-(-total // number_of), total * portions[0] // sum(portions)))
    least = 1 if total - largest >= number_of - 1 else 0
    holding, surplus = [largest] + [least] * (number_of - 1), total - largest - least * (number_of - 1)
    while surplus > 0:
        movable = [i for i in range(1, number_of) if holding[i] < largest] or [i for i in range(1, number_of) if holding[i] < bound]
        pool, left = sum([portions[i] for i in movable]), surplus
        for i in movable:
            extra = min(bound - holding[i], max(1, left * portions[i] // pool), surplus)
            holding[i] = holding[i] + extra
            surplus = surplus - extra
    return np.array(holding)


def normal_values(rng, shape, deviation, limit, cuts=(), kind=jnp.bfloat16):
    drawn = deviation * jax.random.normal(rng, shape, jnp.float32)
    if cuts:
        drawn = drawn * level_of(rng, shape, cuts, -0.22, 0.18)
    return jnp.clip(drawn, -limit, limit).astype(kind)


def setup_inputs(seed: int = 0) -> dict:
    splits = jax.random.split(jax.random.key(seed), 26)
    resid = draw_resid(jax.random.fold_in(splits[25], 71), 0)
    narrow_head_input = normal_values(splits[1], (TOKENS, HEADS * NARROW_HEAD_DIM), 1.0, 6.0, ((0, 32), (1, 16)))
    wide_head_input = normal_values(splits[2], (TOKENS, HEADS * WIDE_HEAD_DIM), 1.0, 6.0, ((0, 32), (1, 16)))
    key_group_input = normal_values(splits[3], (TOKENS, GROUPS * STATE), 1.0, 6.0, ((0, 32),))
    query_group_input = normal_values(splits[4], (TOKENS, GROUPS * STATE), 1.0, 6.0, ((0, 32),))
    narrow_output_gate = normal_values(splits[5], (TOKENS, HEADS * NARROW_HEAD_DIM), 1.0, 6.0, ((0, 32), (1, 16)))
    wide_output_gate = normal_values(splits[6], (TOKENS, HEADS * WIDE_HEAD_DIM), 1.0, 6.0, ((0, 32), (1, 16)))
    step_input_rows = draw_step_input_rows(jax.random.fold_in(splits[25], 71), 0)
    head_decay_logarithm = draw_head_decay_logarithm(jax.random.fold_in(splits[25], 71), 0)
    position_log_decay = draw_position_log_decay(jax.random.fold_in(splits[25], 71), 0)
    direct_input_weight = jnp.clip(0.5 + 1.5 * jax.random.uniform(splits[10], (2, HEADS), jnp.float32) ** level_of(splits[10], (2, HEADS), ((1, 16),), -0.2, 0.2), 0.5, 2.0)
    narrow_conv_taps = normal_values(splits[11], (CONV_W, HEADS * NARROW_HEAD_DIM), CONV_W ** -0.5, 3.0, ((1, 16),), jnp.float32)
    wide_conv_taps = normal_values(splits[12], (CONV_W, HEADS * WIDE_HEAD_DIM), CONV_W ** -0.5, 3.0, ((1, 16),), jnp.float32)
    key_conv_taps = normal_values(splits[13], (CONV_W, GROUPS * STATE), CONV_W ** -0.5, 3.0, (), jnp.float32)
    query_conv_taps = normal_values(splits[14], (CONV_W, GROUPS * STATE), CONV_W ** -0.5, 3.0, (), jnp.float32)
    narrow_norm_gain = jnp.clip(1.0 + 0.18 * jax.random.normal(splits[15], (HEADS * NARROW_HEAD_DIM,), jnp.float32), 0.1, 1.9)
    wide_norm_gain = jnp.clip(1.0 + 0.18 * jax.random.normal(splits[16], (HEADS * WIDE_HEAD_DIM,), jnp.float32), 0.1, 1.9)
    narrow_output_rows = normal_values(splits[17], (HEADS * NARROW_HEAD_DIM, D), (HEADS * (NARROW_HEAD_DIM + WIDE_HEAD_DIM)) ** -0.5, 0.109375, ((0, 16),))
    wide_output_rows = normal_values(splits[18], (HEADS * WIDE_HEAD_DIM, D), (HEADS * (NARROW_HEAD_DIM + WIDE_HEAD_DIM)) ** -0.5, 0.109375, ((0, 16),))
    feedforward_norm_gain = jnp.clip(1.0 + 0.18 * jax.random.normal(splits[19], (D,), jnp.float32), 0.1, 1.9)
    routes_keys = jax.random.split(jax.random.fold_in(splits[20], 1), TOKENS // TOK_SP)
    routes_turns = jax.random.permutation(jax.random.fold_in(splits[20], 3), TOKENS // TOK_SP)
    routes = jax.vmap(lambda own, number: shared_out(jax.random.fold_in(splits[20], 2), own, number, TOK_SP, EXPERTS, TOPK, CAP, 1))(routes_keys, routes_turns).reshape((TOKENS, TOPK))
    routing_weight_values = jnp.clip(0.1 + 0.9 * jax.random.uniform(splits[21], (TOKENS, TOPK), jnp.float32) ** level_of(splits[21], (TOKENS, TOPK), ((0, 32),), -0.2, 0.2), 0.1, 1.0)
    expert_gate_matrix = draw_expert_gate_matrix(jax.random.fold_in(splits[25], 71), 0)
    expert_up_matrix = draw_expert_up_matrix(jax.random.fold_in(splits[25], 71), 0)
    expert_down_matrix = normal_values(splits[24], (EXPERTS, FF, D), (64 * FF) ** -0.5, 0.015625, ((0, 32), (1, 16)))
    return {"resid": resid, "narrow_head_input": narrow_head_input, "wide_head_input": wide_head_input, "key_group_input": key_group_input, "query_group_input": query_group_input, "narrow_output_gate": narrow_output_gate, "wide_output_gate": wide_output_gate, "step_input_rows": step_input_rows, "head_decay_logarithm": head_decay_logarithm, "position_log_decay": position_log_decay, "direct_input_weight": direct_input_weight, "narrow_conv_taps": narrow_conv_taps, "wide_conv_taps": wide_conv_taps, "key_conv_taps": key_conv_taps, "query_conv_taps": query_conv_taps, "narrow_norm_gain": narrow_norm_gain, "wide_norm_gain": wide_norm_gain, "narrow_output_rows": narrow_output_rows, "wide_output_rows": wide_output_rows, "feedforward_norm_gain": feedforward_norm_gain, "routes": routes, "routing_weight_values": routing_weight_values, "expert_gate_matrix": expert_gate_matrix, "expert_up_matrix": expert_up_matrix, "expert_down_matrix": expert_down_matrix}


NORM_EPS = 1e-06
CLAMP_LIMIT = 7.0
SIGMOID_SCALE = 1.702
FULL_PRECISION = lax.Precision.HIGHEST

def conv_with_rim(values, rim_rows, weight):
    length = values.shape[0]
    padded = jnp.concatenate([rim_rows, values], axis=0).astype(jnp.float32)
    accumulated = jnp.zeros((length, values.shape[1]), jnp.float32)
    for tap_index in range(weight.shape[0]):
        accumulated = accumulated + weight[tap_index] * padded[tap_index:tap_index + length]
    return jax.nn.silu(accumulated)

def pick_groups(channel_table, first_head, head_count):
    length = channel_table.shape[0]
    grouped = channel_table.reshape(length, GROUPS, -1)
    owners = (first_head + jnp.arange(head_count, dtype=jnp.int32)) // (HEADS // GROUPS)
    chooser = (owners[:, None] == jnp.arange(GROUPS, dtype=jnp.int32)[None, :]).astype(jnp.float32)
    return jnp.einsum('sgn,hg->shn', grouped, chooser, precision=FULL_PRECISION)

def local_head(values, step_logarithm, key_head_rows, query_head_rows, block_len):
    block_count = values.shape[0] // block_len
    values = values.reshape(block_count, block_len, -1)
    step_logarithm = step_logarithm.reshape(block_count, block_len)
    key_head_rows = key_head_rows.reshape(block_count, block_len, -1)
    query_head_rows = query_head_rows.reshape(block_count, block_len, -1)
    cum_decay = jnp.cumsum(step_logarithm, axis=1)
    causal_mask = jnp.arange(block_len)[:, None] >= jnp.arange(block_len)[None, :]
    decay_gaps = jnp.where(causal_mask[None], cum_decay[:, :, None] - cum_decay[:, None, :], -1e+30)
    scores = jnp.einsum('bln,bsn->bls', query_head_rows, key_head_rows, precision=FULL_PRECISION) * jnp.exp(decay_gaps)
    inside = jnp.einsum('bls,bsp->blp', scores, values, precision=FULL_PRECISION)
    tail_decay = jnp.exp(cum_decay[:, -1:] - cum_decay)
    states = jnp.einsum('bln,blp->bnp', key_head_rows * tail_decay[..., None], values, precision=FULL_PRECISION)
    totals = cum_decay[:, -1]

    def walk(running, member):
        return (jnp.exp(member[1]) * running + member[0], running)
    closing, entering = lax.scan(walk, jnp.zeros(states.shape[1:], jnp.float32), (states, totals))
    before = jnp.cumsum(totals) - totals
    return (inside, entering, closing, jnp.sum(totals), before, cum_decay, query_head_rows)

def finish_head(inside, entering, before, cum_decay, query_blocks, carried):
    starting = entering + jnp.exp(before)[:, None, None] * carried[None]
    readout = jnp.einsum('bln,bnp->blp', query_blocks * jnp.exp(cum_decay)[..., None], starting, precision=FULL_PRECISION)
    return (inside + readout).reshape(-1, inside.shape[-1])

def group_out(scanned, mixed_input_rows, direct_input_term, gate_input_rows, norm_gain_vector):
    length, head_count, head_dimension = mixed_input_rows.shape
    gated = jax.nn.silu(gate_input_rows.astype(jnp.float32)).reshape(length, head_count, head_dimension)
    result = (scanned + direct_input_term[None, :, None] * mixed_input_rows) * gated
    result = result * lax.rsqrt(lax.optimization_barrier(jnp.mean(result * result, axis=-1, keepdims=True)) + NORM_EPS)
    return (result.reshape(length, head_count * head_dimension) * norm_gain_vector).astype(jnp.bfloat16)

def mixer_head_group(unprojected_input, gate_input_rows, convolution_weight, key_head_table, query_head_table, unsoftened_step, decay_vector, position_decay_rows, direct_input_term, norm_gain_vector, head_dimension):
    length = unprojected_input.shape[0]
    zero_rim = jnp.zeros((convolution_weight.shape[0] - 1, unprojected_input.shape[1]), unprojected_input.dtype)
    mixed_input_rows = conv_with_rim(unprojected_input, zero_rim, convolution_weight).reshape(length, -1, head_dimension)
    head_count = mixed_input_rows.shape[1]
    key_head_rows = pick_groups(key_head_table, 0, head_count)
    query_head_rows = pick_groups(query_head_table, 0, head_count)
    step_length_values = jax.nn.softplus(unsoftened_step.astype(jnp.float32))
    step_logarithm = -jnp.exp(decay_vector)[None, :] * step_length_values + position_decay_rows
    values = mixed_input_rows * step_length_values[..., None]

    def one_head(head_values, head_log, head_keys, head_queries):
        parts = local_head(head_values, head_log, head_keys, head_queries, BLOCK)
        return finish_head(parts[0], parts[1], parts[4], parts[5], parts[6], jnp.zeros_like(parts[2]))
    scanned = jax.vmap(one_head, in_axes=(1, 1, 1, 1), out_axes=1)(values, step_logarithm, key_head_rows, query_head_rows)
    return group_out(scanned, mixed_input_rows, direct_input_term, gate_input_rows, norm_gain_vector)

def expert_layer(normed, routes, expert_gate_matrix, expert_up_matrix, expert_down_matrix):
    tokens = normed.shape[0]
    flat_routes = routes.reshape(-1).astype(jnp.int32)
    order_ids = jnp.argsort(flat_routes, stable=True).astype(jnp.int32)
    sorted_routes = flat_routes[order_ids]
    counts = lax.optimization_barrier(jnp.sum((flat_routes[:, None] == jnp.arange(EXPERTS, dtype=jnp.int32)[None, :]).astype(jnp.int32), axis=0))
    starts = (jnp.cumsum(counts) - counts).astype(jnp.int32)
    room = CAP * N_SP
    padded_ids = jnp.concatenate([order_ids, jnp.zeros((room,), jnp.int32)])

    def one_expert(member):
        start, gate_weight, up_weight, down_weight = member
        picked = lax.dynamic_slice_in_dim(padded_ids, start, room)
        rows = normed[picked // TOPK]
        gate_pre = jnp.dot(rows, gate_weight, preferred_element_type=jnp.float32)
        up_pre = jnp.dot(rows, up_weight, preferred_element_type=jnp.float32)
        clamped = jnp.minimum(gate_pre, CLAMP_LIMIT)
        act = ((jnp.clip(up_pre, -CLAMP_LIMIT, CLAMP_LIMIT) + 1.0) * clamped * jax.nn.sigmoid(SIGMOID_SCALE * clamped)).astype(jnp.bfloat16)
        pieces = act.reshape(room, N_TP, -1).astype(jnp.float32)
        blocks = down_weight.reshape(N_TP, -1, down_weight.shape[1]).astype(jnp.float32)
        partials = jnp.einsum('rtf,tfd->rtd', pieces, blocks)
        rounded = lax.optimization_barrier(partials.astype(jnp.bfloat16)).astype(jnp.float32)
        return lax.optimization_barrier(jnp.sum(rounded, axis=1)).astype(jnp.bfloat16)
    outputs = lax.map(one_expert, (starts, expert_gate_matrix, expert_up_matrix, expert_down_matrix))
    within = jnp.arange(tokens * TOPK, dtype=jnp.int32) - starts[sorted_routes]
    per_sorted = outputs.reshape(EXPERTS * room, -1)[sorted_routes * room + within]
    per_entry = jnp.zeros((tokens * TOPK, per_sorted.shape[1]), jnp.bfloat16).at[order_ids].set(per_sorted)
    return per_entry.reshape(tokens, TOPK, -1)

def reference(resid, narrow_head_input, wide_head_input, key_group_input, query_group_input, narrow_output_gate, wide_output_gate, step_input_rows, head_decay_logarithm, position_log_decay, direct_input_weight, narrow_conv_taps, wide_conv_taps, key_conv_taps, query_conv_taps, narrow_norm_gain, wide_norm_gain, narrow_output_rows, wide_output_rows, feedforward_norm_gain, routes, routing_weight_values, expert_gate_matrix, expert_up_matrix, expert_down_matrix):
    length = resid.shape[0]
    zero_rim = jnp.zeros((CONV_W - 1, key_group_input.shape[1]), key_group_input.dtype)
    key_head_table = conv_with_rim(key_group_input, zero_rim, key_conv_taps)
    query_head_table = conv_with_rim(query_group_input, zero_rim, query_conv_taps)
    narrow_head_output = mixer_head_group(narrow_head_input, narrow_output_gate, narrow_conv_taps, key_head_table, query_head_table, step_input_rows[:, 0], head_decay_logarithm[0], position_log_decay[:, 0], direct_input_weight[0], narrow_norm_gain, NARROW_HEAD_DIM)
    wide_head_output = mixer_head_group(wide_head_input, wide_output_gate, wide_conv_taps, key_head_table, query_head_table, step_input_rows[:, 1], head_decay_logarithm[1], position_log_decay[:, 1], direct_input_weight[1], wide_norm_gain, WIDE_HEAD_DIM)
    narrow_blocks = narrow_head_output.reshape(length, N_TP, -1).transpose(1, 0, 2)
    wide_blocks = wide_head_output.reshape(length, N_TP, -1).transpose(1, 0, 2)
    narrow_weights = narrow_output_rows.reshape(N_TP, -1, narrow_output_rows.shape[1])
    wide_weights = wide_output_rows.reshape(N_TP, -1, wide_output_rows.shape[1])

    def project(running, member):
        part_narrow, part_wide, weight_narrow, weight_wide = member
        term = jnp.dot(part_narrow, weight_narrow, preferred_element_type=jnp.float32)
        term = term + jnp.dot(part_wide, weight_wide, preferred_element_type=jnp.float32)
        return (running + lax.optimization_barrier(term.astype(jnp.bfloat16)).astype(jnp.float32), None)
    mixed, _ = lax.scan(project, jnp.zeros((length, narrow_output_rows.shape[1]), jnp.float32), (narrow_blocks, wide_blocks, narrow_weights, wide_weights))
    hidden_state = resid.astype(jnp.float32) + mixed
    normed = (hidden_state * lax.rsqrt(lax.optimization_barrier(jnp.mean(hidden_state * hidden_state, axis=-1, keepdims=True)) + NORM_EPS) * feedforward_norm_gain).astype(jnp.bfloat16)
    expert_rows = expert_layer(normed, routes, expert_gate_matrix, expert_up_matrix, expert_down_matrix)
    combined = lax.optimization_barrier(jnp.sum(expert_rows.astype(jnp.float32) * routing_weight_values[..., None], axis=1))
    return (hidden_state + combined).astype(jnp.bfloat16)
```

```python
import functools

import jax
import jax.numpy as jnp
from jax import lax
from jax.experimental import pallas as pl
from jax.experimental.pallas import tpu as pltpu
from jax.sharding import PartitionSpec as P

HEADS = 16
NARROW_HEAD_DIM = 64
WIDE_HEAD_DIM = 128
GROUPS = 4
BLOCK = 128
SP = "sp"


NORM_EPS = 1e-06
CLAMP_LIMIT = 7.0
SIGMOID_SCALE = 1.702
FULL_PRECISION = lax.Precision.HIGHEST


def passed_along(block, axis, distance):
    devices = range(lax.axis_size(axis))
    route = [(i - distance, i) for i in devices if i - distance in devices]
    return lax.ppermute(block, axis, route)


def filled_with(x, identity):
    return jax.tree.map(
        lambda part, zero: jnp.zeros_like(part) + jnp.asarray(zero, part.dtype), x, identity
    )


def all_in_one(x, axis):
    leaves = jax.tree.leaves(x)
    turns = sorted(range(len(leaves)), key=lambda k: -leaves[k].size)
    width = (1, *leaves[turns[0]].shape)[-1]
    lines = [
        jnp.pad(leaves[k].reshape(-1), (0, -leaves[k].size % width)).reshape(-1, width)
        for k in turns
    ]
    both, at, found = (lax.all_gather(jnp.concatenate(lines), axis), 0, {})
    for k, line in zip(turns, lines):
        piece = both[:, at : at + len(line)].reshape(len(both), -1)
        found[k] = piece[:, : leaves[k].size].reshape(-1, *leaves[k].shape)
        at += len(line)
    numbers = iter(range(len(leaves)))
    return jax.tree.map(lambda _: found[next(numbers)], x)


def entering_2(x, axes, combine, identity):
    before = start = filled_with(x, identity)
    running = x
    for axis in (axes,):
        length, mine = (lax.axis_size(axis), lax.axis_index(axis))
        pieces = all_in_one(
            jax.tree.map(
                lambda part, kind: part.astype(kind),
                running,
                jax.tree.map(lambda a: jnp.bfloat16 if a.dtype == jnp.float32 else a.dtype, x),
            ),
            axis,
        )
        inside, running = (start, start)
        for k in range(length):
            passed = k < mine
            running = combine(
                running, jax.tree.map(lambda part, own: part[k].astype(own.dtype), pieces, x)
            )
            inside = jax.tree.map(lambda new, old: jnp.where(passed, new, old), running, inside)
        before = combine(inside, before)
    return before


def split_up(x, dim, length):
    lengths = x.shape
    parts = x.reshape(*lengths[:dim], length, lengths[dim] // length, *lengths[dim + 1 :])
    return jnp.moveaxis(parts, dim, 0)


def sent_and_summed(x, axis, dim):
    length = lax.axis_size(axis)
    parts = lax.all_to_all(split_up(x, dim, length), axis, 0, 0, tiled=True)
    return jnp.sum(parts.astype(jnp.float32), axis=0)


def padded_to(lines, length):
    spare = -len(lines) % length
    return jnp.pad(lines, [(0, spare)] + [(0, 0)] * (lines.ndim - 1))


def in_order(parts, dim):
    parts = jnp.moveaxis(parts, 0, dim)
    lengths = parts.shape
    return parts.reshape(*lengths[:dim], lengths[dim] * lengths[dim + 1], *lengths[dim + 2 :])


def from_everyone(x, axis):
    copies = jnp.broadcast_to(x, (lax.axis_size(axis), *x.shape))
    return lax.all_to_all(copies, axis, split_axis=0, concat_axis=0, tiled=True)


def collect(x, axis, dim):
    return in_order(from_everyone(x, axis), dim)


def total_of(x, axes):
    lines = x.reshape(-1, x.shape[-1])
    own = sent_and_summed(padded_to(lines, lax.axis_size(axes)), axes, 0)
    whole = collect(own.astype(jnp.bfloat16), axes, 0)
    return whole[: len(lines)].reshape(x.shape).astype(jnp.float32)


def conv_with_rim(values, rim_rows, weight):
    length = values.shape[0]
    padded = jnp.concatenate([rim_rows, values], axis=0).astype(jnp.float32)
    accumulated = jnp.zeros((length, values.shape[1]), jnp.float32)
    for tap_index in range(weight.shape[0]):
        accumulated = accumulated + weight[tap_index] * padded[tap_index : tap_index + length]
    return jax.nn.silu(accumulated)


def pick_groups(channel_table, first_head, head_count):
    length = channel_table.shape[0]
    grouped = channel_table.reshape(length, GROUPS, -1)
    owners = (first_head + jnp.arange(head_count, dtype=jnp.int32)) // (HEADS // GROUPS)
    chooser = (owners[:, None] == jnp.arange(GROUPS, dtype=jnp.int32)[None, :]).astype(jnp.float32)
    return jnp.einsum("sgn,hg->shn", grouped, chooser, precision=FULL_PRECISION)


def local_head(values, step_logarithm, key_head_rows, query_head_rows, block_len):
    block_count = values.shape[0] // block_len
    values = values.reshape(block_count, block_len, -1)
    step_logarithm = step_logarithm.reshape(block_count, block_len)
    key_head_rows = key_head_rows.reshape(block_count, block_len, -1)
    query_head_rows = query_head_rows.reshape(block_count, block_len, -1)
    cum_decay = jnp.cumsum(step_logarithm, axis=1)
    causal_mask = jnp.arange(block_len)[:, None] >= jnp.arange(block_len)[None, :]
    decay_gaps = jnp.where(causal_mask[None], cum_decay[:, :, None] - cum_decay[:, None, :], -1e30)
    scores = jnp.einsum(
        "bln,bsn->bls", query_head_rows, key_head_rows, precision=FULL_PRECISION
    ) * jnp.exp(decay_gaps)
    inside = jnp.einsum("bls,bsp->blp", scores, values, precision=FULL_PRECISION)
    tail_decay = jnp.exp(cum_decay[:, -1:] - cum_decay)
    states = jnp.einsum(
        "bln,blp->bnp", key_head_rows * tail_decay[..., None], values, precision=FULL_PRECISION
    )
    totals = cum_decay[:, -1]

    def walk(running, member):
        return (jnp.exp(member[1]) * running + member[0], running)

    closing, entering = lax.scan(walk, jnp.zeros(states.shape[1:], jnp.float32), (states, totals))
    before = jnp.cumsum(totals) - totals
    return (inside, entering, closing, jnp.sum(totals), before, cum_decay, query_head_rows)


def finish_head(inside, entering, before, cum_decay, query_blocks, carried):
    starting = entering + jnp.exp(before)[:, None, None] * carried[None]
    readout = jnp.einsum(
        "bln,bnp->blp",
        query_blocks * jnp.exp(cum_decay)[..., None],
        starting,
        precision=FULL_PRECISION,
    )
    return (inside + readout).reshape(-1, inside.shape[-1])


def group_out(scanned, mixed_input_rows, direct_input_term, gate_input_rows, norm_gain_vector):
    length, head_count, head_dimension = mixed_input_rows.shape
    gated = jax.nn.silu(gate_input_rows.astype(jnp.float32)).reshape(
        length, head_count, head_dimension
    )
    result = (scanned + direct_input_term[None, :, None] * mixed_input_rows) * gated
    result = result * lax.rsqrt(jnp.mean(result * result, axis=-1, keepdims=True) + NORM_EPS)
    return (result.reshape(length, head_count * head_dimension) * norm_gain_vector).astype(
        jnp.bfloat16
    )


def head_pieces_list(
    mixed_input_rows,
    step_length_values,
    decay_vector,
    position_decay_rows,
    key_head_rows,
    query_head_rows,
):
    step_logarithm = -jnp.exp(decay_vector)[None, :] * step_length_values + position_decay_rows
    values = mixed_input_rows * step_length_values[..., None]
    walker = functools.partial(local_head, block_len=BLOCK)
    return jax.vmap(walker, in_axes=(1, 1, 1, 1))(
        values, step_logarithm, key_head_rows, query_head_rows
    )


def finish_group(parts, carried_states):
    return jax.vmap(finish_head, in_axes=(0, 0, 0, 0, 0, 0), out_axes=1)(
        parts[0], parts[1], parts[4], parts[5], parts[6], carried_states
    )


def chain_combine(earlier, later):
    return (
        earlier[0] + later[0],
        earlier[1] + later[1],
        jnp.exp(later[0])[:, None, None] * earlier[2] + later[2],
        jnp.exp(later[1])[:, None, None] * earlier[3] + later[3],
    )


MESH = pl.DeviceIdType.MESH
CORES = 2
SIDE = 4


def remote(src, dst, send_sem, recv_sem, device):
    return pltpu.make_async_remote_copy(
        src_ref=src,
        dst_ref=dst,
        send_sem=send_sem,
        recv_sem=recv_sem,
        device_id=device,
        device_id_type=MESH,
    )


class Place:
    def __init__(self, chips):
        self.chips = chips
        self.sp = lax.axis_index("sp")
        self.tp = lax.axis_index("tp")
        self.z, self.core = self.sp // CORES, self.sp % CORES
        self.at = {"y": self.tp // SIDE, "x": self.tp % SIDE}

    def plane(self, axis, step):
        moved = (self.at[axis] + step + SIDE) % SIDE
        if axis == "x":
            return (self.sp, self.at["y"] * SIDE + moved)
        return (self.sp, moved * SIDE + self.at["x"])

    def index(self, axis, step):
        return (self.at[axis] + step + SIDE) % SIDE

    def along(self, step, core):
        return (((self.z + step + self.chips) % self.chips) * CORES + core, self.tp)


def chip_order(chips):
    if chips == 16:
        return [1, 15, 3, 13, 5, 11, 7, 9, 8, 6, 10, 4, 12, 2, 14, 0]
    return [d % chips for d in range(1, chips + 1)]


def greet(place):
    barrier = pltpu.get_barrier_semaphore()
    count = 0
    for axis in ("x", "y"):
        for step in (1, SIDE - 1):
            pl.semaphore_signal(barrier, inc=1, device_id=place.plane(axis, step), device_id_type=MESH)
            count += 1
    for step in range(place.chips):
        if step:
            pl.semaphore_signal(
                barrier, inc=1, device_id=place.along(step, place.core), device_id_type=MESH
            )
            count += 1
        pl.semaphore_signal(
            barrier, inc=1, device_id=place.along(step, 1 - place.core), device_id_type=MESH
        )
        count += 1
    return barrier, count


def chunk_of(ref, axis, index):
    return ref.at[index] if axis == "y" else ref.at[:, index]


class Summer:
    def __init__(self, place, first, blocks, relay, sums, half, last, sent, got):
        self.place, self.first, self.second = place, first, "y" if first == "x" else "x"
        self.blocks, self.relay, self.sums = blocks, relay, sums
        self.half, self.last, self.sent, self.got = half, last, sent, got
        self.started = []
        rows = blocks.shape[2]
        self.low, self.high = pl.ds(0, rows // 2), pl.ds(rows // 2, rows // 2)

    def send(self, src, dst, axis, step, number):
        copy = remote(
            src, dst, self.sent.at[number], self.got.at[number], self.place.plane(axis, step)
        )
        copy.start()
        self.started.append(copy)

    def open(self):
        far = chunk_of(self.blocks, self.first, self.place.index(self.first, 2))
        self.send(far.at[:, self.low], self.relay.at[0], self.first, 1, 0)
        self.send(far.at[:, self.high], self.relay.at[1], self.first, SIDE - 1, 1)

    def pass_on(self):
        for side, step in ((0, 1), (1, SIDE - 1)):
            part = self.low if side == 0 else self.high
            self.started[side].wait_recv()
            near = chunk_of(self.blocks, self.first, self.place.index(self.first, step))
            piece = near.at[:, part]
            piece[...] = (
                piece[...].astype(jnp.float32) + self.relay[side].astype(jnp.float32)
            ).astype(jnp.bfloat16)
            self.send(near, self.sums.at[side], self.first, step, 2 + side)

    def turn(self):
        self.started[2].wait_recv()
        self.started[3].wait_recv()
        own = chunk_of(self.blocks, self.first, self.place.at[self.first])
        own[...] = (
            own[...].astype(jnp.float32)
            + self.sums[0].astype(jnp.float32)
            + self.sums[1].astype(jnp.float32)
        ).astype(jnp.bfloat16)
        far = own.at[self.place.index(self.second, 2)]
        self.send(far.at[self.low], self.half.at[0], self.second, 1, 4)
        self.send(far.at[self.high], self.half.at[1], self.second, SIDE - 1, 5)

    def pass_again(self):
        own = chunk_of(self.blocks, self.first, self.place.at[self.first])
        for side, step in ((0, 1), (1, SIDE - 1)):
            part = self.low if side == 0 else self.high
            self.started[4 + side].wait_recv()
            near = own.at[self.place.index(self.second, step)]
            piece = near.at[part]
            piece[...] = (
                piece[...].astype(jnp.float32) + self.half[side].astype(jnp.float32)
            ).astype(jnp.bfloat16)
            self.send(near, self.last.at[side], self.second, step, 6 + side)

    def close(self):
        self.started[6].wait_recv()
        self.started[7].wait_recv()
        own = chunk_of(self.blocks, self.first, self.place.at[self.first])
        mine = own.at[self.place.at[self.second]]
        return (
            mine[...].astype(jnp.float32)
            + self.last[0].astype(jnp.float32)
            + self.last[1].astype(jnp.float32)
        )


class Spreader:
    def __init__(self, place, first, blocks, sent, got):
        self.place, self.first, self.second = place, first, "y" if first == "x" else "x"
        self.blocks, self.sent, self.got = blocks, sent, got
        self.started = []
        rows = blocks.shape[2]
        self.low, self.high = pl.ds(0, rows // 2), pl.ds(rows // 2, rows // 2)

    def send(self, ref, axis, step, number):
        copy = remote(
            ref, ref, self.sent.at[number], self.got.at[number], self.place.plane(axis, step)
        )
        copy.start()
        self.started.append(copy)

    def block(self, step):
        line = chunk_of(self.blocks, self.second, self.place.at[self.second])
        return line.at[self.place.index(self.first, step)]

    def line(self, step):
        return chunk_of(self.blocks, self.second, self.place.index(self.second, step))

    def open(self):
        self.send(self.block(0), self.first, 1, 0)
        self.send(self.block(0), self.first, SIDE - 1, 1)

    def pass_on(self):
        self.started[0].wait_recv()
        self.send(self.block(SIDE - 1).at[self.low], self.first, 1, 2)
        self.started[1].wait_recv()
        self.send(self.block(1).at[self.high], self.first, SIDE - 1, 3)

    def turn(self):
        self.started[2].wait_recv()
        self.started[3].wait_recv()
        self.send(self.line(0), self.second, 1, 4)
        self.send(self.line(0), self.second, SIDE - 1, 5)

    def pass_again(self):
        self.started[4].wait_recv()
        self.send(self.line(SIDE - 1).at[:, self.low], self.second, 1, 6)
        self.started[5].wait_recv()
        self.send(self.line(1).at[:, self.high], self.second, SIDE - 1, 7)

    def close(self):
        self.started[6].wait_recv()
        self.started[7].wait_recv()


def iota(shape, dim):
    return lax.broadcasted_iota(jnp.int32, shape, dim)


def ones_where(mask):
    return jnp.where(mask, 1.0, 0.0).astype(jnp.bfloat16)


def dot(a, b):
    return jnp.dot(a, b, preferred_element_type=jnp.float32)


def in_two(x):
    high = x.astype(jnp.bfloat16)
    return high, (x - high.astype(jnp.float32)).astype(jnp.bfloat16)


def routing_tables(experts, cap, routes, routes_turned, weights, choice, share):
    tokens, picks = routes.shape
    slots = experts * cap
    shift = cap.bit_length() - 1
    named = routes[...]
    turned = routes_turned[...]
    amount = weights[...]
    lines = iota((experts, tokens), 0)
    there = turned[0:1, :] == lines
    for k in range(1, picks):
        there = there | (turned[k : k + 1, :] == lines)
    before = ones_where(iota((tokens, tokens), 0) < iota((tokens, tokens), 1))
    rank = jnp.where(there, dot(ones_where(there), before), -1.0).astype(jnp.bfloat16)
    spread = ones_where((iota((slots, experts), 0) >> shift) == iota((slots, experts), 1))
    wide = dot(spread, rank)
    number = (iota((slots, tokens), 0) & (cap - 1)).astype(jnp.float32)
    choice[...] = ones_where(wide == number)

    columns = iota((tokens, experts), 1)
    hit = named[:, 0:1] == columns
    weight = jnp.where(hit, amount[:, 0:1], 0.0)
    for k in range(1, picks):
        now = named[:, k : k + 1] == columns
        hit = hit | now
        weight = weight + jnp.where(now, amount[:, k : k + 1], 0.0)
    after = ones_where(iota((tokens, tokens), 1) < iota((tokens, tokens), 0))
    rank = jnp.where(hit, dot(after, ones_where(hit)), -1.0).astype(jnp.bfloat16)
    spread = ones_where(iota((experts, slots), 0) == (iota((experts, slots), 1) >> shift))
    wide = dot(rank, spread)
    number = (iota((tokens, slots), 1) & (cap - 1)).astype(jnp.float32)
    mine = wide == number
    for part, piece in enumerate(in_two(weight)):
        share[part] = jnp.where(mine, dot(piece, spread), 0.0).astype(jnp.bfloat16)


def expert_kernel(
    chips,
    cap,
    unit_chips,
    normed,
    state,
    routes,
    routes_turned,
    weights,
    gate_hbm,
    up_hbm,
    down_hbm,
    out,
    choice,
    share,
    outgoing,
    tokens,
    gate_up,
    down,
    partial,
    relay,
    sums,
    half,
    last,
    result,
    back,
    load_sem,
    out_sent,
    out_got,
    spread_sent,
    spread_got,
    sum_sent,
    sum_got,
    back_sent,
    back_got,
):
    place = Place(chips)
    experts = chips * CORES
    barrier, count = greet(place)
    loads = [
        pltpu.make_async_copy(gate_hbm, gate_up.at[:, pl.ds(0, gate_hbm.shape[1])], load_sem.at[0]),
        pltpu.make_async_copy(
            up_hbm, gate_up.at[:, pl.ds(gate_hbm.shape[1], gate_hbm.shape[1])], load_sem.at[1]
        ),
        pltpu.make_async_copy(down_hbm, down, load_sem.at[2]),
    ]
    for load in loads:
        load.start()
    routing_tables(experts, cap, routes, routes_turned, weights, choice, share)
    outgoing[...] = dot(choice[...], normed[...]).astype(jnp.bfloat16)
    pl.semaphore_wait(barrier, count)

    order = chip_order(chips)
    spot = {d: k for k, d in enumerate(order)}
    y, x = place.at["y"], place.at["x"]

    def slot_rows(number):
        return pl.ds(pl.multiple_of(number * cap, cap), cap)

    dispatch = {}
    for d in order:
        for other in (0, 1):
            core = place.core if other == 0 else 1 - place.core
            device = place.along((chips - d) % chips, core)
            rows = slot_rows(device[0])
            to = slot_rows(spot[d] * CORES + place.core)
            if d == 0 and other == 0:
                tokens[y, x, to, :] = outgoing[rows, :]
                continue
            number = spot[d] * CORES + other
            copy = remote(
                outgoing.at[rows],
                tokens.at[y, x, to],
                out_sent.at[number],
                out_got.at[number],
                device,
            )
            copy.start()
            dispatch[(d, other)] = copy

    unit = unit_chips * CORES * cap
    units = chips // unit_chips
    width = gate_hbm.shape[1]
    returns = {}

    def steps(u):
        first = "x" if u % 2 == 0 else "y"
        rows = pl.ds(u * unit, unit)
        spread = Spreader(
            place, first, tokens.at[:, :, rows], spread_sent.at[u], spread_got.at[u]
        )
        total = Summer(
            place, first, partial.at[u], relay.at[u], sums.at[u], half.at[u], last.at[u],
            sum_sent.at[u], sum_got.at[u],
        )

        def arrive():
            for d in order[u * unit_chips : (u + 1) * unit_chips]:
                for other in (0, 1):
                    if (d, other) in dispatch:
                        dispatch[(d, other)].wait_recv()
            spread.open()

        def compute():
            spread.close()
            if u == 0:
                for load in loads:
                    load.wait()
            lines = jnp.concatenate(
                [tokens[i, j, rows, :] for i in range(SIDE) for j in range(SIDE)], axis=1
            )
            both = dot(lines, gate_up[...])
            gate = jnp.minimum(both[:, :width], CLAMP_LIMIT)
            up = jnp.clip(both[:, width:], -CLAMP_LIMIT, CLAMP_LIMIT)
            act = ((up + 1.0) * gate * jax.nn.sigmoid(SIGMOID_SCALE * gate)).astype(jnp.bfloat16)
            for i in range(SIDE):
                wide = dot(act, down[:, i * SIDE * width : (i + 1) * SIDE * width])
                for j in range(SIDE):
                    partial[u, i, j] = wide[:, j * width : (j + 1) * width].astype(jnp.bfloat16)
            total.open()

        def close():
            result[u] = total.close().astype(jnp.bfloat16)
            for k, d in enumerate(order[u * unit_chips : (u + 1) * unit_chips]):
                for other in (0, 1):
                    core = place.core if other == 0 else 1 - place.core
                    piece = slot_rows(k * CORES + core)
                    to = slot_rows(place.sp)
                    if d == 0 and other == 0:
                        back[to, :] = result[u, piece, :]
                        continue
                    number = spot[d] * CORES + other
                    copy = remote(
                        result.at[u, piece],
                        back.at[to],
                        back_sent.at[number],
                        back_got.at[number],
                        place.along(d, core),
                    )
                    copy.start()
                    returns[(d, other)] = copy

        plan = [
            arrive, spread.pass_on, spread.turn, spread.pass_again, compute,
            total.pass_on, total.turn, total.pass_again, close,
        ]
        return plan, spread, total

    plans = [steps(u) for u in range(units)]
    depth = len(plans[0][0])
    for tick in range(units + depth - 1):
        for u in range(units):
            if 0 <= tick - u < depth:
                plans[u][0][tick - u]()
    for copy in returns.values():
        copy.wait_recv()
    combined = state[...] + dot(share[0], back[...]) + dot(share[1], back[...])
    out[...] = combined.astype(jnp.bfloat16)
    for copy in list(dispatch.values()) + list(returns.values()):
        copy.wait_send()
    for _, spread, total in plans:
        for copy in spread.started + total.started:
            copy.wait_send()


def expert_layer(normed, state, routes, weights, gate, up, down, chips, unit_chips):
    length, width = normed.shape
    experts = chips * CORES
    picks = routes.shape[1]
    cap = 4 * length * picks // (3 * experts)
    features = gate.shape[0]
    unit = unit_chips * CORES * cap
    units = chips // unit_chips
    slots = experts * cap
    vmem, any_ = pl.BlockSpec(memory_space=pltpu.VMEM), pl.BlockSpec(memory_space=pl.ANY)
    bf16 = jnp.bfloat16
    return pl.pallas_call(
        functools.partial(expert_kernel, chips, cap, unit_chips),
        out_shape=jax.ShapeDtypeStruct((length, width), bf16),
        in_specs=[vmem] * 5 + [any_] * 3,
        out_specs=vmem,
        scratch_shapes=[
            pltpu.VMEM((slots, length), bf16),
            pltpu.VMEM((2, length, slots), bf16),
            pltpu.VMEM((slots, width), bf16),
            pltpu.VMEM((SIDE, SIDE, slots, width), bf16),
            pltpu.VMEM((features, 2 * gate.shape[1]), bf16),
            pltpu.VMEM(down.shape, bf16),
            pltpu.VMEM((units, SIDE, SIDE, unit, width), bf16),
            pltpu.VMEM((units, 2, SIDE, unit // 2, width), bf16),
            pltpu.VMEM((units, 2, SIDE, unit, width), bf16),
            pltpu.VMEM((units, 2, unit // 2, width), bf16),
            pltpu.VMEM((units, 2, unit, width), bf16),
            pltpu.VMEM((units, unit, width), bf16),
            pltpu.VMEM((slots, width), bf16),
            pltpu.SemaphoreType.DMA((3,)),
            pltpu.SemaphoreType.DMA((experts,)),
            pltpu.SemaphoreType.DMA((experts,)),
            pltpu.SemaphoreType.DMA((units, 8)),
            pltpu.SemaphoreType.DMA((units, 8)),
            pltpu.SemaphoreType.DMA((units, 8)),
            pltpu.SemaphoreType.DMA((units, 8)),
            pltpu.SemaphoreType.DMA((experts,)),
            pltpu.SemaphoreType.DMA((experts,)),
        ],
        compiler_params=pltpu.CompilerParams(
            collective_id=1, has_side_effects=True, vmem_limit_bytes=56 * 1024 * 1024
        ),
    )(normed, state, routes, routes.T, weights, gate, up, down)


def local(
    resid,
    narrow_head_input,
    wide_head_input,
    key_group_input,
    query_group_input,
    narrow_output_gate,
    wide_output_gate,
    step_input_rows,
    head_decay_logarithm,
    position_log_decay,
    direct_input_weight,
    narrow_conv_taps,
    wide_conv_taps,
    key_conv_taps,
    query_conv_taps,
    narrow_norm_gain,
    wide_norm_gain,
    narrow_output_rows,
    wide_output_rows,
    feedforward_norm_gain,
    routes,
    routing_weight_values,
    expert_gate_matrix,
    expert_up_matrix,
    expert_down_matrix,
):
    length = resid.shape[0]
    head_count = narrow_head_input.shape[1] // NARROW_HEAD_DIM
    rim_len = narrow_conv_taps.shape[0] - 1
    rim_rows = passed_along(
        (
            narrow_head_input[length - rim_len :],
            wide_head_input[length - rim_len :],
            key_group_input[length - rim_len :],
            query_group_input[length - rim_len :],
        ),
        SP,
        1,
    )
    narrow_head_mix = conv_with_rim(narrow_head_input, rim_rows[0], narrow_conv_taps).reshape(
        length, head_count, NARROW_HEAD_DIM
    )
    wide_head_mix = conv_with_rim(wide_head_input, rim_rows[1], wide_conv_taps).reshape(
        length, head_count, WIDE_HEAD_DIM
    )
    first_head = lax.axis_index("tp") * head_count
    key_head_rows = pick_groups(
        conv_with_rim(key_group_input, rim_rows[2], key_conv_taps), first_head, head_count
    )
    query_head_rows = pick_groups(
        conv_with_rim(query_group_input, rim_rows[3], query_conv_taps), first_head, head_count
    )
    step_length_values = jax.nn.softplus(step_input_rows.astype(jnp.float32))
    narrow_parts = head_pieces_list(
        narrow_head_mix,
        step_length_values[:, 0],
        head_decay_logarithm[0],
        position_log_decay[:, 0],
        key_head_rows,
        query_head_rows,
    )
    wide_parts = head_pieces_list(
        wide_head_mix,
        step_length_values[:, 1],
        head_decay_logarithm[1],
        position_log_decay[:, 1],
        key_head_rows,
        query_head_rows,
    )
    summary = (narrow_parts[3], wide_parts[3], narrow_parts[2], wide_parts[2])
    carried = entering_2(
        summary,
        SP,
        chain_combine,
        (
            jnp.zeros_like(summary[0]),
            jnp.zeros_like(summary[1]),
            jnp.zeros_like(summary[2]),
            jnp.zeros_like(summary[3]),
        ),
    )
    narrow_carry, wide_carry = (carried[2], carried[3])
    narrow_head_output = group_out(
        finish_group(narrow_parts, narrow_carry),
        narrow_head_mix,
        direct_input_weight[0],
        narrow_output_gate,
        narrow_norm_gain,
    )
    wide_head_output = group_out(
        finish_group(wide_parts, wide_carry),
        wide_head_mix,
        direct_input_weight[1],
        wide_output_gate,
        wide_norm_gain,
    )
    partial_mix = jnp.dot(
        narrow_head_output, narrow_output_rows, preferred_element_type=jnp.float32
    )
    partial_mix = partial_mix + jnp.dot(
        wide_head_output, wide_output_rows, preferred_element_type=jnp.float32
    )
    mixed = total_of(partial_mix.astype(jnp.bfloat16), "tp")
    hidden_state = resid.astype(jnp.float32) + mixed
    normed = (
        hidden_state
        * lax.rsqrt(jnp.mean(hidden_state * hidden_state, axis=-1, keepdims=True) + NORM_EPS)
        * feedforward_norm_gain
    ).astype(jnp.bfloat16)
    column_width = normed.shape[1] // lax.axis_size("tp")
    tp_index = lax.axis_index("tp")
    own_columns = lax.dynamic_slice_in_dim(normed, tp_index * column_width, column_width, 1)
    own_state = lax.dynamic_slice_in_dim(hidden_state, tp_index * column_width, column_width, 1)
    return expert_layer(
        own_columns,
        own_state,
        routes,
        routing_weight_values,
        expert_gate_matrix[0],
        expert_up_matrix[0],
        expert_down_matrix[0],
        lax.axis_size(SP) // CORES,
        2,
    )


def solution(mesh):
    return jax.shard_map(
        local,
        mesh=mesh,
        in_specs=(
            P(SP, None),
            P(SP, "tp"),
            P(SP, "tp"),
            P(SP, None),
            P(SP, None),
            P(SP, "tp"),
            P(SP, "tp"),
            P(SP, None, "tp"),
            P(None, "tp"),
            P(SP, None, "tp"),
            P(None, "tp"),
            P(None, "tp"),
            P(None, "tp"),
            P(),
            P(),
            P("tp"),
            P("tp"),
            P("tp", None),
            P("tp", None),
            P(),
            P(SP, None),
            P(SP, None),
            P(SP, None, "tp"),
            P(SP, None, "tp"),
            P(SP, "tp", None),
        ),
        out_specs=P(SP, "tp"),
        check_vma=False,
    )
```

```python
import functools

import jax
import jax.numpy as jnp
from jax import lax
from jax.experimental import pallas as pl
from jax.experimental.pallas import tpu as pltpu
from jax.sharding import PartitionSpec as P

HEADS = 16
NARROW_HEAD_DIM = 64
WIDE_HEAD_DIM = 128
GROUPS = 4
CONV = 4
SP = "sp"


NORM_EPS = 1e-06
CLAMP_LIMIT = 7.0
SIGMOID_SCALE = 1.702
FULL_PRECISION = lax.Precision.HIGHEST


MESH = pl.DeviceIdType.MESH
CORES = 2
SIDE = 4
LAG = 2


def remote(src, dst, send_sem, recv_sem, device):
    return pltpu.make_async_remote_copy(
        src_ref=src,
        dst_ref=dst,
        send_sem=send_sem,
        recv_sem=recv_sem,
        device_id=device,
        device_id_type=MESH,
    )


class Place:
    def __init__(self, chips):
        self.chips = chips
        self.sp = lax.axis_index("sp")
        self.tp = lax.axis_index("tp")
        self.z, self.core = self.sp // CORES, self.sp % CORES
        self.at = {"y": self.tp // SIDE, "x": self.tp % SIDE}

    def plane(self, axis, step):
        moved = (self.at[axis] + step + SIDE) % SIDE
        if axis == "x":
            return (self.sp, self.at["y"] * SIDE + moved)
        return (self.sp, moved * SIDE + self.at["x"])

    def index(self, axis, step):
        return (self.at[axis] + step + SIDE) % SIDE

    def along(self, step, core):
        return (((self.z + step + self.chips) % self.chips) * CORES + core, self.tp)


def chip_order(chips):
    if chips == 16:
        return [1, 15, 3, 13, 5, 11, 7, 9, 8, 6, 10, 4, 12, 2, 14, 0]
    return [d % chips for d in range(1, chips + 1)]


def greet(place):
    barrier = pltpu.get_barrier_semaphore()
    count = 0
    for axis in ("x", "y"):
        for step in (1, SIDE - 1):
            pl.semaphore_signal(barrier, inc=1, device_id=place.plane(axis, step), device_id_type=MESH)
            count += 1
    for step in range(place.chips):
        if step:
            pl.semaphore_signal(
                barrier, inc=1, device_id=place.along(step, place.core), device_id_type=MESH
            )
            count += 1
        pl.semaphore_signal(
            barrier, inc=1, device_id=place.along(step, 1 - place.core), device_id_type=MESH
        )
        count += 1
    return barrier, count


def chunk_of(ref, axis, index):
    return ref.at[index] if axis == "y" else ref.at[:, index]


class Summer:
    def __init__(self, place, first, blocks, relay, sums, half, last, sent, got):
        self.place, self.first, self.second = place, first, "y" if first == "x" else "x"
        self.blocks, self.relay, self.sums = blocks, relay, sums
        self.half, self.last, self.sent, self.got = half, last, sent, got
        self.started = []
        rows = blocks.shape[2]
        self.low, self.high = pl.ds(0, rows // 2), pl.ds(rows // 2, rows // 2)

    def send(self, src, dst, axis, step, number):
        copy = remote(
            src, dst, self.sent.at[number], self.got.at[number], self.place.plane(axis, step)
        )
        copy.start()
        self.started.append(copy)

    def open(self):
        far = chunk_of(self.blocks, self.first, self.place.index(self.first, 2))
        self.send(far.at[:, self.low], self.relay.at[0], self.first, 1, 0)
        self.send(far.at[:, self.high], self.relay.at[1], self.first, SIDE - 1, 1)

    def pass_on(self):
        for side, step in ((0, 1), (1, SIDE - 1)):
            part = self.low if side == 0 else self.high
            self.started[side].wait_recv()
            near = chunk_of(self.blocks, self.first, self.place.index(self.first, step))
            piece = near.at[:, part]
            piece[...] = (
                piece[...].astype(jnp.float32) + self.relay[side].astype(jnp.float32)
            ).astype(jnp.bfloat16)
            self.send(near, self.sums.at[side], self.first, step, 2 + side)

    def turn(self):
        self.started[2].wait_recv()
        self.started[3].wait_recv()
        own = chunk_of(self.blocks, self.first, self.place.at[self.first])
        own[...] = (
            own[...].astype(jnp.float32)
            + self.sums[0].astype(jnp.float32)
            + self.sums[1].astype(jnp.float32)
        ).astype(jnp.bfloat16)
        far = own.at[self.place.index(self.second, 2)]
        self.send(far.at[self.low], self.half.at[0], self.second, 1, 4)
        self.send(far.at[self.high], self.half.at[1], self.second, SIDE - 1, 5)

    def pass_again(self):
        own = chunk_of(self.blocks, self.first, self.place.at[self.first])
        for side, step in ((0, 1), (1, SIDE - 1)):
            part = self.low if side == 0 else self.high
            self.started[4 + side].wait_recv()
            near = own.at[self.place.index(self.second, step)]
            piece = near.at[part]
            piece[...] = (
                piece[...].astype(jnp.float32) + self.half[side].astype(jnp.float32)
            ).astype(jnp.bfloat16)
            self.send(near, self.last.at[side], self.second, step, 6 + side)

    def close(self):
        self.started[6].wait_recv()
        self.started[7].wait_recv()
        own = chunk_of(self.blocks, self.first, self.place.at[self.first])
        mine = own.at[self.place.at[self.second]]
        return (
            mine[...].astype(jnp.float32)
            + self.last[0].astype(jnp.float32)
            + self.last[1].astype(jnp.float32)
        )


class Spreader:
    def __init__(self, place, first, blocks, sent, got):
        self.place, self.first, self.second = place, first, "y" if first == "x" else "x"
        self.blocks, self.sent, self.got = blocks, sent, got
        self.started = []
        rows = blocks.shape[2]
        self.low, self.high = pl.ds(0, rows // 2), pl.ds(rows // 2, rows // 2)

    def send(self, ref, axis, step, number):
        copy = remote(
            ref, ref, self.sent.at[number], self.got.at[number], self.place.plane(axis, step)
        )
        copy.start()
        self.started.append(copy)

    def block(self, step):
        line = chunk_of(self.blocks, self.second, self.place.at[self.second])
        return line.at[self.place.index(self.first, step)]

    def line(self, step):
        return chunk_of(self.blocks, self.second, self.place.index(self.second, step))

    def open(self):
        self.send(self.block(0), self.first, 1, 0)
        self.send(self.block(0), self.first, SIDE - 1, 1)

    def pass_on(self):
        self.started[0].wait_recv()
        self.send(self.block(SIDE - 1).at[self.low], self.first, 1, 2)
        self.started[1].wait_recv()
        self.send(self.block(1).at[self.high], self.first, SIDE - 1, 3)

    def turn(self):
        self.started[2].wait_recv()
        self.started[3].wait_recv()
        self.send(self.line(0), self.second, 1, 4)
        self.send(self.line(0), self.second, SIDE - 1, 5)

    def pass_again(self):
        self.started[4].wait_recv()
        self.send(self.line(SIDE - 1).at[:, self.low], self.second, 1, 6)
        self.started[5].wait_recv()
        self.send(self.line(1).at[:, self.high], self.second, SIDE - 1, 7)

    def close(self):
        self.started[6].wait_recv()
        self.started[7].wait_recv()


def iota(shape, dim):
    return lax.broadcasted_iota(jnp.int32, shape, dim)


def ones_where(mask):
    return jnp.where(mask, 1.0, 0.0).astype(jnp.bfloat16)


def dot(a, b):
    return jnp.dot(a, b, preferred_element_type=jnp.float32)


def in_two(x):
    high = x.astype(jnp.bfloat16)
    return high, (x - high.astype(jnp.float32)).astype(jnp.bfloat16)


def routing_tables(experts, cap, routes, routes_turned, weights, choice, share):
    tokens, picks = routes.shape
    slots = experts * cap
    shift = cap.bit_length() - 1
    named = routes[...]
    turned = routes_turned[...]
    amount = weights[...]
    lines = iota((experts, tokens), 0)
    there = turned[0:1, :] == lines
    for k in range(1, picks):
        there = there | (turned[k : k + 1, :] == lines)
    before = ones_where(iota((tokens, tokens), 0) < iota((tokens, tokens), 1))
    rank = jnp.where(there, dot(ones_where(there), before), -1.0).astype(jnp.bfloat16)
    spread = ones_where((iota((slots, experts), 0) >> shift) == iota((slots, experts), 1))
    wide = dot(spread, rank)
    number = (iota((slots, tokens), 0) & (cap - 1)).astype(jnp.float32)
    choice[...] = ones_where(wide == number)

    columns = iota((tokens, experts), 1)
    hit = named[:, 0:1] == columns
    weight = jnp.where(hit, amount[:, 0:1], 0.0)
    for k in range(1, picks):
        now = named[:, k : k + 1] == columns
        hit = hit | now
        weight = weight + jnp.where(now, amount[:, k : k + 1], 0.0)
    after = ones_where(iota((tokens, tokens), 1) < iota((tokens, tokens), 0))
    rank = jnp.where(hit, dot(after, ones_where(hit)), -1.0).astype(jnp.bfloat16)
    spread = ones_where(iota((experts, slots), 0) == (iota((experts, slots), 1) >> shift))
    wide = dot(rank, spread)
    number = (iota((tokens, slots), 1) & (cap - 1)).astype(jnp.float32)
    mine = wide == number
    for part, piece in enumerate(in_two(weight)):
        share[part] = jnp.where(mine, dot(piece, spread), 0.0).astype(jnp.bfloat16)


def expert_kernel(
    chips,
    cap,
    unit_chips,
    normed,
    state,
    routes,
    routes_turned,
    weights,
    gate_hbm,
    up_hbm,
    down_hbm,
    out,
    choice,
    share,
    outgoing,
    tokens,
    gate_up,
    down,
    partial,
    relay,
    sums,
    half,
    last,
    result,
    back,
    load_sem,
    out_sent,
    out_got,
    spread_sent,
    spread_got,
    sum_sent,
    sum_got,
    back_sent,
    back_got,
):
    place = Place(chips)
    experts = chips * CORES
    barrier, count = greet(place)
    loads = [
        pltpu.make_async_copy(gate_hbm, gate_up.at[:, pl.ds(0, gate_hbm.shape[1])], load_sem.at[0]),
        pltpu.make_async_copy(
            up_hbm, gate_up.at[:, pl.ds(gate_hbm.shape[1], gate_hbm.shape[1])], load_sem.at[1]
        ),
        pltpu.make_async_copy(down_hbm, down, load_sem.at[2]),
    ]
    for load in loads:
        load.start()
    routing_tables(experts, cap, routes, routes_turned, weights, choice, share)
    outgoing[...] = dot(choice[...], normed[...]).astype(jnp.bfloat16)
    pl.semaphore_wait(barrier, count)

    order = chip_order(chips)
    spot = {d: k for k, d in enumerate(order)}
    y, x = place.at["y"], place.at["x"]

    def slot_rows(number):
        return pl.ds(pl.multiple_of(number * cap, cap), cap)

    dispatch = {}
    for d in order:
        for other in (0, 1):
            core = place.core if other == 0 else 1 - place.core
            device = place.along((chips - d) % chips, core)
            rows = slot_rows(device[0])
            to = slot_rows(spot[d] * CORES + place.core)
            if d == 0 and other == 0:
                tokens[y, x, to, :] = outgoing[rows, :]
                continue
            number = spot[d] * CORES + other
            copy = remote(
                outgoing.at[rows],
                tokens.at[y, x, to],
                out_sent.at[number],
                out_got.at[number],
                device,
            )
            copy.start()
            dispatch[(d, other)] = copy

    unit = unit_chips * CORES * cap
    units = chips // unit_chips
    width = gate_hbm.shape[1]
    returns = {}

    def steps(u):
        first = "x" if u % 2 == 0 else "y"
        rows = pl.ds(u * unit, unit)
        spread = Spreader(
            place, first, tokens.at[:, :, rows], spread_sent.at[u], spread_got.at[u]
        )
        total = Summer(
            place, first, partial.at[u], relay.at[u], sums.at[u], half.at[u], last.at[u],
            sum_sent.at[u], sum_got.at[u],
        )

        def arrive():
            for d in order[u * unit_chips : (u + 1) * unit_chips]:
                for other in (0, 1):
                    if (d, other) in dispatch:
                        dispatch[(d, other)].wait_recv()
            spread.open()

        def compute():
            spread.close()
            if u == 0:
                for load in loads:
                    load.wait()
            lines = jnp.concatenate(
                [tokens[i, j, rows, :] for i in range(SIDE) for j in range(SIDE)], axis=1
            )
            both = dot(lines, gate_up[...])
            gate = jnp.minimum(both[:, :width], CLAMP_LIMIT)
            up = jnp.clip(both[:, width:], -CLAMP_LIMIT, CLAMP_LIMIT)
            act = ((up + 1.0) * gate * jax.nn.sigmoid(SIGMOID_SCALE * gate)).astype(jnp.bfloat16)
            for i in range(SIDE):
                wide = dot(act, down[:, i * SIDE * width : (i + 1) * SIDE * width])
                for j in range(SIDE):
                    partial[u, i, j] = wide[:, j * width : (j + 1) * width].astype(jnp.bfloat16)
            total.open()

        def close():
            result[u] = total.close().astype(jnp.bfloat16)
            for k, d in enumerate(order[u * unit_chips : (u + 1) * unit_chips]):
                for other in (0, 1):
                    core = place.core if other == 0 else 1 - place.core
                    piece = slot_rows(k * CORES + core)
                    to = slot_rows(place.sp)
                    if d == 0 and other == 0:
                        back[to, :] = result[u, piece, :]
                        continue
                    number = spot[d] * CORES + other
                    copy = remote(
                        result.at[u, piece],
                        back.at[to],
                        back_sent.at[number],
                        back_got.at[number],
                        place.along(d, core),
                    )
                    copy.start()
                    returns[(d, other)] = copy

        plan = [
            arrive, spread.pass_on, spread.turn, spread.pass_again, compute,
            total.pass_on, total.turn, total.pass_again, close,
        ]
        return plan, spread, total

    plans = [steps(u) for u in range(units)]
    depth = len(plans[0][0])
    turns = sorted((u + LAG * k, -k, u) for u in range(units) for k in range(depth))
    for _, k, u in turns:
        plans[u][0][-k]()
    for copy in returns.values():
        copy.wait_recv()
    combined = state[...] + dot(share[0], back[...]) + dot(share[1], back[...])
    out[...] = combined.astype(jnp.bfloat16)
    for copy in list(dispatch.values()) + list(returns.values()):
        copy.wait_send()
    for _, spread, total in plans:
        for copy in spread.started + total.started:
            copy.wait_send()


def expert_layer(normed, state, routes, weights, gate, up, down, chips, unit_chips):
    length, width = normed.shape
    experts = chips * CORES
    picks = routes.shape[1]
    cap = 4 * length * picks // (3 * experts)
    features = gate.shape[0]
    unit = unit_chips * CORES * cap
    units = chips // unit_chips
    slots = experts * cap
    vmem, any_ = pl.BlockSpec(memory_space=pltpu.VMEM), pl.BlockSpec(memory_space=pl.ANY)
    bf16 = jnp.bfloat16
    return pl.pallas_call(
        functools.partial(expert_kernel, chips, cap, unit_chips),
        out_shape=jax.ShapeDtypeStruct((length, width), bf16),
        in_specs=[vmem] * 5 + [any_] * 3,
        out_specs=vmem,
        scratch_shapes=[
            pltpu.VMEM((slots, length), bf16),
            pltpu.VMEM((2, length, slots), bf16),
            pltpu.VMEM((slots, width), bf16),
            pltpu.VMEM((SIDE, SIDE, slots, width), bf16),
            pltpu.VMEM((features, 2 * gate.shape[1]), bf16),
            pltpu.VMEM(down.shape, bf16),
            pltpu.VMEM((units, SIDE, SIDE, unit, width), bf16),
            pltpu.VMEM((units, 2, SIDE, unit // 2, width), bf16),
            pltpu.VMEM((units, 2, SIDE, unit, width), bf16),
            pltpu.VMEM((units, 2, unit // 2, width), bf16),
            pltpu.VMEM((units, 2, unit, width), bf16),
            pltpu.VMEM((units, unit, width), bf16),
            pltpu.VMEM((slots, width), bf16),
            pltpu.SemaphoreType.DMA((3,)),
            pltpu.SemaphoreType.DMA((experts,)),
            pltpu.SemaphoreType.DMA((experts,)),
            pltpu.SemaphoreType.DMA((units, 8)),
            pltpu.SemaphoreType.DMA((units, 8)),
            pltpu.SemaphoreType.DMA((units, 8)),
            pltpu.SemaphoreType.DMA((units, 8)),
            pltpu.SemaphoreType.DMA((experts,)),
            pltpu.SemaphoreType.DMA((experts,)),
        ],
        compiler_params=pltpu.CompilerParams(
            collective_id=1, has_side_effects=True, vmem_limit_bytes=56 * 1024 * 1024
        ),
    )(normed, state, routes, routes.T, weights, gate, up, down)


def fine_dot(a, b, dims=(((1,), (0,)), ((), ()))):
    return lax.dot_general(
        a, b, dims, precision=FULL_PRECISION, preferred_element_type=jnp.float32
    )


def in_three(x):
    high, rest = x.astype(jnp.bfloat16), None
    rest = x - high.astype(jnp.float32)
    middle = rest.astype(jnp.bfloat16)
    low = (rest - middle.astype(jnp.float32)).astype(jnp.bfloat16)
    return high, middle, low


def silu(x):
    return x * jax.nn.sigmoid(x)


RIM = 16
STATE_ROWS = 8


def mixer_kernel(
    chips,
    narrow_in,
    wide_in,
    narrow_gate,
    wide_gate,
    columns,
    lines,
    narrow_taps,
    wide_taps,
    key_taps,
    query_taps,
    narrow_gain,
    wide_gain,
    last_gain,
    key_hbm,
    query_hbm,
    resid_hbm,
    narrow_rows_hbm,
    wide_rows_hbm,
    normed_out,
    state_out,
    keys,
    queries,
    resid,
    narrow_rows,
    wide_rows,
    narrow_rim,
    wide_rim,
    key_rim,
    query_rim,
    padded,
    told,
    heard,
    answer,
    carried,
    partial,
    relay,
    sums,
    half,
    last,
    squares_out,
    squares,
    load_sem,
    rim_sent,
    rim_got,
    told_sent,
    told_got,
    answer_sent,
    answer_got,
    sum_sent,
    sum_got,
    square_sent,
    square_got,
):
    place = Place(chips)
    devices = chips * CORES
    length = narrow_in.shape[0]
    width = keys.shape[1]
    plane = SIDE * SIDE
    barrier = pltpu.get_barrier_semaphore()
    count = 0
    for step in range(1, plane):
        pl.semaphore_signal(
            barrier, inc=1, device_id=(place.sp, (place.tp + step) % plane), device_id_type=MESH
        )
        count += 1
    for step in range(1, devices):
        pl.semaphore_signal(
            barrier, inc=1, device_id=((place.sp + step) % devices, place.tp), device_id_type=MESH
        )
        count += 1
    group = pl.multiple_of((place.tp // (HEADS // GROUPS)) * width, width)
    mine = pl.ds(pl.multiple_of(place.tp * width, width), width)
    pairs = (
        (key_hbm.at[:, pl.ds(group, width)], keys),
        (query_hbm.at[:, pl.ds(group, width)], queries),
        (resid_hbm.at[:, mine], resid),
        (narrow_rows_hbm, narrow_rows),
        (wide_rows_hbm, wide_rows),
    )
    loads = [pltpu.make_async_copy(src, dst, load_sem.at[k]) for k, (src, dst) in enumerate(pairs)]
    for load in loads:
        load.start()

    upper = ones_where(iota((length, length), 0) <= iota((length, length), 1))
    causal = iota((length, length), 0) >= iota((length, length), 1)
    lower = ones_where(causal)
    tall, flat = columns[...], lines[...]
    tall_sum = sum(dot(lower, piece) for piece in in_three(tall))
    flat_sum = sum(dot(piece, upper) for piece in in_three(flat))
    decay, tails, totals, steps = [], [], [], []
    for kind in (0, 1):
        down_column = tall_sum[:, 2 + kind : 3 + kind]
        across = flat_sum[2 + kind : 3 + kind, :]
        decay.append(jnp.exp(jnp.where(causal, down_column - across, -1e30)))
        total = down_column[length - 1 : length, :]
        totals.append(total)
        tails.append(jnp.exp(total - down_column))
        steps.append(tall[:, kind : kind + 1])
    fades = [jnp.exp(tall_sum[:, 2 + kind : 3 + kind]) for kind in (0, 1)]
    rows = iota((width, devices * STATE_ROWS), 0)
    spots = iota((width, devices * STATE_ROWS), 1)
    per = STATE_ROWS // 2
    owner_row = (spots >> 3) * per + (spots & (per - 1))
    wide_spread = jnp.where((owner_row == rows) & ((spots & 7) < per), 1.0, 0.0)
    narrow_spread = jnp.where((owner_row == rows) & ((spots & 7) >= per), 1.0, 0.0)

    loads[0].wait()
    loads[1].wait()
    pl.semaphore_wait(barrier, count)
    following = ((place.sp + 1) % devices, place.tp)
    rims = []
    tail = pl.ds(length - RIM, RIM)
    for k, (src, dst) in enumerate(
        ((narrow_in, narrow_rim), (wide_in, wide_rim), (keys, key_rim), (queries, query_rim))
    ):
        copy = remote(src.at[tail], dst, rim_sent.at[k], rim_got.at[k], following)
        copy.start()
        rims.append(copy)
    for copy in rims:
        copy.wait_recv()

    inner = place.sp > 0

    def mixed_rows(values, rim, taps):
        size = values.shape[1]
        before = jnp.where(inner, rim[...].astype(jnp.float32), 0.0)
        padded[0:RIM, 0:size] = before
        padded[RIM : RIM + length, 0:size] = values[...].astype(jnp.float32)
        total = jnp.zeros((length, size), jnp.float32)
        for k in range(CONV):
            start = RIM - CONV + 1 + k
            total = total + taps[k : k + 1, :] * padded[start : start + length, 0:size]
        return silu(total)

    key = mixed_rows(keys, key_rim, key_taps[:, pl.ds(group, width)])
    query = mixed_rows(queries, query_rim, query_taps[:, pl.ds(group, width)])
    narrow_mix = mixed_rows(narrow_in, narrow_rim, narrow_taps[...])
    wide_mix = mixed_rows(wide_in, wide_rim, wide_taps[...])
    narrow_size = narrow_mix.shape[1]
    narrow_value, wide_value = narrow_mix * steps[0], wide_mix * steps[1]

    turned = (((0,), (0,)), ((), ()))
    wide_keys = fine_dot(key, wide_spread)
    narrow_keys = fine_dot(key, narrow_spread)
    wide_state = fine_dot(wide_keys, wide_value * tails[1], turned)
    narrow_state = fine_dot(
        narrow_keys,
        jnp.concatenate(
            [narrow_value * tails[0], jnp.zeros((length, width - narrow_size), jnp.float32)], axis=1
        ),
        turned,
    )
    tile = iota((devices * STATE_ROWS, width), 0) & 7
    lane = iota((devices * STATE_ROWS, width), 1)
    spare = jnp.where(lane < (narrow_size + width) // 2, totals[1], totals[0])
    message = wide_state + narrow_state
    message = jnp.where((tile >= per) & (lane >= narrow_size), spare, message)
    told[...] = message.reshape(devices, STATE_ROWS, width).astype(jnp.bfloat16)

    def exchange(src, dst, sent, got):
        copies = []
        dst[place.sp] = src[place.sp]
        for step in range(1, devices):
            other = (place.sp + step) % devices
            copy = remote(
                src.at[other], dst.at[place.sp], sent.at[step], got.at[step], (other, place.tp)
            )
            copy.start()
            copies.append(copy)
        return copies

    tells = exchange(told, heard, told_sent, told_got)

    scores = fine_dot(query, key, (((1,), (1,)), ((), ())))
    narrow_inside = fine_dot(scores * decay[0], narrow_value)
    wide_inside = fine_dot(scores * decay[1], wide_value)
    wide_query = fine_dot(query * fades[1], wide_spread)
    narrow_query = fine_dot(query * fades[0], narrow_spread)
    narrow_open, wide_open = silu(narrow_gate[...].astype(jnp.float32)), silu(
        wide_gate[...].astype(jnp.float32)
    )

    for copy in tells:
        copy.wait_recv()
    running = jnp.zeros((STATE_ROWS, width), jnp.float32)
    upper_rows = iota((STATE_ROWS, width), 0) < per
    for source in range(devices):
        answer[source] = running.astype(jnp.bfloat16)
        piece = heard[source].astype(jnp.float32)
        wide_total = piece[per : per + 1, narrow_size : narrow_size + 1]
        middle = (narrow_size + width) // 2
        narrow_total = piece[per : per + 1, middle : middle + 1]
        factor = jnp.exp(jnp.where(upper_rows, wide_total, narrow_total))
        running = factor * running + piece
    answers = exchange(answer, carried, answer_sent, answer_got)

    for load in loads[2:]:
        load.wait()
    for copy in answers:
        copy.wait_recv()
    entering = carried[...].astype(jnp.float32).reshape(devices * STATE_ROWS, width)

    def head(inside, asked, size, kind, mix, opened, gain):
        result = inside + fine_dot(asked, entering)[:, :size]
        result = (result + tall[:, 4 + kind : 5 + kind] * mix) * opened
        mean = jnp.sum(result * result, axis=-1, keepdims=True) * (1.0 / size)
        return (result * lax.rsqrt(mean + NORM_EPS) * gain[...]).astype(jnp.bfloat16)

    narrow = head(narrow_inside, narrow_query, narrow_size, 0, narrow_mix, narrow_open, narrow_gain)
    wide = head(wide_inside, wide_query, width, 1, wide_mix, wide_open, wide_gain)

    totals_of = [
        Summer(
            place, first, partial.at[u], relay.at[u], sums.at[u], half.at[u], last.at[u],
            sum_sent.at[u], sum_got.at[u],
        )
        for u, first in ((0, "x"), (1, "y"))
    ]
    unit = length // 2
    for i in range(SIDE):
        part = pl.ds(i * SIDE * width, SIDE * width)
        product = dot(narrow, narrow_rows[:, part]) + dot(wide, wide_rows[:, part])
        product = product.astype(jnp.bfloat16)
        for j in range(SIDE):
            for u in (0, 1):
                partial[u, i, j] = product[u * unit : (u + 1) * unit, j * width : (j + 1) * width]
    for move in ("open", "pass_on", "turn", "pass_again"):
        for total in totals_of:
            getattr(total, move)()
    mixed = jnp.concatenate([total.close() for total in totals_of], axis=0)
    hidden = resid[...].astype(jnp.float32) + mixed
    state_out[...] = hidden
    ones = jnp.ones((8, width), jnp.float32)
    own = fine_dot(ones, hidden * hidden, (((1,), (1,)), ((), ())))[0:1, :]
    squares_out[...] = own
    squares[place.tp] = own
    shares = []
    for step in range(1, plane):
        other = (place.tp + step) % plane
        copy = remote(
            squares_out, squares.at[place.tp], square_sent.at[step], square_got.at[step],
            (place.sp, other),
        )
        copy.start()
        shares.append(copy)
    for copy in shares:
        copy.wait_recv()
    whole = squares[0]
    for k in range(1, plane):
        whole = whole + squares[k]
    diagonal = iota((length, length), 0) == iota((length, length), 1)
    mean = jnp.sum(jnp.where(diagonal, whole, 0.0), axis=1, keepdims=True) * (1.0 / (plane * width))
    normed_out[...] = (
        hidden * lax.rsqrt(mean + NORM_EPS) * last_gain[:, mine]
    ).astype(jnp.bfloat16)
    for copy in rims + tells + answers + shares:
        copy.wait_send()
    for total in totals_of:
        for copy in total.started:
            copy.wait_send()


def mixer_layer(
    narrow_in,
    wide_in,
    narrow_gate,
    wide_gate,
    columns,
    narrow_taps,
    wide_taps,
    key_taps,
    query_taps,
    narrow_gain,
    wide_gain,
    last_gain,
    key_in,
    query_in,
    resid,
    narrow_rows,
    wide_rows,
    chips,
):
    length, width = wide_in.shape
    devices = chips * CORES
    plane = SIDE * SIDE
    unit = length // 2
    bf16, f32 = jnp.bfloat16, jnp.float32
    vmem, any_ = pl.BlockSpec(memory_space=pltpu.VMEM), pl.BlockSpec(memory_space=pl.ANY)
    dma = pltpu.SemaphoreType.DMA
    return pl.pallas_call(
        functools.partial(mixer_kernel, chips),
        out_shape=(
            jax.ShapeDtypeStruct((length, width), bf16),
            jax.ShapeDtypeStruct((length, width), f32),
        ),
        in_specs=[vmem] * 13 + [any_] * 5,
        out_specs=(vmem, vmem),
        scratch_shapes=[
            pltpu.VMEM((length, width), bf16),
            pltpu.VMEM((length, width), bf16),
            pltpu.VMEM((length, width), bf16),
            pltpu.VMEM(narrow_rows.shape, bf16),
            pltpu.VMEM(wide_rows.shape, bf16),
            pltpu.VMEM((RIM, narrow_in.shape[1]), bf16),
            pltpu.VMEM((RIM, width), bf16),
            pltpu.VMEM((RIM, width), bf16),
            pltpu.VMEM((RIM, width), bf16),
            pltpu.VMEM((RIM + length, width), f32),
            pltpu.VMEM((devices, STATE_ROWS, width), bf16),
            pltpu.VMEM((devices, STATE_ROWS, width), bf16),
            pltpu.VMEM((devices, STATE_ROWS, width), bf16),
            pltpu.VMEM((devices, STATE_ROWS, width), bf16),
            pltpu.VMEM((2, SIDE, SIDE, unit, width), bf16),
            pltpu.VMEM((2, 2, SIDE, unit // 2, width), bf16),
            pltpu.VMEM((2, 2, SIDE, unit, width), bf16),
            pltpu.VMEM((2, 2, unit // 2, width), bf16),
            pltpu.VMEM((2, 2, unit, width), bf16),
            pltpu.VMEM((1, length), f32),
            pltpu.VMEM((plane, 1, length), f32),
            dma((5,)),
            dma((4,)),
            dma((4,)),
            dma((devices,)),
            dma((devices,)),
            dma((devices,)),
            dma((devices,)),
            dma((2, 8)),
            dma((2, 8)),
            dma((plane,)),
            dma((plane,)),
        ],
        compiler_params=pltpu.CompilerParams(
            collective_id=0, has_side_effects=True, vmem_limit_bytes=56 * 1024 * 1024
        ),
    )(
        narrow_in,
        wide_in,
        narrow_gate,
        wide_gate,
        columns,
        columns.T,
        narrow_taps,
        wide_taps,
        key_taps,
        query_taps,
        narrow_gain.reshape(1, -1),
        wide_gain.reshape(1, -1),
        last_gain.reshape(1, -1),
        key_in,
        query_in,
        resid,
        narrow_rows,
        wide_rows,
    )


def local(
    resid,
    narrow_head_input,
    wide_head_input,
    key_group_input,
    query_group_input,
    narrow_output_gate,
    wide_output_gate,
    step_input_rows,
    head_decay_logarithm,
    position_log_decay,
    direct_input_weight,
    narrow_conv_taps,
    wide_conv_taps,
    key_conv_taps,
    query_conv_taps,
    narrow_norm_gain,
    wide_norm_gain,
    narrow_output_rows,
    wide_output_rows,
    feedforward_norm_gain,
    routes,
    routing_weight_values,
    expert_gate_matrix,
    expert_up_matrix,
    expert_down_matrix,
):
    chips = lax.axis_size(SP) // CORES
    steps = jax.nn.softplus(step_input_rows[:, :, 0].astype(jnp.float32))
    decays = -jnp.exp(head_decay_logarithm[:, 0])[None, :] * steps + position_log_decay[:, :, 0]
    direct = jnp.broadcast_to(direct_input_weight[:, 0][None, :], steps.shape)
    columns = jnp.concatenate([steps, decays, direct, jnp.zeros_like(direct)], axis=1)
    own_columns, own_state = mixer_layer(
        narrow_head_input,
        wide_head_input,
        narrow_output_gate,
        wide_output_gate,
        columns,
        narrow_conv_taps,
        wide_conv_taps,
        key_conv_taps,
        query_conv_taps,
        narrow_norm_gain,
        wide_norm_gain,
        feedforward_norm_gain,
        key_group_input,
        query_group_input,
        resid,
        narrow_output_rows,
        wide_output_rows,
        chips,
    )
    return expert_layer(
        own_columns,
        own_state,
        routes,
        routing_weight_values,
        expert_gate_matrix[0],
        expert_up_matrix[0],
        expert_down_matrix[0],
        chips,
        2,
    )


def solution(mesh):
    return jax.shard_map(
        local,
        mesh=mesh,
        in_specs=(
            P(SP, None),
            P(SP, "tp"),
            P(SP, "tp"),
            P(SP, None),
            P(SP, None),
            P(SP, "tp"),
            P(SP, "tp"),
            P(SP, None, "tp"),
            P(None, "tp"),
            P(SP, None, "tp"),
            P(None, "tp"),
            P(None, "tp"),
            P(None, "tp"),
            P(),
            P(),
            P("tp"),
            P("tp"),
            P("tp", None),
            P("tp", None),
            P(),
            P(SP, None),
            P(SP, None),
            P(SP, None, "tp"),
            P(SP, None, "tp"),
            P(SP, "tp", None),
        ),
        out_specs=P(SP, "tp"),
        check_vma=False,
    )
```

```python
import functools

import jax
import jax.numpy as jnp
from jax import lax
from jax.experimental import pallas as pl
from jax.experimental.pallas import tpu as pltpu
from jax.sharding import PartitionSpec as P

HEADS = 16
NARROW_HEAD_DIM = 64
WIDE_HEAD_DIM = 128
GROUPS = 4
CONV = 4
SP = "sp"


NORM_EPS = 1e-06
CLAMP_LIMIT = 7.0
SIGMOID_SCALE = 1.702
FULL_PRECISION = lax.Precision.HIGHEST


MESH = pl.DeviceIdType.MESH
CORES = 2
SIDE = 4
LAG = 2
CHUNKS = 4


def remote(src, dst, send_sem, recv_sem, device):
    return pltpu.make_async_remote_copy(
        src_ref=src,
        dst_ref=dst,
        send_sem=send_sem,
        recv_sem=recv_sem,
        device_id=device,
        device_id_type=MESH,
    )


class Place:
    def __init__(self, chips):
        self.chips = chips
        self.sp = lax.axis_index("sp")
        self.tp = lax.axis_index("tp")
        self.z, self.core = self.sp // CORES, self.sp % CORES
        self.at = {"y": self.tp // SIDE, "x": self.tp % SIDE}

    def plane(self, axis, step):
        moved = (self.at[axis] + step + SIDE) % SIDE
        if axis == "x":
            return (self.sp, self.at["y"] * SIDE + moved)
        return (self.sp, moved * SIDE + self.at["x"])

    def index(self, axis, step):
        return (self.at[axis] + step + SIDE) % SIDE

    def along(self, step, core):
        return (((self.z + step + self.chips) % self.chips) * CORES + core, self.tp)


def chip_order(chips):
    if chips == 16:
        return [1, 15, 3, 13, 5, 11, 7, 9, 8, 6, 10, 4, 12, 2, 14, 0]
    return [d % chips for d in range(1, chips + 1)]


def greet(place):
    barrier = pltpu.get_barrier_semaphore()
    count = 0
    devices = place.chips * CORES
    for step in range(devices):
        for side in range(SIDE):
            if step or side:
                device = (
                    (place.sp + step) % devices,
                    place.at["y"] * SIDE + (place.at["x"] + side) % SIDE,
                )
                pl.semaphore_signal(barrier, inc=1, device_id=device, device_id_type=MESH)
                count += 1
    for step in range(1, SIDE):
        for side in range(SIDE):
            device = (place.sp, ((place.at["y"] + step) % SIDE) * SIDE + (place.at["x"] + side) % SIDE)
            pl.semaphore_signal(barrier, inc=1, device_id=device, device_id_type=MESH)
            count += 1
    return barrier, count


class Gather:
    def __init__(self, place, gate_up, down, sent, got):
        self.place, self.gate_up, self.down = place, gate_up, down
        self.sent, self.got, self.started, self.loads = sent, got, {}, []
        self.width = down.shape[0] // SIDE

    def piece(self, kind, step, part=None):
        index = self.place.index("x", step)
        if kind == 2:
            ref = self.down.at[pl.ds(pl.multiple_of(index * self.width, self.width), self.width)]
        else:
            start = pl.multiple_of(index * self.width + kind * SIDE * self.width, self.width)
            ref = self.gate_up.at[:, pl.ds(start, self.width)]
        if part is None:
            return ref
        size = ref.shape[0] // 2
        return ref.at[pl.ds(part * size, size)]

    def load(self, gate_hbm, up_hbm, down_hbm, sem):
        for kind, src in enumerate((gate_hbm, up_hbm, down_hbm)):
            copy = pltpu.make_async_copy(src, self.piece(kind, 0), sem.at[kind])
            copy.start()
            self.loads.append(copy)

    def send(self, ref, kind, number, step):
        copy = remote(
            ref, ref, self.sent.at[kind, number], self.got.at[kind, number],
            self.place.plane("x", step),
        )
        copy.start()
        self.started[(kind, number)] = copy

    def open(self):
        for kind in range(3):
            self.loads[kind].wait()
            self.send(self.piece(kind, 0), kind, 0, 1)
            self.send(self.piece(kind, 0), kind, 1, SIDE - 1)

    def pass_on(self, kind):
        self.started[(kind, 0)].wait_recv()
        self.send(self.piece(kind, SIDE - 1, 0), kind, 2, 1)
        self.started[(kind, 1)].wait_recv()
        self.send(self.piece(kind, 1, 1), kind, 3, SIDE - 1)

    def close(self):
        for kind in range(3):
            self.started[(kind, 2)].wait_recv()
            self.started[(kind, 3)].wait_recv()


class Line:
    def __init__(self, place, tokens, blocks, relay, sums, sent, got):
        self.place, self.tokens, self.blocks = place, tokens, blocks
        self.relay, self.sums, self.sent, self.got = relay, sums, sent, got
        self.started = []
        rows = tokens.shape[2]
        self.low, self.high = pl.ds(0, rows // 2), pl.ds(rows // 2, rows // 2)

    def send(self, src, dst, step):
        number = len(self.started)
        copy = remote(
            src, dst, self.sent.at[number], self.got.at[number], self.place.plane("y", step)
        )
        copy.start()
        self.started.append(copy)

    def open(self):
        own = self.tokens.at[self.place.at["y"]]
        self.send(own, own, 1)
        self.send(own, own, SIDE - 1)

    def pass_on(self):
        for side, step in ((0, SIDE - 1), (1, 1)):
            self.started[side].wait_recv()
            part = self.low if side == 0 else self.high
            ref = self.tokens.at[self.place.index("y", step)].at[:, part]
            self.send(ref, ref, SIDE - step)

    def arrived(self):
        self.started[2].wait_recv()
        self.started[3].wait_recv()

    def give(self):
        far = self.blocks.at[self.place.index("y", 2)]
        self.send(far.at[:, self.low], self.relay.at[0], 1)
        self.send(far.at[:, self.high], self.relay.at[1], SIDE - 1)

    def add(self):
        for side, step in ((0, 1), (1, SIDE - 1)):
            part = self.low if side == 0 else self.high
            self.started[4 + side].wait_recv()
            near = self.blocks.at[self.place.index("y", step)]
            piece = near.at[:, part]
            piece[...] = (
                piece[...].astype(jnp.float32) + self.relay[side].astype(jnp.float32)
            ).astype(jnp.bfloat16)
            self.send(near, self.sums.at[side], step)

    def total(self):
        self.started[6].wait_recv()
        self.started[7].wait_recv()
        return (
            self.blocks[self.place.at["y"]].astype(jnp.float32)
            + self.sums[0].astype(jnp.float32)
            + self.sums[1].astype(jnp.float32)
        )


def chunk_of(ref, axis, index):
    return ref.at[index] if axis == "y" else ref.at[:, index]


class Summer:
    def __init__(self, place, first, blocks, relay, sums, half, last, sent, got):
        self.place, self.first, self.second = place, first, "y" if first == "x" else "x"
        self.blocks, self.relay, self.sums = blocks, relay, sums
        self.half, self.last, self.sent, self.got = half, last, sent, got
        self.started = []
        rows = blocks.shape[2]
        self.low, self.high = pl.ds(0, rows // 2), pl.ds(rows // 2, rows // 2)

    def send(self, src, dst, axis, step, number):
        copy = remote(
            src, dst, self.sent.at[number], self.got.at[number], self.place.plane(axis, step)
        )
        copy.start()
        self.started.append(copy)

    def open(self):
        far = chunk_of(self.blocks, self.first, self.place.index(self.first, 2))
        self.send(far.at[:, self.low], self.relay.at[0], self.first, 1, 0)
        self.send(far.at[:, self.high], self.relay.at[1], self.first, SIDE - 1, 1)

    def pass_on(self):
        for side, step in ((0, 1), (1, SIDE - 1)):
            part = self.low if side == 0 else self.high
            self.started[side].wait_recv()
            near = chunk_of(self.blocks, self.first, self.place.index(self.first, step))
            piece = near.at[:, part]
            piece[...] = (
                piece[...].astype(jnp.float32) + self.relay[side].astype(jnp.float32)
            ).astype(jnp.bfloat16)
            self.send(near, self.sums.at[side], self.first, step, 2 + side)

    def turn(self):
        self.started[2].wait_recv()
        self.started[3].wait_recv()
        own = chunk_of(self.blocks, self.first, self.place.at[self.first])
        own[...] = (
            own[...].astype(jnp.float32)
            + self.sums[0].astype(jnp.float32)
            + self.sums[1].astype(jnp.float32)
        ).astype(jnp.bfloat16)
        far = own.at[self.place.index(self.second, 2)]
        self.send(far.at[self.low], self.half.at[0], self.second, 1, 4)
        self.send(far.at[self.high], self.half.at[1], self.second, SIDE - 1, 5)

    def pass_again(self):
        own = chunk_of(self.blocks, self.first, self.place.at[self.first])
        for side, step in ((0, 1), (1, SIDE - 1)):
            part = self.low if side == 0 else self.high
            self.started[4 + side].wait_recv()
            near = own.at[self.place.index(self.second, step)]
            piece = near.at[part]
            piece[...] = (
                piece[...].astype(jnp.float32) + self.half[side].astype(jnp.float32)
            ).astype(jnp.bfloat16)
            self.send(near, self.last.at[side], self.second, step, 6 + side)

    def close(self):
        self.started[6].wait_recv()
        self.started[7].wait_recv()
        own = chunk_of(self.blocks, self.first, self.place.at[self.first])
        mine = own.at[self.place.at[self.second]]
        return (
            mine[...].astype(jnp.float32)
            + self.last[0].astype(jnp.float32)
            + self.last[1].astype(jnp.float32)
        )


def iota(shape, dim):
    return lax.broadcasted_iota(jnp.int32, shape, dim)


def ones_where(mask):
    return jnp.where(mask, 1.0, 0.0).astype(jnp.bfloat16)


def dot(a, b):
    return jnp.dot(a, b, preferred_element_type=jnp.float32)


def in_two(x):
    high = x.astype(jnp.bfloat16)
    return high, (x - high.astype(jnp.float32)).astype(jnp.bfloat16)


def routing_tables(experts, cap, routes, routes_turned, weights, choice, share):
    tokens, picks = routes.shape
    slots = experts * cap
    shift = cap.bit_length() - 1
    named = routes[...]
    turned = routes_turned[...]
    amount = weights[...]
    lines = iota((experts, tokens), 0)
    there = turned[0:1, :] == lines
    for k in range(1, picks):
        there = there | (turned[k : k + 1, :] == lines)
    before = ones_where(iota((tokens, tokens), 0) < iota((tokens, tokens), 1))
    rank = jnp.where(there, dot(ones_where(there), before), -1.0).astype(jnp.bfloat16)
    spread = ones_where((iota((slots, experts), 0) >> shift) == iota((slots, experts), 1))
    wide = dot(spread, rank)
    number = (iota((slots, tokens), 0) & (cap - 1)).astype(jnp.float32)
    choice[...] = ones_where(wide == number)

    columns = iota((tokens, experts), 1)
    hit = named[:, 0:1] == columns
    weight = jnp.where(hit, amount[:, 0:1], 0.0)
    for k in range(1, picks):
        now = named[:, k : k + 1] == columns
        hit = hit | now
        weight = weight + jnp.where(now, amount[:, k : k + 1], 0.0)
    after = ones_where(iota((tokens, tokens), 1) < iota((tokens, tokens), 0))
    rank = jnp.where(hit, dot(after, ones_where(hit)), -1.0).astype(jnp.bfloat16)
    spread = ones_where(iota((experts, slots), 0) == (iota((experts, slots), 1) >> shift))
    wide = dot(rank, spread)
    number = (iota((tokens, slots), 1) & (cap - 1)).astype(jnp.float32)
    mine = wide == number
    for part, piece in enumerate(in_two(weight)):
        share[part] = jnp.where(mine, dot(piece, spread), 0.0).astype(jnp.bfloat16)


def fine_dot(a, b, dims=(((1,), (0,)), ((), ()))):
    return lax.dot_general(
        a, b, dims, precision=FULL_PRECISION, preferred_element_type=jnp.float32
    )


def in_three(x):
    high, rest = x.astype(jnp.bfloat16), None
    rest = x - high.astype(jnp.float32)
    middle = rest.astype(jnp.bfloat16)
    low = (rest - middle.astype(jnp.float32)).astype(jnp.bfloat16)
    return high, middle, low


def silu(x):
    return x * jax.nn.sigmoid(x)


RIM = 16
STATE_ROWS = 8


def layer_kernel(
    chips,
    cap,
    chunks,
    narrow_in,
    wide_in,
    narrow_gate,
    wide_gate,
    columns,
    lines,
    narrow_taps,
    wide_taps,
    key_taps,
    query_taps,
    narrow_gain,
    wide_gain,
    last_gain,
    key_hbm,
    query_hbm,
    resid_hbm,
    narrow_rows_hbm,
    wide_rows_hbm,
    routes,
    routes_turned,
    weights,
    gate_hbm,
    up_hbm,
    down_hbm,
    out,
    keys,
    queries,
    resid,
    narrow_rows,
    wide_rows,
    narrow_rim,
    wide_rim,
    key_rim,
    query_rim,
    padded,
    told,
    heard,
    answer,
    carried,
    partial,
    relay,
    sums,
    half,
    last,
    squares_out,
    squares,
    load_sem,
    rim_sent,
    rim_got,
    told_sent,
    told_got,
    answer_sent,
    answer_got,
    sum_sent,
    sum_got,
    square_sent,
    square_got,
    state,
    choice,
    share,
    outgoing,
    tokens,
    gate_up,
    down,
    blocks,
    line_relay,
    line_sums,
    result,
    back,
    weight_load,
    weight_sent,
    weight_got,
    out_sent,
    out_got,
    line_sent,
    line_got,
    back_sent,
    back_got,
):
    place = Place(chips)
    devices = chips * CORES
    length = narrow_in.shape[0]
    width = keys.shape[1]
    plane = SIDE * SIDE
    barrier, count = greet(place)
    group = pl.multiple_of((place.tp // (HEADS // GROUPS)) * width, width)
    mine = pl.ds(pl.multiple_of(place.tp * width, width), width)
    pairs = (
        (key_hbm.at[:, pl.ds(group, width)], keys),
        (query_hbm.at[:, pl.ds(group, width)], queries),
        (resid_hbm.at[:, mine], resid),
        (narrow_rows_hbm, narrow_rows),
        (wide_rows_hbm, wide_rows),
    )
    gather = Gather(place, gate_up, down, weight_sent, weight_got)
    gather.load(gate_hbm, up_hbm, down_hbm, weight_load)
    loads = [pltpu.make_async_copy(src, dst, load_sem.at[k]) for k, (src, dst) in enumerate(pairs)]
    for load in loads:
        load.start()

    upper = ones_where(iota((length, length), 0) <= iota((length, length), 1))
    causal = iota((length, length), 0) >= iota((length, length), 1)
    lower = ones_where(causal)
    tall, flat = columns[...], lines[...]
    tall_sum = sum(dot(lower, piece) for piece in in_three(tall))
    flat_sum = sum(dot(piece, upper) for piece in in_three(flat))
    decay, tails, totals, steps = [], [], [], []
    for kind in (0, 1):
        down_column = tall_sum[:, 2 + kind : 3 + kind]
        across = flat_sum[2 + kind : 3 + kind, :]
        decay.append(jnp.exp(jnp.where(causal, down_column - across, -1e30)))
        total = down_column[length - 1 : length, :]
        totals.append(total)
        tails.append(jnp.exp(total - down_column))
        steps.append(tall[:, kind : kind + 1])
    fades = [jnp.exp(tall_sum[:, 2 + kind : 3 + kind]) for kind in (0, 1)]
    rows = iota((width, devices * STATE_ROWS), 0)
    spots = iota((width, devices * STATE_ROWS), 1)
    per = STATE_ROWS // 2
    owner_row = (spots >> 3) * per + (spots & (per - 1))
    wide_spread = jnp.where((owner_row == rows) & ((spots & 7) < per), 1.0, 0.0)
    narrow_spread = jnp.where((owner_row == rows) & ((spots & 7) >= per), 1.0, 0.0)

    loads[0].wait()
    loads[1].wait()
    pl.semaphore_wait(barrier, count)
    gather.open()
    following = ((place.sp + 1) % devices, place.tp)
    rims = []
    tail = pl.ds(length - RIM, RIM)
    for k, (src, dst) in enumerate(
        ((narrow_in, narrow_rim), (wide_in, wide_rim), (keys, key_rim), (queries, query_rim))
    ):
        copy = remote(src.at[tail], dst, rim_sent.at[k], rim_got.at[k], following)
        copy.start()
        rims.append(copy)
    for copy in rims:
        copy.wait_recv()

    inner = place.sp > 0

    def mixed_rows(values, rim, taps):
        size = values.shape[1]
        before = jnp.where(inner, rim[...].astype(jnp.float32), 0.0)
        padded[0:RIM, 0:size] = before
        padded[RIM : RIM + length, 0:size] = values[...].astype(jnp.float32)
        total = jnp.zeros((length, size), jnp.float32)
        for k in range(CONV):
            start = RIM - CONV + 1 + k
            total = total + taps[k : k + 1, :] * padded[start : start + length, 0:size]
        return silu(total)

    key = mixed_rows(keys, key_rim, key_taps[:, pl.ds(group, width)])
    query = mixed_rows(queries, query_rim, query_taps[:, pl.ds(group, width)])
    narrow_mix = mixed_rows(narrow_in, narrow_rim, narrow_taps[...])
    wide_mix = mixed_rows(wide_in, wide_rim, wide_taps[...])
    narrow_size = narrow_mix.shape[1]
    narrow_value, wide_value = narrow_mix * steps[0], wide_mix * steps[1]

    turned = (((0,), (0,)), ((), ()))
    wide_keys = fine_dot(key, wide_spread)
    narrow_keys = fine_dot(key, narrow_spread)
    wide_state = fine_dot(wide_keys, wide_value * tails[1], turned)
    narrow_state = fine_dot(
        narrow_keys,
        jnp.concatenate(
            [narrow_value * tails[0], jnp.zeros((length, width - narrow_size), jnp.float32)], axis=1
        ),
        turned,
    )
    tile = iota((devices * STATE_ROWS, width), 0) & 7
    lane = iota((devices * STATE_ROWS, width), 1)
    spare = jnp.where(lane < (narrow_size + width) // 2, totals[1], totals[0])
    message = wide_state + narrow_state
    message = jnp.where((tile >= per) & (lane >= narrow_size), spare, message)
    told[...] = message.reshape(devices, STATE_ROWS, width).astype(jnp.bfloat16)

    def exchange(src, dst, sent, got):
        copies = []
        dst[place.sp] = src[place.sp]
        for step in range(1, devices):
            other = (place.sp + step) % devices
            copy = remote(
                src.at[other], dst.at[place.sp], sent.at[step], got.at[step], (other, place.tp)
            )
            copy.start()
            copies.append(copy)
        return copies

    tells = exchange(told, heard, told_sent, told_got)

    scores = fine_dot(query, key, (((1,), (1,)), ((), ())))
    narrow_inside = fine_dot(scores * decay[0], narrow_value)
    wide_inside = fine_dot(scores * decay[1], wide_value)
    wide_query = fine_dot(query * fades[1], wide_spread)
    narrow_query = fine_dot(query * fades[0], narrow_spread)
    narrow_open, wide_open = silu(narrow_gate[...].astype(jnp.float32)), silu(
        wide_gate[...].astype(jnp.float32)
    )

    for copy in tells:
        copy.wait_recv()
    gather.pass_on(0)
    running = jnp.zeros((STATE_ROWS, width), jnp.float32)
    upper_rows = iota((STATE_ROWS, width), 0) < per
    for source in range(devices):
        answer[source] = running.astype(jnp.bfloat16)
        piece = heard[source].astype(jnp.float32)
        wide_total = piece[per : per + 1, narrow_size : narrow_size + 1]
        middle = (narrow_size + width) // 2
        narrow_total = piece[per : per + 1, middle : middle + 1]
        factor = jnp.exp(jnp.where(upper_rows, wide_total, narrow_total))
        running = factor * running + piece
    answers = exchange(answer, carried, answer_sent, answer_got)
    routing_tables(devices, cap, routes, routes_turned, weights, choice, share)

    for load in loads[2:]:
        load.wait()
    for copy in answers:
        copy.wait_recv()
    gather.pass_on(1)
    entering = carried[...].astype(jnp.float32).reshape(devices * STATE_ROWS, width)

    def head(inside, asked, size, kind, mix, opened, gain):
        result = inside + fine_dot(asked, entering)[:, :size]
        result = (result + tall[:, 4 + kind : 5 + kind] * mix) * opened
        mean = jnp.sum(result * result, axis=-1, keepdims=True) * (1.0 / size)
        return (result * lax.rsqrt(mean + NORM_EPS) * gain[...]).astype(jnp.bfloat16)

    narrow = head(narrow_inside, narrow_query, narrow_size, 0, narrow_mix, narrow_open, narrow_gain)
    wide = head(wide_inside, wide_query, width, 1, wide_mix, wide_open, wide_gain)

    totals_of = [
        Summer(
            place, first, partial.at[u], relay.at[u], sums.at[u], half.at[u], last.at[u],
            sum_sent.at[u], sum_got.at[u],
        )
        for u, first in ((0, "y"), (1, "y"))
    ]
    unit = length // 2
    for i in range(SIDE):
        part = pl.ds(i * SIDE * width, SIDE * width)
        product = dot(narrow, narrow_rows[:, part]) + dot(wide, wide_rows[:, part])
        product = product.astype(jnp.bfloat16)
        for j in range(SIDE):
            for u in (0, 1):
                partial[u, i, j] = product[u * unit : (u + 1) * unit, j * width : (j + 1) * width]
    for move in ("open", "pass_on", "turn", "pass_again"):
        for total in totals_of:
            getattr(total, move)()
    mixed = jnp.concatenate([total.close() for total in totals_of], axis=0)
    hidden = resid[...].astype(jnp.float32) + mixed
    ones = jnp.ones((8, width), jnp.float32)
    own = fine_dot(ones, hidden * hidden, (((1,), (1,)), ((), ())))[0:1, :]
    gather.pass_on(2)
    squares_out[...] = own
    squares[place.tp] = own
    shares = []
    for step in range(1, plane):
        other = (place.tp + step) % plane
        copy = remote(
            squares_out, squares.at[place.tp], square_sent.at[step], square_got.at[step],
            (place.sp, other),
        )
        copy.start()
        shares.append(copy)
    for copy in shares:
        copy.wait_recv()
    whole = squares[0]
    for k in range(1, plane):
        whole = whole + squares[k]
    diagonal = iota((length, length), 0) == iota((length, length), 1)
    mean = jnp.sum(jnp.where(diagonal, whole, 0.0), axis=1, keepdims=True) * (1.0 / (plane * width))
    state[...] = hidden
    normed = (hidden * lax.rsqrt(mean + NORM_EPS) * last_gain[:, mine]).astype(jnp.bfloat16)

    outgoing[...] = dot(choice[...], normed).astype(jnp.bfloat16)
    order = chip_order(chips)
    spot = {d: k for k, d in enumerate(order)}
    y, x, core = place.at["y"], place.at["x"], place.core
    home = spot[0]
    inside = x == 2 * (home % 2) + core
    outside = x != 2 * (home % 2) + core
    waits = []

    def slot_rows(number):
        return pl.ds(pl.multiple_of(number * cap, cap), cap)

    def guarded(apart, act):
        if apart:
            pl.when(outside)(act)
        else:
            act()

    for s, d in enumerate(order):
        for other in (0, 1):
            aim = core if other == 0 else 1 - core
            target = ((place.z + chips - d) % chips) * CORES + aim
            device = (target, y * SIDE + 2 * (s % 2) + core)
            rows = slot_rows(target)
            to = pl.ds((s // 2) * cap, cap)
            copy = remote(
                outgoing.at[rows],
                tokens.at[y, x, to],
                out_sent.at[s * 2 + other],
                out_got.at[s // 2, x],
                device,
            )
            apart = d == 0 and other == 0
            guarded(apart, copy.start)
            waits.append((apart, copy))
            if apart:

                @pl.when(inside)
                def _(rows=rows, to=to):
                    tokens[y, x, to, :] = outgoing[rows, :]

    units = chips // 2
    per = units // chunks
    size = per * cap
    parts = []

    def steps(k):
        rows = pl.ds(k * size, size)
        line = Line(
            place, tokens.at[:, :, rows], blocks.at[k], line_relay.at[k], line_sums.at[k],
            line_sent.at[k], line_got.at[k],
        )
        parts.append(line)

        def arrive():
            for u in range(k * per, (k + 1) * per):
                for side in range(SIDE):
                    column = (x + side) % SIDE
                    to = pl.ds(u * cap, cap)
                    copy = remote(
                        outgoing.at[pl.ds(0, cap)],
                        tokens.at[y, column, to],
                        out_sent.at[0],
                        out_got.at[u, column],
                        place.plane("y", 1),
                    )
                    guarded(side == 0 and u == home // 2, copy.wait_recv)
            line.open()

        def compute():
            line.arrived()
            if k == 0:
                gather.close()
            values = jnp.concatenate(
                [tokens[i, j, rows, :] for i in range(SIDE) for j in range(SIDE)], axis=1
            )
            both = dot(values, gate_up[...])
            hidden_units = both.shape[1] // 2
            gate = jnp.minimum(both[:, :hidden_units], CLAMP_LIMIT)
            up = jnp.clip(both[:, hidden_units:], -CLAMP_LIMIT, CLAMP_LIMIT)
            act = ((up + 1.0) * gate * jax.nn.sigmoid(SIGMOID_SCALE * gate)).astype(jnp.bfloat16)
            for i in range(SIDE):
                wide_part = dot(act, down[:, i * SIDE * width : (i + 1) * SIDE * width])
                for j in range(SIDE):
                    blocks[k, i, j] = wide_part[:, j * width : (j + 1) * width].astype(jnp.bfloat16)
            line.give()

        def close():
            result[k] = line.total().astype(jnp.bfloat16)
            for u in range(k * per, (k + 1) * per):
                d = order[2 * u] + (x // 2) * (order[2 * u + 1] - order[2 * u])
                source = ((place.z + d) % chips) * CORES + x % 2
                number = (2 * u + x // 2) * 2 + (x % 2 + core) % 2
                piece = pl.ds((u - k * per) * cap, cap)
                for side in range(SIDE):
                    column = (x + side) % SIDE
                    copy = remote(
                        result.at[k, column, piece],
                        back.at[slot_rows(place.sp)],
                        back_sent.at[u, side],
                        back_got.at[number],
                        (source, y * SIDE + column),
                    )
                    apart = side == 0 and u == home // 2
                    guarded(apart, copy.start)
                    waits.append((apart, copy))
                    if apart:

                        @pl.when(inside)
                        def _(piece=piece):
                            back[slot_rows(place.sp), :] = result[k, x, piece, :]

        return [arrive, line.pass_on, compute, line.add, close]

    plans = [steps(k) for k in range(chunks)]
    depth = len(plans[0])
    turns = sorted((k + LAG * n, -n, k) for k in range(chunks) for n in range(depth))
    for _, n, k in turns:
        plans[k][-n]()
    for s in range(chips):
        for other in (0, 1):
            copy = remote(
                outgoing.at[pl.ds(0, cap)],
                back.at[pl.ds(0, cap)],
                out_sent.at[0],
                back_got.at[s * 2 + other],
                place.plane("y", 1),
            )
            guarded(s == home and other == 0, copy.wait_recv)
    combined = state[...] + dot(share[0], back[...]) + dot(share[1], back[...])
    out[...] = combined.astype(jnp.bfloat16)
    for apart, copy in waits:
        guarded(apart, copy.wait_send)
    for copy in gather.started.values():
        copy.wait_send()
    for line in parts:
        for copy in line.started:
            copy.wait_send()
    for copy in rims + tells + answers + shares:
        copy.wait_send()
    for total in totals_of:
        for copy in total.started:
            copy.wait_send()


def layer_call(
    inputs, loose, chips, cap
):
    length, width = inputs[1].shape
    narrow_in = inputs[0]
    narrow_rows, wide_rows, gate_hbm, down_hbm = loose[3], loose[4], loose[5], loose[7]
    devices = chips * CORES
    plane = SIDE * SIDE
    unit = length // 2
    chunks = CHUNKS
    slots = devices * cap
    rows = slots // SIDE
    size = rows // chunks
    features, hidden_units = gate_hbm.shape
    bf16, f32 = jnp.bfloat16, jnp.float32
    vmem, any_ = pl.BlockSpec(memory_space=pltpu.VMEM), pl.BlockSpec(memory_space=pl.ANY)
    dma = pltpu.SemaphoreType.DMA
    return pl.pallas_call(
        functools.partial(layer_kernel, chips, cap, chunks),
        out_shape=jax.ShapeDtypeStruct((length, width), bf16),
        in_specs=[vmem] * 13 + [any_] * 5 + [vmem] * 3 + [any_] * 3,
        out_specs=vmem,
        scratch_shapes=[
            pltpu.VMEM((length, width), bf16),
            pltpu.VMEM((length, width), bf16),
            pltpu.VMEM((length, width), bf16),
            pltpu.VMEM(narrow_rows.shape, bf16),
            pltpu.VMEM(wide_rows.shape, bf16),
            pltpu.VMEM((RIM, narrow_in.shape[1]), bf16),
            pltpu.VMEM((RIM, width), bf16),
            pltpu.VMEM((RIM, width), bf16),
            pltpu.VMEM((RIM, width), bf16),
            pltpu.VMEM((RIM + length, width), f32),
            pltpu.VMEM((devices, STATE_ROWS, width), bf16),
            pltpu.VMEM((devices, STATE_ROWS, width), bf16),
            pltpu.VMEM((devices, STATE_ROWS, width), bf16),
            pltpu.VMEM((devices, STATE_ROWS, width), bf16),
            pltpu.VMEM((2, SIDE, SIDE, unit, width), bf16),
            pltpu.VMEM((2, 2, SIDE, unit // 2, width), bf16),
            pltpu.VMEM((2, 2, SIDE, unit, width), bf16),
            pltpu.VMEM((2, 2, unit // 2, width), bf16),
            pltpu.VMEM((2, 2, unit, width), bf16),
            pltpu.VMEM((1, length), f32),
            pltpu.VMEM((plane, 1, length), f32),
            dma((5,)),
            dma((4,)),
            dma((4,)),
            dma((devices,)),
            dma((devices,)),
            dma((devices,)),
            dma((devices,)),
            dma((2, 8)),
            dma((2, 8)),
            dma((plane,)),
            dma((plane,)),
            pltpu.VMEM((length, width), f32),
            pltpu.VMEM((slots, length), bf16),
            pltpu.VMEM((2, length, slots), bf16),
            pltpu.VMEM((slots, width), bf16),
            pltpu.VMEM((SIDE, SIDE, rows, width), bf16),
            pltpu.VMEM((features, 2 * SIDE * hidden_units), bf16),
            pltpu.VMEM((SIDE * hidden_units, features), bf16),
            pltpu.VMEM((chunks, SIDE, SIDE, size, width), bf16),
            pltpu.VMEM((chunks, 2, SIDE, size // 2, width), bf16),
            pltpu.VMEM((chunks, 2, SIDE, size, width), bf16),
            pltpu.VMEM((chunks, SIDE, size, width), bf16),
            pltpu.VMEM((slots, width), bf16),
            dma((3,)),
            dma((3, 4)),
            dma((3, 4)),
            dma((devices,)),
            dma((chips // 2, SIDE)),
            dma((chunks, 8)),
            dma((chunks, 8)),
            dma((chips // 2, SIDE)),
            dma((devices,)),
        ],
        compiler_params=pltpu.CompilerParams(
            collective_id=0, has_side_effects=True, vmem_limit_bytes=56 * 1024 * 1024
        ),
    )(*inputs, *loose[:5], *inputs_of_routes(loose), *loose[5:8])


def inputs_of_routes(loose):
    return loose[8], loose[8].T, loose[9]


def local(
    resid,
    narrow_head_input,
    wide_head_input,
    key_group_input,
    query_group_input,
    narrow_output_gate,
    wide_output_gate,
    step_input_rows,
    head_decay_logarithm,
    position_log_decay,
    direct_input_weight,
    narrow_conv_taps,
    wide_conv_taps,
    key_conv_taps,
    query_conv_taps,
    narrow_norm_gain,
    wide_norm_gain,
    narrow_output_rows,
    wide_output_rows,
    feedforward_norm_gain,
    routes,
    routing_weight_values,
    expert_gate_matrix,
    expert_up_matrix,
    expert_down_matrix,
):
    chips = lax.axis_size(SP) // CORES
    steps = jax.nn.softplus(step_input_rows[:, :, 0].astype(jnp.float32))
    decays = -jnp.exp(head_decay_logarithm[:, 0])[None, :] * steps + position_log_decay[:, :, 0]
    direct = jnp.broadcast_to(direct_input_weight[:, 0][None, :], steps.shape)
    columns = jnp.concatenate([steps, decays, direct, jnp.zeros_like(direct)], axis=1)
    length, picks = routes.shape
    inputs = (
        narrow_head_input,
        wide_head_input,
        narrow_output_gate,
        wide_output_gate,
        columns,
        columns.T,
        narrow_conv_taps,
        wide_conv_taps,
        key_conv_taps,
        query_conv_taps,
        narrow_norm_gain.reshape(1, -1),
        wide_norm_gain.reshape(1, -1),
        feedforward_norm_gain.reshape(1, -1),
    )
    loose = (
        key_group_input,
        query_group_input,
        resid,
        narrow_output_rows,
        wide_output_rows,
        expert_gate_matrix[0],
        expert_up_matrix[0],
        expert_down_matrix[0],
        routes,
        routing_weight_values,
    )
    return layer_call(inputs, loose, chips, 4 * length * picks // (3 * chips * CORES))


def solution(mesh):
    return jax.shard_map(
        local,
        mesh=mesh,
        in_specs=(
            P(SP, None),
            P(SP, "tp"),
            P(SP, "tp"),
            P(SP, None),
            P(SP, None),
            P(SP, "tp"),
            P(SP, "tp"),
            P(SP, None, "tp"),
            P(None, "tp"),
            P(SP, None, "tp"),
            P(None, "tp"),
            P(None, "tp"),
            P(None, "tp"),
            P(),
            P(),
            P("tp"),
            P("tp"),
            P("tp", None),
            P("tp", None),
            P(),
            P(SP, None),
            P(SP, None),
            P(SP, None, "tp"),
            P(SP, None, "tp"),
            P(SP, "tp", None),
        ),
        out_specs=P(SP, "tp"),
        check_vma=False,
    )
```

```python
import functools

import jax
import jax.numpy as jnp
from jax import lax
from jax.experimental import pallas as pl
from jax.experimental.pallas import tpu as pltpu
from jax.sharding import PartitionSpec as P

HEADS = 16
NARROW_HEAD_DIM = 64
WIDE_HEAD_DIM = 128
GROUPS = 4
CONV = 4
SP = "sp"


NORM_EPS = 1e-06
CLAMP_LIMIT = 7.0
SIGMOID_SCALE = 1.702
FULL_PRECISION = lax.Precision.HIGHEST


MESH = pl.DeviceIdType.MESH
CORES = 2
SIDE = 4
LAG = 2
CHUNKS = 4


def remote(src, dst, send_sem, recv_sem, device):
    return pltpu.make_async_remote_copy(
        src_ref=src,
        dst_ref=dst,
        send_sem=send_sem,
        recv_sem=recv_sem,
        device_id=device,
        device_id_type=MESH,
    )


class Place:
    def __init__(self, chips):
        self.chips = chips
        self.sp = lax.axis_index("sp")
        self.tp = lax.axis_index("tp")
        self.z, self.core = self.sp // CORES, self.sp % CORES
        self.at = {"y": self.tp // SIDE, "x": self.tp % SIDE}

        self.at["a"] = self.pick(self.core, self.at["x"], self.at["y"])
        self.at["b"] = self.pick(self.core, self.at["y"], self.at["x"])

    def pick(self, core, first, second):
        return first + core * (second - first)

    def flat(self, core, a, b):
        return b * (SIDE - (SIDE - 1) * core) + a * (1 + (SIDE - 1) * core)

    def plane(self, axis, step):
        if axis == "a":
            return (self.sp, self.flat(self.core, self.index("a", step), self.at["b"]))
        if axis == "b":
            return (self.sp, self.flat(self.core, self.at["a"], self.index("b", step)))
        moved = (self.at[axis] + step + SIDE) % SIDE
        if axis == "x":
            return (self.sp, self.at["y"] * SIDE + moved)
        return (self.sp, moved * SIDE + self.at["x"])

    def index(self, axis, step):
        return (self.at[axis] + step + SIDE) % SIDE

    def along(self, step, core):
        return (((self.z + step + self.chips) % self.chips) * CORES + core, self.tp)


def chip_order(chips):
    if chips == 16:
        return [1, 15, 3, 13, 5, 11, 7, 9, 8, 6, 10, 4, 12, 2, 14, 0]
    return [d % chips for d in range(1, chips + 1)]


def greet(place):
    barrier = pltpu.get_barrier_semaphore()
    count = 0
    devices = place.chips * CORES

    def tell(sp, a, b):
        device = (sp, place.flat(place.core, a, b))
        pl.semaphore_signal(barrier, inc=1, device_id=device, device_id_type=MESH)

    own_a, own_b = place.at["a"], place.at["b"]
    for step in range(devices):
        for side in range(SIDE):
            if step or side:
                tell((place.sp + step) % devices, (own_a + side) % SIDE, own_b)
                count += 1
    for side in range(1, SIDE):
        for step in range(place.chips):
            other = ((place.z + step) % place.chips) * CORES + 1 - place.core
            tell(other, own_a, (own_b + side) % SIDE)
            count += 1
        for step in range(SIDE):
            tell(place.sp, (own_a + step) % SIDE, (own_b + side) % SIDE)
            count += 1
    return barrier, count


class Gather:
    def __init__(self, place, gate_up, down, sent, got):
        self.place, self.gate_up, self.down = place, gate_up, down
        self.sent, self.got, self.started, self.loads = sent, got, {}, []
        self.width = down.shape[0] // SIDE

    def piece(self, kind, step, part=None):
        index = self.place.index("a", step)
        if kind == 2:
            ref = self.down.at[pl.ds(pl.multiple_of(index * self.width, self.width), self.width)]
        else:
            start = pl.multiple_of(index * self.width + kind * SIDE * self.width, self.width)
            ref = self.gate_up.at[:, pl.ds(start, self.width)]
        if part is None:
            return ref
        size = ref.shape[0] // 2
        return ref.at[pl.ds(part * size, size)]

    def load(self, gate_hbm, up_hbm, down_hbm, sem):
        for kind, src in enumerate((gate_hbm, up_hbm, down_hbm)):
            dst = self.piece(kind, 0)
            copies = []
            for i in range(SIDE):
                for j in range(SIDE):
                    number = i * SIDE + j
                    there = self.place.flat(self.place.core, j, i) * self.width
                    there = pl.ds(pl.multiple_of(there, self.width), self.width)
                    here = pl.ds(number * self.width, self.width)
                    if kind == 2:
                        copy = pltpu.make_async_copy(
                            src.at[:, there], dst.at[:, here], sem.at[kind, number]
                        )
                    else:
                        copy = pltpu.make_async_copy(
                            src.at[there], dst.at[here], sem.at[kind, number]
                        )
                    copy.start()
                    copies.append(copy)
            self.loads.append(copies)

    def send(self, ref, kind, number, step):
        copy = remote(
            ref, ref, self.sent.at[kind, number], self.got.at[kind, number],
            self.place.plane("a", step),
        )
        copy.start()
        self.started[(kind, number)] = copy

    def open(self):
        for kind in range(3):
            for copy in self.loads[kind]:
                copy.wait()
            self.send(self.piece(kind, 0), kind, 0, 1)
            self.send(self.piece(kind, 0), kind, 1, SIDE - 1)

    def pass_on(self, kind):
        self.started[(kind, 0)].wait_recv()
        self.send(self.piece(kind, SIDE - 1, 0), kind, 2, 1)
        self.started[(kind, 1)].wait_recv()
        self.send(self.piece(kind, 1, 1), kind, 3, SIDE - 1)

    def close(self):
        for kind in range(3):
            self.started[(kind, 2)].wait_recv()
            self.started[(kind, 3)].wait_recv()


class Line:
    def __init__(self, place, tokens, blocks, relay, sums, sent, got):
        self.place, self.tokens, self.blocks = place, tokens, blocks
        self.relay, self.sums, self.sent, self.got = relay, sums, sent, got
        self.started = []
        rows = tokens.shape[2]
        self.low, self.high = pl.ds(0, rows // 2), pl.ds(rows // 2, rows // 2)

    def send(self, src, dst, step):
        number = len(self.started)
        copy = remote(
            src, dst, self.sent.at[number], self.got.at[number], self.place.plane("b", step)
        )
        copy.start()
        self.started.append(copy)

    def open(self):
        own = self.tokens.at[self.place.at["b"]]
        self.send(own, own, 1)
        self.send(own, own, SIDE - 1)

    def pass_on(self):
        for side, step in ((0, SIDE - 1), (1, 1)):
            self.started[side].wait_recv()
            part = self.low if side == 0 else self.high
            ref = self.tokens.at[self.place.index("b", step)].at[:, part]
            self.send(ref, ref, SIDE - step)

    def arrived(self):
        self.started[2].wait_recv()
        self.started[3].wait_recv()

    def give(self):
        far = self.blocks.at[self.place.index("b", 2)]
        self.send(far.at[:, self.low], self.relay.at[0], 1)
        self.send(far.at[:, self.high], self.relay.at[1], SIDE - 1)

    def add(self):
        for side, step in ((0, 1), (1, SIDE - 1)):
            part = self.low if side == 0 else self.high
            self.started[4 + side].wait_recv()
            near = self.blocks.at[self.place.index("b", step)]
            piece = near.at[:, part]
            piece[...] = (
                piece[...].astype(jnp.float32) + self.relay[side].astype(jnp.float32)
            ).astype(jnp.bfloat16)
            self.send(near, self.sums.at[side], step)

    def total(self):
        self.started[6].wait_recv()
        self.started[7].wait_recv()
        return (
            self.blocks[self.place.at["b"]].astype(jnp.float32)
            + self.sums[0].astype(jnp.float32)
            + self.sums[1].astype(jnp.float32)
        )


def chunk_of(ref, axis, index):
    return ref.at[index] if axis == "y" else ref.at[:, index]


class Summer:
    def __init__(self, place, first, blocks, relay, sums, half, last, sent, got):
        self.place, self.first, self.second = place, first, "y" if first == "x" else "x"
        self.blocks, self.relay, self.sums = blocks, relay, sums
        self.half, self.last, self.sent, self.got = half, last, sent, got
        self.started = []
        rows = blocks.shape[2]
        self.low, self.high = pl.ds(0, rows // 2), pl.ds(rows // 2, rows // 2)

    def send(self, src, dst, axis, step, number):
        copy = remote(
            src, dst, self.sent.at[number], self.got.at[number], self.place.plane(axis, step)
        )
        copy.start()
        self.started.append(copy)

    def open(self):
        far = chunk_of(self.blocks, self.first, self.place.index(self.first, 2))
        self.send(far.at[:, self.low], self.relay.at[0], self.first, 1, 0)
        self.send(far.at[:, self.high], self.relay.at[1], self.first, SIDE - 1, 1)

    def pass_on(self):
        for side, step in ((0, 1), (1, SIDE - 1)):
            part = self.low if side == 0 else self.high
            self.started[side].wait_recv()
            near = chunk_of(self.blocks, self.first, self.place.index(self.first, step))
            piece = near.at[:, part]
            piece[...] = (
                piece[...].astype(jnp.float32) + self.relay[side].astype(jnp.float32)
            ).astype(jnp.bfloat16)
            self.send(near, self.sums.at[side], self.first, step, 2 + side)

    def turn(self):
        self.started[2].wait_recv()
        self.started[3].wait_recv()
        own = chunk_of(self.blocks, self.first, self.place.at[self.first])
        own[...] = (
            own[...].astype(jnp.float32)
            + self.sums[0].astype(jnp.float32)
            + self.sums[1].astype(jnp.float32)
        ).astype(jnp.bfloat16)
        far = own.at[self.place.index(self.second, 2)]
        self.send(far.at[self.low], self.half.at[0], self.second, 1, 4)
        self.send(far.at[self.high], self.half.at[1], self.second, SIDE - 1, 5)

    def pass_again(self):
        own = chunk_of(self.blocks, self.first, self.place.at[self.first])
        for side, step in ((0, 1), (1, SIDE - 1)):
            part = self.low if side == 0 else self.high
            self.started[4 + side].wait_recv()
            near = own.at[self.place.index(self.second, step)]
            piece = near.at[part]
            piece[...] = (
                piece[...].astype(jnp.float32) + self.half[side].astype(jnp.float32)
            ).astype(jnp.bfloat16)
            self.send(near, self.last.at[side], self.second, step, 6 + side)

    def close(self):
        self.started[6].wait_recv()
        self.started[7].wait_recv()
        own = chunk_of(self.blocks, self.first, self.place.at[self.first])
        mine = own.at[self.place.at[self.second]]
        return (
            mine[...].astype(jnp.float32)
            + self.last[0].astype(jnp.float32)
            + self.last[1].astype(jnp.float32)
        )


def iota(shape, dim):
    return lax.broadcasted_iota(jnp.int32, shape, dim)


def ones_where(mask):
    return jnp.where(mask, 1.0, 0.0).astype(jnp.bfloat16)


def dot(a, b):
    return jnp.dot(a, b, preferred_element_type=jnp.float32)


def in_two(x):
    high = x.astype(jnp.bfloat16)
    return high, (x - high.astype(jnp.float32)).astype(jnp.bfloat16)


def routing_tables(experts, cap, routes, routes_turned, weights, choice, share):
    tokens, picks = routes.shape
    slots = experts * cap
    shift = cap.bit_length() - 1
    named = routes[...]
    turned = routes_turned[...]
    amount = weights[...]
    lines = iota((experts, tokens), 0)
    there = turned[0:1, :] == lines
    for k in range(1, picks):
        there = there | (turned[k : k + 1, :] == lines)
    before = ones_where(iota((tokens, tokens), 0) < iota((tokens, tokens), 1))
    rank = jnp.where(there, dot(ones_where(there), before), -1.0).astype(jnp.bfloat16)
    spread = ones_where((iota((slots, experts), 0) >> shift) == iota((slots, experts), 1))
    wide = dot(spread, rank)
    number = (iota((slots, tokens), 0) & (cap - 1)).astype(jnp.float32)
    choice[...] = ones_where(wide == number)

    columns = iota((tokens, experts), 1)
    hit = named[:, 0:1] == columns
    weight = jnp.where(hit, amount[:, 0:1], 0.0)
    for k in range(1, picks):
        now = named[:, k : k + 1] == columns
        hit = hit | now
        weight = weight + jnp.where(now, amount[:, k : k + 1], 0.0)
    after = ones_where(iota((tokens, tokens), 1) < iota((tokens, tokens), 0))
    rank = jnp.where(hit, dot(after, ones_where(hit)), -1.0).astype(jnp.bfloat16)
    spread = ones_where(iota((experts, slots), 0) == (iota((experts, slots), 1) >> shift))
    wide = dot(rank, spread)
    number = (iota((tokens, slots), 1) & (cap - 1)).astype(jnp.float32)
    mine = wide == number
    for part, piece in enumerate(in_two(weight)):
        share[part] = jnp.where(mine, dot(piece, spread), 0.0).astype(jnp.bfloat16)


def fine_dot(a, b, dims=(((1,), (0,)), ((), ()))):
    return lax.dot_general(
        a, b, dims, precision=FULL_PRECISION, preferred_element_type=jnp.float32
    )


def quick_dot(a, b, dims=(((1,), (0,)), ((), ()))):
    a, b = a.astype(jnp.bfloat16), b.astype(jnp.bfloat16)
    return lax.dot_general(a, b, dims, preferred_element_type=jnp.float32)


def in_three(x):
    high, rest = x.astype(jnp.bfloat16), None
    rest = x - high.astype(jnp.float32)
    middle = rest.astype(jnp.bfloat16)
    low = (rest - middle.astype(jnp.float32)).astype(jnp.bfloat16)
    return high, middle, low


def silu(x):
    return x * jax.nn.sigmoid(x)


RIM = 16
STATE_ROWS = 8


def layer_kernel(
    chips,
    cap,
    chunks,
    narrow_in,
    wide_in,
    narrow_gate,
    wide_gate,
    columns,
    lines,
    narrow_taps,
    wide_taps,
    key_taps,
    query_taps,
    narrow_gain,
    wide_gain,
    last_gain,
    key_hbm,
    query_hbm,
    resid_hbm,
    narrow_rows_hbm,
    wide_rows_hbm,
    routes,
    routes_turned,
    weights,
    gate_hbm,
    up_hbm,
    down_hbm,
    out,
    keys,
    queries,
    resid,
    narrow_rows,
    wide_rows,
    narrow_rim,
    wide_rim,
    key_rim,
    query_rim,
    padded,
    told,
    heard,
    answer,
    carried,
    partial,
    relay,
    sums,
    half,
    last,
    squares_out,
    squares,
    load_sem,
    rim_sent,
    rim_got,
    told_sent,
    told_got,
    answer_sent,
    answer_got,
    sum_sent,
    sum_got,
    square_sent,
    square_got,
    state,
    choice,
    share,
    outgoing,
    tokens,
    gate_up,
    down,
    blocks,
    line_relay,
    line_sums,
    result,
    back,
    weight_load,
    weight_sent,
    weight_got,
    out_sent,
    out_got,
    line_sent,
    line_got,
    back_sent,
    back_got,
):
    place = Place(chips)
    devices = chips * CORES
    length = narrow_in.shape[0]
    width = keys.shape[1]
    plane = SIDE * SIDE
    barrier, count = greet(place)
    group = pl.multiple_of((place.tp // (HEADS // GROUPS)) * width, width)
    mine = pl.ds(pl.multiple_of(place.tp * width, width), width)
    pairs = (
        (key_hbm.at[:, pl.ds(group, width)], keys),
        (query_hbm.at[:, pl.ds(group, width)], queries),
        (resid_hbm.at[:, mine], resid),
        (narrow_rows_hbm, narrow_rows),
        (wide_rows_hbm, wide_rows),
    )
    gather = Gather(place, gate_up, down, weight_sent, weight_got)
    gather.load(gate_hbm, up_hbm, down_hbm, weight_load)
    loads = [pltpu.make_async_copy(src, dst, load_sem.at[k]) for k, (src, dst) in enumerate(pairs)]
    for load in loads:
        load.start()

    upper = ones_where(iota((length, length), 0) <= iota((length, length), 1))
    causal = iota((length, length), 0) >= iota((length, length), 1)
    lower = ones_where(causal)
    tall, flat = columns[...], lines[...]
    tall_sum = sum(dot(lower, piece) for piece in in_three(tall))
    flat_sum = sum(dot(piece, upper) for piece in in_three(flat))
    decay, tails, totals, steps = [], [], [], []
    for kind in (0, 1):
        down_column = tall_sum[:, 2 + kind : 3 + kind]
        across = flat_sum[2 + kind : 3 + kind, :]
        decay.append(jnp.exp(jnp.where(causal, down_column - across, -1e30)))
        total = down_column[length - 1 : length, :]
        totals.append(total)
        tails.append(jnp.exp(total - down_column))
        steps.append(tall[:, kind : kind + 1])
    fades = [jnp.exp(tall_sum[:, 2 + kind : 3 + kind]) for kind in (0, 1)]
    rows = iota((width, devices * STATE_ROWS), 0)
    spots = iota((width, devices * STATE_ROWS), 1)
    per = STATE_ROWS // 2
    owner_row = (spots >> 3) * per + (spots & (per - 1))
    wide_spread = jnp.where((owner_row == rows) & ((spots & 7) < per), 1.0, 0.0)
    narrow_spread = jnp.where((owner_row == rows) & ((spots & 7) >= per), 1.0, 0.0)

    loads[0].wait()
    loads[1].wait()
    pl.semaphore_wait(barrier, count)
    gather.open()
    following = ((place.sp + 1) % devices, place.tp)
    rims = []
    tail = pl.ds(length - RIM, RIM)
    for k, (src, dst) in enumerate(
        ((narrow_in, narrow_rim), (wide_in, wide_rim), (keys, key_rim), (queries, query_rim))
    ):
        copy = remote(src.at[tail], dst, rim_sent.at[k], rim_got.at[k], following)
        copy.start()
        rims.append(copy)
    for copy in rims:
        copy.wait_recv()

    inner = place.sp > 0

    def mixed_rows(values, rim, taps):
        size = values.shape[1]
        before = jnp.where(inner, rim[...].astype(jnp.float32), 0.0)
        padded[0:RIM, 0:size] = before
        padded[RIM : RIM + length, 0:size] = values[...].astype(jnp.float32)
        total = jnp.zeros((length, size), jnp.float32)
        for k in range(CONV):
            start = RIM - CONV + 1 + k
            total = total + taps[k : k + 1, :] * padded[start : start + length, 0:size]
        return silu(total)

    key = mixed_rows(keys, key_rim, key_taps[:, pl.ds(group, width)])
    query = mixed_rows(queries, query_rim, query_taps[:, pl.ds(group, width)])
    narrow_mix = mixed_rows(narrow_in, narrow_rim, narrow_taps[...])
    wide_mix = mixed_rows(wide_in, wide_rim, wide_taps[...])
    narrow_size = narrow_mix.shape[1]
    narrow_value, wide_value = narrow_mix * steps[0], wide_mix * steps[1]

    turned = (((0,), (0,)), ((), ()))
    wide_keys = quick_dot(key, wide_spread)
    narrow_keys = quick_dot(key, narrow_spread)
    wide_state = quick_dot(wide_keys, wide_value * tails[1], turned)
    narrow_state = quick_dot(
        narrow_keys,
        jnp.concatenate(
            [narrow_value * tails[0], jnp.zeros((length, width - narrow_size), jnp.float32)], axis=1
        ),
        turned,
    )
    tile = iota((devices * STATE_ROWS, width), 0) & 7
    lane = iota((devices * STATE_ROWS, width), 1)
    spare = jnp.where(lane < (narrow_size + width) // 2, totals[1], totals[0])
    message = wide_state + narrow_state
    message = jnp.where((tile >= per) & (lane >= narrow_size), spare, message)
    told[...] = message.reshape(devices, STATE_ROWS, width).astype(jnp.bfloat16)

    def exchange(src, dst, sent, got):
        copies = []
        dst[place.sp] = src[place.sp]
        for step in range(1, devices):
            other = (place.sp + step) % devices
            copy = remote(
                src.at[other], dst.at[place.sp], sent.at[step], got.at[step], (other, place.tp)
            )
            copy.start()
            copies.append(copy)
        return copies

    tells = exchange(told, heard, told_sent, told_got)

    scores = quick_dot(query, key, (((1,), (1,)), ((), ())))
    narrow_inside = quick_dot(scores * decay[0], narrow_value)
    wide_inside = quick_dot(scores * decay[1], wide_value)
    wide_query = quick_dot(query * fades[1], wide_spread)
    narrow_query = quick_dot(query * fades[0], narrow_spread)
    narrow_open, wide_open = silu(narrow_gate[...].astype(jnp.float32)), silu(
        wide_gate[...].astype(jnp.float32)
    )

    for copy in tells:
        copy.wait_recv()
    gather.pass_on(0)
    running = jnp.zeros((STATE_ROWS, width), jnp.float32)
    upper_rows = iota((STATE_ROWS, width), 0) < per
    for source in range(devices):
        answer[source] = running.astype(jnp.bfloat16)
        piece = heard[source].astype(jnp.float32)
        wide_total = piece[per : per + 1, narrow_size : narrow_size + 1]
        middle = (narrow_size + width) // 2
        narrow_total = piece[per : per + 1, middle : middle + 1]
        factor = jnp.exp(jnp.where(upper_rows, wide_total, narrow_total))
        running = factor * running + piece
    answers = exchange(answer, carried, answer_sent, answer_got)
    routing_tables(devices, cap, routes, routes_turned, weights, choice, share)

    for load in loads[2:]:
        load.wait()
    for copy in answers:
        copy.wait_recv()
    gather.pass_on(1)
    entering = carried[...].astype(jnp.float32).reshape(devices * STATE_ROWS, width)

    def head(inside, asked, size, kind, mix, opened, gain):
        result = inside + quick_dot(asked, entering)[:, :size]
        result = (result + tall[:, 4 + kind : 5 + kind] * mix) * opened
        mean = jnp.sum(result * result, axis=-1, keepdims=True) * (1.0 / size)
        return (result * lax.rsqrt(mean + NORM_EPS) * gain[...]).astype(jnp.bfloat16)

    narrow = head(narrow_inside, narrow_query, narrow_size, 0, narrow_mix, narrow_open, narrow_gain)
    wide = head(wide_inside, wide_query, width, 1, wide_mix, wide_open, wide_gain)

    totals_of = [
        Summer(
            place, first, partial.at[u], relay.at[u], sums.at[u], half.at[u], last.at[u],
            sum_sent.at[u], sum_got.at[u],
        )
        for u, first in ((0, "x"), (1, "y"))
    ]
    unit = length // 2
    for i in range(SIDE):
        part = pl.ds(i * SIDE * width, SIDE * width)
        product = dot(narrow, narrow_rows[:, part]) + dot(wide, wide_rows[:, part])
        product = product.astype(jnp.bfloat16)
        for j in range(SIDE):
            for u in (0, 1):
                partial[u, i, j] = product[u * unit : (u + 1) * unit, j * width : (j + 1) * width]
    for move in ("open", "pass_on", "turn", "pass_again"):
        for total in totals_of:
            getattr(total, move)()
    mixed = jnp.concatenate([total.close() for total in totals_of], axis=0)
    hidden = resid[...].astype(jnp.float32) + mixed
    ones = jnp.ones((8, width), jnp.float32)
    own = fine_dot(ones, hidden * hidden, (((1,), (1,)), ((), ())))[0:1, :]
    gather.pass_on(2)
    squares_out[...] = own
    squares[place.tp] = own
    shares = []
    for step in range(1, plane):
        other = (place.tp + step) % plane
        copy = remote(
            squares_out, squares.at[place.tp], square_sent.at[step], square_got.at[step],
            (place.sp, other),
        )
        copy.start()
        shares.append(copy)
    for copy in shares:
        copy.wait_recv()
    whole = squares[0]
    for k in range(1, plane):
        whole = whole + squares[k]
    diagonal = iota((length, length), 0) == iota((length, length), 1)
    mean = jnp.sum(jnp.where(diagonal, whole, 0.0), axis=1, keepdims=True) * (1.0 / (plane * width))
    state[...] = hidden
    normed = (hidden * lax.rsqrt(mean + NORM_EPS) * last_gain[:, mine]).astype(jnp.bfloat16)

    outgoing[...] = dot(choice[...], normed).astype(jnp.bfloat16)
    order = chip_order(chips)
    spot = {d: k for k, d in enumerate(order)}
    row, column_own, core = place.at["b"], place.at["a"], place.core
    home = spot[0]
    inside = column_own == 2 * (home % 2) + core
    outside = column_own != 2 * (home % 2) + core
    waits = []

    def slot_rows(number):
        return pl.ds(pl.multiple_of(number * cap, cap), cap)

    def guarded(apart, act):
        if apart:
            pl.when(outside)(act)
        else:
            act()

    for s, d in enumerate(order):
        for other in (0, 1):
            aim = core if other == 0 else 1 - core
            target = ((place.z + chips - d) % chips) * CORES + aim
            across = place.pick(aim, place.at["x"], place.at["y"])
            along = place.pick(aim, place.at["y"], place.at["x"])
            device = (target, place.flat(aim, 2 * (s % 2) + core, along))
            rows = slot_rows(target)
            to = pl.ds((s // 2) * cap, cap)
            copy = remote(
                outgoing.at[rows],
                tokens.at[along, across, to],
                out_sent.at[s * 2 + other],
                out_got.at[s // 2, across],
                device,
            )
            apart = d == 0 and other == 0
            guarded(apart, copy.start)
            waits.append((apart, copy))
            if apart:

                @pl.when(inside)
                def _(rows=rows, to=to):
                    tokens[row, column_own, to, :] = outgoing[rows, :]

    units = chips // 2
    per = units // chunks
    size = per * cap
    parts = []

    def steps(k):
        rows = pl.ds(k * size, size)
        line = Line(
            place, tokens.at[:, :, rows], blocks.at[k], line_relay.at[k], line_sums.at[k],
            line_sent.at[k], line_got.at[k],
        )
        parts.append(line)

        def arrive():
            for u in range(k * per, (k + 1) * per):
                for side in range(SIDE):
                    column = (column_own + side) % SIDE
                    to = pl.ds(u * cap, cap)
                    copy = remote(
                        outgoing.at[pl.ds(0, cap)],
                        tokens.at[row, column, to],
                        out_sent.at[0],
                        out_got.at[u, column],
                        place.plane("b", 1),
                    )
                    guarded(side == 0 and u == home // 2, copy.wait_recv)
            line.open()

        def compute():
            line.arrived()
            if k == 0:
                gather.close()
            values = jnp.concatenate(
                [tokens[i, j, rows, :] for i in range(SIDE) for j in range(SIDE)], axis=1
            )
            both = dot(values, gate_up[...])
            hidden_units = both.shape[1] // 2
            gate = jnp.minimum(both[:, :hidden_units], CLAMP_LIMIT)
            up = jnp.clip(both[:, hidden_units:], -CLAMP_LIMIT, CLAMP_LIMIT)
            act = ((up + 1.0) * gate * jax.nn.sigmoid(SIGMOID_SCALE * gate)).astype(jnp.bfloat16)
            for i in range(SIDE):
                wide_part = dot(act, down[:, i * SIDE * width : (i + 1) * SIDE * width])
                for j in range(SIDE):
                    blocks[k, i, j] = wide_part[:, j * width : (j + 1) * width].astype(jnp.bfloat16)
            line.give()

        def close():
            result[k] = line.total().astype(jnp.bfloat16)
            for u in range(k * per, (k + 1) * per):
                d = order[2 * u] + (column_own // 2) * (order[2 * u + 1] - order[2 * u])
                source = ((place.z + d) % chips) * CORES + column_own % 2
                number = (2 * u + column_own // 2) * 2 + (column_own % 2 + core) % 2
                piece = pl.ds((u - k * per) * cap, cap)
                for side in range(SIDE):
                    column = (column_own + side) % SIDE
                    copy = remote(
                        result.at[k, column, piece],
                        back.at[slot_rows(place.sp)],
                        back_sent.at[u, side],
                        back_got.at[number],
                        (source, place.flat(core, column, row)),
                    )
                    apart = side == 0 and u == home // 2
                    guarded(apart, copy.start)
                    waits.append((apart, copy))
                    if apart:

                        @pl.when(inside)
                        def _(piece=piece):
                            back[slot_rows(place.sp), :] = result[k, column_own, piece, :]

        return [arrive, line.pass_on, compute, line.add, close]

    plans = [steps(k) for k in range(chunks)]
    depth = len(plans[0])
    turns = sorted((k + LAG * n, -n, k) for k in range(chunks) for n in range(depth))
    for _, n, k in turns:
        plans[k][-n]()
    for s in range(chips):
        for other in (0, 1):
            copy = remote(
                outgoing.at[pl.ds(0, cap)],
                back.at[pl.ds(0, cap)],
                out_sent.at[0],
                back_got.at[s * 2 + other],
                place.plane("b", 1),
            )
            guarded(s == home and other == 0, copy.wait_recv)
    combined = state[...] + dot(share[0], back[...]) + dot(share[1], back[...])
    out[...] = combined.astype(jnp.bfloat16)
    for apart, copy in waits:
        guarded(apart, copy.wait_send)
    for copy in gather.started.values():
        copy.wait_send()
    for line in parts:
        for copy in line.started:
            copy.wait_send()
    for copy in rims + tells + answers + shares:
        copy.wait_send()
    for total in totals_of:
        for copy in total.started:
            copy.wait_send()


def layer_call(
    inputs, loose, chips, cap
):
    length, width = inputs[1].shape
    narrow_in = inputs[0]
    narrow_rows, wide_rows, gate_hbm, down_hbm = loose[3], loose[4], loose[5], loose[7]
    devices = chips * CORES
    plane = SIDE * SIDE
    unit = length // 2
    chunks = CHUNKS
    slots = devices * cap
    rows = slots // SIDE
    size = rows // chunks
    features, hidden_units = gate_hbm.shape
    bf16, f32 = jnp.bfloat16, jnp.float32
    vmem, any_ = pl.BlockSpec(memory_space=pltpu.VMEM), pl.BlockSpec(memory_space=pl.ANY)
    dma = pltpu.SemaphoreType.DMA
    return pl.pallas_call(
        functools.partial(layer_kernel, chips, cap, chunks),
        out_shape=jax.ShapeDtypeStruct((length, width), bf16),
        in_specs=[vmem] * 13 + [any_] * 5 + [vmem] * 3 + [any_] * 3,
        out_specs=vmem,
        scratch_shapes=[
            pltpu.VMEM((length, width), bf16),
            pltpu.VMEM((length, width), bf16),
            pltpu.VMEM((length, width), bf16),
            pltpu.VMEM(narrow_rows.shape, bf16),
            pltpu.VMEM(wide_rows.shape, bf16),
            pltpu.VMEM((RIM, narrow_in.shape[1]), bf16),
            pltpu.VMEM((RIM, width), bf16),
            pltpu.VMEM((RIM, width), bf16),
            pltpu.VMEM((RIM, width), bf16),
            pltpu.VMEM((RIM + length, width), f32),
            pltpu.VMEM((devices, STATE_ROWS, width), bf16),
            pltpu.VMEM((devices, STATE_ROWS, width), bf16),
            pltpu.VMEM((devices, STATE_ROWS, width), bf16),
            pltpu.VMEM((devices, STATE_ROWS, width), bf16),
            pltpu.VMEM((2, SIDE, SIDE, unit, width), bf16),
            pltpu.VMEM((2, 2, SIDE, unit // 2, width), bf16),
            pltpu.VMEM((2, 2, SIDE, unit, width), bf16),
            pltpu.VMEM((2, 2, unit // 2, width), bf16),
            pltpu.VMEM((2, 2, unit, width), bf16),
            pltpu.VMEM((1, length), f32),
            pltpu.VMEM((plane, 1, length), f32),
            dma((5,)),
            dma((4,)),
            dma((4,)),
            dma((devices,)),
            dma((devices,)),
            dma((devices,)),
            dma((devices,)),
            dma((2, 8)),
            dma((2, 8)),
            dma((plane,)),
            dma((plane,)),
            pltpu.VMEM((length, width), f32),
            pltpu.VMEM((slots, length), bf16),
            pltpu.VMEM((2, length, slots), bf16),
            pltpu.VMEM((slots, width), bf16),
            pltpu.VMEM((SIDE, SIDE, rows, width), bf16),
            pltpu.VMEM((features, 2 * SIDE * hidden_units), bf16),
            pltpu.VMEM((SIDE * hidden_units, features), bf16),
            pltpu.VMEM((chunks, SIDE, SIDE, size, width), bf16),
            pltpu.VMEM((chunks, 2, SIDE, size // 2, width), bf16),
            pltpu.VMEM((chunks, 2, SIDE, size, width), bf16),
            pltpu.VMEM((chunks, SIDE, size, width), bf16),
            pltpu.VMEM((slots, width), bf16),
            dma((3, SIDE * SIDE)),
            dma((3, 4)),
            dma((3, 4)),
            dma((devices,)),
            dma((chips // 2, SIDE)),
            dma((chunks, 8)),
            dma((chunks, 8)),
            dma((chips // 2, SIDE)),
            dma((devices,)),
        ],
        compiler_params=pltpu.CompilerParams(
            collective_id=0, has_side_effects=True, vmem_limit_bytes=56 * 1024 * 1024
        ),
    )(*inputs, *loose[:5], *inputs_of_routes(loose), *loose[5:8])


def inputs_of_routes(loose):
    return loose[8], loose[8].T, loose[9]


def local(
    resid,
    narrow_head_input,
    wide_head_input,
    key_group_input,
    query_group_input,
    narrow_output_gate,
    wide_output_gate,
    step_input_rows,
    head_decay_logarithm,
    position_log_decay,
    direct_input_weight,
    narrow_conv_taps,
    wide_conv_taps,
    key_conv_taps,
    query_conv_taps,
    narrow_norm_gain,
    wide_norm_gain,
    narrow_output_rows,
    wide_output_rows,
    feedforward_norm_gain,
    routes,
    routing_weight_values,
    expert_gate_matrix,
    expert_up_matrix,
    expert_down_matrix,
):
    chips = lax.axis_size(SP) // CORES
    steps = jax.nn.softplus(step_input_rows[:, :, 0].astype(jnp.float32))
    decays = -jnp.exp(head_decay_logarithm[:, 0])[None, :] * steps + position_log_decay[:, :, 0]
    direct = jnp.broadcast_to(direct_input_weight[:, 0][None, :], steps.shape)
    columns = jnp.concatenate([steps, decays, direct, jnp.zeros_like(direct)], axis=1)
    length, picks = routes.shape
    inputs = (
        narrow_head_input,
        wide_head_input,
        narrow_output_gate,
        wide_output_gate,
        columns,
        columns.T,
        narrow_conv_taps,
        wide_conv_taps,
        key_conv_taps,
        query_conv_taps,
        narrow_norm_gain.reshape(1, -1),
        wide_norm_gain.reshape(1, -1),
        feedforward_norm_gain.reshape(1, -1),
    )
    loose = (
        key_group_input,
        query_group_input,
        resid,
        narrow_output_rows,
        wide_output_rows,
        expert_gate_matrix[0],
        expert_up_matrix[0],
        expert_down_matrix[0],
        routes,
        routing_weight_values,
    )
    return layer_call(inputs, loose, chips, 4 * length * picks // (3 * chips * CORES))


def solution(mesh):
    return jax.shard_map(
        local,
        mesh=mesh,
        in_specs=(
            P(SP, None),
            P(SP, "tp"),
            P(SP, "tp"),
            P(SP, None),
            P(SP, None),
            P(SP, "tp"),
            P(SP, "tp"),
            P(SP, None, "tp"),
            P(None, "tp"),
            P(SP, None, "tp"),
            P(None, "tp"),
            P(None, "tp"),
            P(None, "tp"),
            P(),
            P(),
            P("tp"),
            P("tp"),
            P("tp", None),
            P("tp", None),
            P(),
            P(SP, None),
            P(SP, None),
            P(SP, None, "tp"),
            P(SP, None, "tp"),
            P(SP, "tp", None),
        ),
        out_specs=P(SP, "tp"),
        check_vma=False,
    )
```

```python
import functools

import jax
import jax.numpy as jnp
from jax import lax
from jax.experimental import pallas as pl
from jax.experimental.pallas import tpu as pltpu
from jax.sharding import PartitionSpec as P

HEADS = 16
NARROW_HEAD_DIM = 64
WIDE_HEAD_DIM = 128
GROUPS = 4
CONV = 4
SP = "sp"


NORM_EPS = 1e-06
CLAMP_LIMIT = 7.0
SIGMOID_SCALE = 1.702
FULL_PRECISION = lax.Precision.HIGHEST


MESH = pl.DeviceIdType.MESH
CORES = 2
SIDE = 4
LAG = 2
CHUNKS = 4
PICKS = 3


def remote(src, dst, send_sem, recv_sem, device):
    return pltpu.make_async_remote_copy(
        src_ref=src,
        dst_ref=dst,
        send_sem=send_sem,
        recv_sem=recv_sem,
        device_id=device,
        device_id_type=MESH,
    )


class Place:
    def __init__(self, chips):
        self.chips = chips
        self.sp = lax.axis_index("sp")
        self.tp = lax.axis_index("tp")
        self.z, self.core = self.sp // CORES, self.sp % CORES
        self.at = {"y": self.tp // SIDE, "x": self.tp % SIDE}

        self.at["a"] = self.pick(self.core, self.at["x"], self.at["y"])
        self.at["b"] = self.pick(self.core, self.at["y"], self.at["x"])

    def pick(self, core, first, second):
        return first + core * (second - first)

    def flat(self, core, a, b):
        return b * (SIDE - (SIDE - 1) * core) + a * (1 + (SIDE - 1) * core)

    def plane(self, axis, step):
        if axis == "a":
            return (self.sp, self.flat(self.core, self.index("a", step), self.at["b"]))
        if axis == "b":
            return (self.sp, self.flat(self.core, self.at["a"], self.index("b", step)))
        moved = (self.at[axis] + step + SIDE) % SIDE
        if axis == "x":
            return (self.sp, self.at["y"] * SIDE + moved)
        return (self.sp, moved * SIDE + self.at["x"])

    def index(self, axis, step):
        return (self.at[axis] + step + SIDE) % SIDE

    def along(self, step, core):
        return (((self.z + step + self.chips) % self.chips) * CORES + core, self.tp)


def chip_order(chips):
    if chips == 16:
        return [1, 15, 3, 13, 5, 11, 7, 9, 8, 6, 10, 4, 12, 2, 14, 0]
    return [d % chips for d in range(1, chips + 1)]


def greet(place):
    barrier = pltpu.get_barrier_semaphore()
    count = 0
    devices = place.chips * CORES

    def tell(sp, a, b):
        device = (sp, place.flat(place.core, a, b))
        pl.semaphore_signal(barrier, inc=1, device_id=device, device_id_type=MESH)

    own_a, own_b = place.at["a"], place.at["b"]
    for step in range(devices):
        for side in range(SIDE):
            if step or side:
                tell((place.sp + step) % devices, (own_a + side) % SIDE, own_b)
                count += 1
    for side in range(1, SIDE):
        for step in range(place.chips):
            other = ((place.z + step) % place.chips) * CORES + 1 - place.core
            tell(other, own_a, (own_b + side) % SIDE)
            count += 1
        tell(place.sp, own_a, (own_b + side) % SIDE)
        count += 1
    return barrier, count


class Gather:
    def __init__(self, place, gate_up, down, sent, got):
        self.place, self.gate_up, self.down = place, gate_up, down
        self.sent, self.got, self.started, self.loads = sent, got, {}, []
        self.width = down.shape[0] // SIDE

    def piece(self, kind, step, part=None):
        index = self.place.index("a", step)
        if kind == 2:
            ref = self.down.at[pl.ds(pl.multiple_of(index * self.width, self.width), self.width)]
        else:
            start = pl.multiple_of(index * self.width + kind * SIDE * self.width, self.width)
            ref = self.gate_up.at[:, pl.ds(start, self.width)]
        if part is None:
            return ref
        size = ref.shape[0] // 2
        return ref.at[pl.ds(part * size, size)]

    def load(self, gate_hbm, up_hbm, down_hbm, sem):
        for kind, src in enumerate((gate_hbm, up_hbm, down_hbm)):
            dst = self.piece(kind, 0)
            copies = []
            for i in range(SIDE):
                for j in range(SIDE):
                    number = i * SIDE + j
                    there = self.place.flat(self.place.core, j, i) * self.width
                    there = pl.ds(pl.multiple_of(there, self.width), self.width)
                    here = pl.ds(number * self.width, self.width)
                    if kind == 2:
                        copy = pltpu.make_async_copy(
                            src.at[:, there], dst.at[:, here], sem.at[kind, number]
                        )
                    else:
                        copy = pltpu.make_async_copy(
                            src.at[there], dst.at[here], sem.at[kind, number]
                        )
                    copy.start()
                    copies.append(copy)
            self.loads.append(copies)

    def send(self, ref, kind, number, step):
        copy = remote(
            ref, ref, self.sent.at[kind, number], self.got.at[kind, number],
            self.place.plane("a", step),
        )
        copy.start()
        self.started[(kind, number)] = copy

    def open(self):
        for kind in range(3):
            for copy in self.loads[kind]:
                copy.wait()
            self.send(self.piece(kind, 0), kind, 0, 1)
            self.send(self.piece(kind, 0), kind, 1, SIDE - 1)

    def pass_on(self, kind):
        self.started[(kind, 0)].wait_recv()
        self.send(self.piece(kind, SIDE - 1, 0), kind, 2, 1)
        self.started[(kind, 1)].wait_recv()
        self.send(self.piece(kind, 1, 1), kind, 3, SIDE - 1)

    def close(self):
        for kind in range(3):
            self.started[(kind, 2)].wait_recv()
            self.started[(kind, 3)].wait_recv()


class Line:
    def __init__(self, place, tokens, blocks, relay, sums, sent, got):
        self.place, self.tokens, self.blocks = place, tokens, blocks
        self.relay, self.sums, self.sent, self.got = relay, sums, sent, got
        self.started = []
        rows = tokens.shape[2]
        self.low, self.high = pl.ds(0, rows // 2), pl.ds(rows // 2, rows // 2)

    def send(self, src, dst, step):
        number = len(self.started)
        copy = remote(
            src, dst, self.sent.at[number], self.got.at[number], self.place.plane("b", step)
        )
        copy.start()
        self.started.append(copy)

    def open(self):
        own = self.tokens.at[self.place.at["b"]]
        self.send(own, own, 1)
        self.send(own, own, SIDE - 1)

    def pass_on(self):
        for side, step in ((0, SIDE - 1), (1, 1)):
            self.started[side].wait_recv()
            part = self.low if side == 0 else self.high
            ref = self.tokens.at[self.place.index("b", step)].at[:, part]
            self.send(ref, ref, SIDE - step)

    def arrived(self):
        self.started[2].wait_recv()
        self.started[3].wait_recv()

    def give(self):
        far = self.blocks.at[self.place.index("b", 2)]
        self.send(far.at[:, self.low], self.relay.at[0], 1)
        self.send(far.at[:, self.high], self.relay.at[1], SIDE - 1)

    def add(self):
        for side, step in ((0, 1), (1, SIDE - 1)):
            part = self.low if side == 0 else self.high
            self.started[4 + side].wait_recv()
            near = self.blocks.at[self.place.index("b", step)]
            piece = near.at[:, part]
            piece[...] = (
                piece[...].astype(jnp.float32) + self.relay[side].astype(jnp.float32)
            ).astype(jnp.bfloat16)
            self.send(near, self.sums.at[side], step)

    def total(self):
        self.started[6].wait_recv()
        self.started[7].wait_recv()
        return (
            self.blocks[self.place.at["b"]].astype(jnp.float32)
            + self.sums[0].astype(jnp.float32)
            + self.sums[1].astype(jnp.float32)
        )


def chunk_of(ref, axis, index):
    return ref.at[index] if axis == "y" else ref.at[:, index]


class Summer:
    def __init__(self, place, first, blocks, relay, sums, half, last, sent, got):
        self.place, self.first, self.second = place, first, "y" if first == "x" else "x"
        self.blocks, self.relay, self.sums = blocks, relay, sums
        self.half, self.last, self.sent, self.got = half, last, sent, got
        self.started = []
        rows = blocks.shape[2]
        self.low, self.high = pl.ds(0, rows // 2), pl.ds(rows // 2, rows // 2)

    def send(self, src, dst, axis, step, number):
        copy = remote(
            src, dst, self.sent.at[number], self.got.at[number], self.place.plane(axis, step)
        )
        copy.start()
        self.started.append(copy)

    def open(self):
        far = chunk_of(self.blocks, self.first, self.place.index(self.first, 2))
        self.send(far.at[:, self.low], self.relay.at[0], self.first, 1, 0)
        self.send(far.at[:, self.high], self.relay.at[1], self.first, SIDE - 1, 1)

    def pass_on(self):
        for side, step in ((0, 1), (1, SIDE - 1)):
            part = self.low if side == 0 else self.high
            self.started[side].wait_recv()
            near = chunk_of(self.blocks, self.first, self.place.index(self.first, step))
            piece = near.at[:, part]
            piece[...] = (
                piece[...].astype(jnp.float32) + self.relay[side].astype(jnp.float32)
            ).astype(jnp.bfloat16)
            self.send(near, self.sums.at[side], self.first, step, 2 + side)

    def turn(self):
        self.started[2].wait_recv()
        self.started[3].wait_recv()
        own = chunk_of(self.blocks, self.first, self.place.at[self.first])
        own[...] = (
            own[...].astype(jnp.float32)
            + self.sums[0].astype(jnp.float32)
            + self.sums[1].astype(jnp.float32)
        ).astype(jnp.bfloat16)
        far = own.at[self.place.index(self.second, 2)]
        self.send(far.at[self.low], self.half.at[0], self.second, 1, 4)
        self.send(far.at[self.high], self.half.at[1], self.second, SIDE - 1, 5)

    def pass_again(self):
        own = chunk_of(self.blocks, self.first, self.place.at[self.first])
        for side, step in ((0, 1), (1, SIDE - 1)):
            part = self.low if side == 0 else self.high
            self.started[4 + side].wait_recv()
            near = own.at[self.place.index(self.second, step)]
            piece = near.at[part]
            piece[...] = (
                piece[...].astype(jnp.float32) + self.half[side].astype(jnp.float32)
            ).astype(jnp.bfloat16)
            self.send(near, self.last.at[side], self.second, step, 6 + side)

    def close(self):
        self.started[6].wait_recv()
        self.started[7].wait_recv()
        own = chunk_of(self.blocks, self.first, self.place.at[self.first])
        mine = own.at[self.place.at[self.second]]
        return (
            mine[...].astype(jnp.float32)
            + self.last[0].astype(jnp.float32)
            + self.last[1].astype(jnp.float32)
        )


def iota(shape, dim):
    return lax.broadcasted_iota(jnp.int32, shape, dim)


def ones_where(mask):
    return jnp.where(mask, 1.0, 0.0).astype(jnp.bfloat16)


def dot(a, b):
    return jnp.dot(a, b, preferred_element_type=jnp.float32)


def in_two(x):
    high = x.astype(jnp.bfloat16)
    return high, (x - high.astype(jnp.float32)).astype(jnp.bfloat16)


def routing_tables(experts, cap, tall, flat, choice, share):
    tokens, picks = tall.shape[0], PICKS
    slots = experts * cap
    shift = cap.bit_length() - 1
    start = 8 + picks
    named = (tall[:, start : start + picks] + 0.5).astype(jnp.int32)
    turned = (flat[start : start + picks, :] + 0.5).astype(jnp.int32)
    amount = tall[:, 8 : 8 + picks]
    lines = iota((experts, tokens), 0)
    there = turned[0:1, :] == lines
    for k in range(1, picks):
        there = there | (turned[k : k + 1, :] == lines)
    before = ones_where(iota((tokens, tokens), 0) < iota((tokens, tokens), 1))
    rank = jnp.where(there, dot(ones_where(there), before), -1.0).astype(jnp.bfloat16)
    spread = ones_where((iota((slots, experts), 0) >> shift) == iota((slots, experts), 1))
    wide = dot(spread, rank)
    number = (iota((slots, tokens), 0) & (cap - 1)).astype(jnp.float32)
    choice[...] = ones_where(wide == number)

    columns = iota((tokens, experts), 1)
    hit = named[:, 0:1] == columns
    weight = jnp.where(hit, amount[:, 0:1], 0.0)
    for k in range(1, picks):
        now = named[:, k : k + 1] == columns
        hit = hit | now
        weight = weight + jnp.where(now, amount[:, k : k + 1], 0.0)
    after = ones_where(iota((tokens, tokens), 1) < iota((tokens, tokens), 0))
    rank = jnp.where(hit, dot(after, ones_where(hit)), -1.0).astype(jnp.bfloat16)
    spread = ones_where(iota((experts, slots), 0) == (iota((experts, slots), 1) >> shift))
    wide = dot(rank, spread)
    number = (iota((tokens, slots), 1) & (cap - 1)).astype(jnp.float32)
    mine = wide == number
    for part, piece in enumerate(in_two(weight)):
        share[part] = jnp.where(mine, dot(piece, spread), 0.0).astype(jnp.bfloat16)


def fine_dot(a, b, dims=(((1,), (0,)), ((), ()))):
    return lax.dot_general(
        a, b, dims, precision=FULL_PRECISION, preferred_element_type=jnp.float32
    )


def quick_dot(a, b, dims=(((1,), (0,)), ((), ()))):
    a, b = a.astype(jnp.bfloat16), b.astype(jnp.bfloat16)
    return lax.dot_general(a, b, dims, preferred_element_type=jnp.float32)


def in_three(x):
    high, rest = x.astype(jnp.bfloat16), None
    rest = x - high.astype(jnp.float32)
    middle = rest.astype(jnp.bfloat16)
    low = (rest - middle.astype(jnp.float32)).astype(jnp.bfloat16)
    return high, middle, low


def silu(x):
    return x * jax.nn.sigmoid(x)


RIM = 16
STATE_ROWS = 8


def layer_kernel(
    chips,
    cap,
    chunks,
    narrow_turned,
    wide_in,
    gate_turned,
    wide_gate,
    lines,
    narrow_taps,
    wide_taps,
    key_taps,
    query_taps,
    narrow_gain,
    wide_gain,
    last_gain,
    key_hbm,
    query_hbm,
    resid_hbm,
    narrow_rows_hbm,
    wide_rows_hbm,
    gate_hbm,
    up_hbm,
    down_hbm,
    out,
    narrow_in,
    keys,
    queries,
    resid,
    narrow_rows,
    wide_rows,
    narrow_rim,
    wide_rim,
    key_rim,
    query_rim,
    padded,
    told,
    heard,
    answer,
    carried,
    partial,
    relay,
    sums,
    half,
    last,
    load_sem,
    rim_sent,
    rim_got,
    told_sent,
    told_got,
    answer_sent,
    answer_got,
    sum_sent,
    sum_got,
    state,
    choice,
    share,
    outgoing,
    tokens,
    gate_up,
    down,
    blocks,
    line_relay,
    line_sums,
    result,
    back,
    weight_load,
    weight_sent,
    weight_got,
    out_sent,
    out_got,
    line_sent,
    line_got,
    back_sent,
    back_got,
):
    place = Place(chips)
    devices = chips * CORES
    length = narrow_in.shape[0]
    width = keys.shape[1]
    plane = SIDE * SIDE
    barrier, count = greet(place)
    group = pl.multiple_of((place.tp // (HEADS // GROUPS)) * width, width)
    mine = pl.ds(pl.multiple_of(place.tp * width, width), width)
    pairs = (
        (key_hbm.at[:, pl.ds(group, width)], keys),
        (query_hbm.at[:, pl.ds(group, width)], queries),
        (resid_hbm.at[:, mine], resid),
        (narrow_rows_hbm, narrow_rows),
        (wide_rows_hbm, wide_rows),
    )
    gather = Gather(place, gate_up, down, weight_sent, weight_got)
    gather.load(gate_hbm, up_hbm, down_hbm, weight_load)
    loads = [pltpu.make_async_copy(src, dst, load_sem.at[k]) for k, (src, dst) in enumerate(pairs)]
    for load in loads:
        load.start()

    upper = ones_where(iota((length, length), 0) <= iota((length, length), 1))
    causal = iota((length, length), 0) >= iota((length, length), 1)
    lower = ones_where(causal)
    same = iota((length, length), 0) == iota((length, length), 1)
    across = (((1,), (1,)), ((), ()))
    flat = lines[...]
    tall = fine_dot(jnp.where(same, 1.0, 0.0), flat, across)
    narrow_in[...] = quick_dot(ones_where(same), narrow_turned[...], across).astype(jnp.bfloat16)
    narrow_open = silu(quick_dot(ones_where(same), gate_turned[...], across))
    wide_open = silu(wide_gate[...].astype(jnp.float32))
    tall_sum = sum(dot(lower, piece) for piece in in_three(tall))
    flat_sum = sum(dot(piece, upper) for piece in in_three(flat))
    decay, tails, totals, steps = [], [], [], []
    for kind in (0, 1):
        down_column = tall_sum[:, 2 + kind : 3 + kind]
        across = flat_sum[2 + kind : 3 + kind, :]
        decay.append(jnp.exp(jnp.where(causal, down_column - across, -1e30)))
        total = down_column[length - 1 : length, :]
        totals.append(total)
        tails.append(jnp.exp(total - down_column))
        steps.append(tall[:, kind : kind + 1])
    fades = [jnp.exp(tall_sum[:, 2 + kind : 3 + kind]) for kind in (0, 1)]
    rows = iota((width, devices * STATE_ROWS), 0)
    spots = iota((width, devices * STATE_ROWS), 1)
    per = STATE_ROWS // 2
    owner_row = (spots >> 3) * per + (spots & (per - 1))
    wide_spread = jnp.where((owner_row == rows) & ((spots & 7) < per), 1.0, 0.0)
    narrow_spread = jnp.where((owner_row == rows) & ((spots & 7) >= per), 1.0, 0.0)

    loads[0].wait()
    loads[1].wait()
    pl.semaphore_wait(barrier, count)
    gather.open()
    following = ((place.sp + 1) % devices, place.tp)
    rims = []
    tail = pl.ds(length - RIM, RIM)
    for k, (src, dst) in enumerate(
        ((narrow_in, narrow_rim), (wide_in, wide_rim), (keys, key_rim), (queries, query_rim))
    ):
        copy = remote(src.at[tail], dst, rim_sent.at[k], rim_got.at[k], following)
        copy.start()
        rims.append(copy)
    for copy in rims:
        copy.wait_recv()

    inner = place.sp > 0

    def mixed_rows(values, rim, taps):
        size = values.shape[1]
        before = jnp.where(inner, rim[...].astype(jnp.float32), 0.0)
        padded[0:RIM, 0:size] = before
        padded[RIM : RIM + length, 0:size] = values[...].astype(jnp.float32)
        total = jnp.zeros((length, size), jnp.float32)
        for k in range(CONV):
            start = RIM - CONV + 1 + k
            total = total + taps[k : k + 1, :] * padded[start : start + length, 0:size]
        return silu(total)

    key = mixed_rows(keys, key_rim, key_taps[:, pl.ds(group, width)])
    query = mixed_rows(queries, query_rim, query_taps[:, pl.ds(group, width)])
    narrow_mix = mixed_rows(narrow_in, narrow_rim, narrow_taps[...])
    wide_mix = mixed_rows(wide_in, wide_rim, wide_taps[...])
    narrow_size = narrow_mix.shape[1]
    narrow_value, wide_value = narrow_mix * steps[0], wide_mix * steps[1]

    turned = (((0,), (0,)), ((), ()))
    wide_keys = quick_dot(key, wide_spread)
    narrow_keys = quick_dot(key, narrow_spread)
    wide_state = quick_dot(wide_keys, wide_value * tails[1], turned)
    narrow_state = quick_dot(
        narrow_keys,
        jnp.concatenate(
            [narrow_value * tails[0], jnp.zeros((length, width - narrow_size), jnp.float32)], axis=1
        ),
        turned,
    )
    tile = iota((devices * STATE_ROWS, width), 0) & 7
    lane = iota((devices * STATE_ROWS, width), 1)
    spare = jnp.where(lane < (narrow_size + width) // 2, totals[1], totals[0])
    message = wide_state + narrow_state
    message = jnp.where((tile >= per) & (lane >= narrow_size), spare, message)
    told[...] = message.reshape(devices, STATE_ROWS, width).astype(jnp.bfloat16)

    def exchange(src, dst, sent, got):
        copies = []
        dst[place.sp] = src[place.sp]
        for step in range(1, devices):
            other = (place.sp + step) % devices
            copy = remote(
                src.at[other], dst.at[place.sp], sent.at[step], got.at[step], (other, place.tp)
            )
            copy.start()
            copies.append(copy)
        return copies

    tells = exchange(told, heard, told_sent, told_got)

    scores = quick_dot(query, key, (((1,), (1,)), ((), ())))
    narrow_inside = quick_dot(scores * decay[0], narrow_value)
    wide_inside = quick_dot(scores * decay[1], wide_value)
    wide_query = quick_dot(query * fades[1], wide_spread)
    narrow_query = quick_dot(query * fades[0], narrow_spread)

    for copy in tells:
        copy.wait_recv()
    gather.pass_on(0)
    running = jnp.zeros((STATE_ROWS, width), jnp.float32)
    upper_rows = iota((STATE_ROWS, width), 0) < per
    for source in range(devices):
        answer[source] = running.astype(jnp.bfloat16)
        piece = heard[source].astype(jnp.float32)
        wide_total = piece[per : per + 1, narrow_size : narrow_size + 1]
        middle = (narrow_size + width) // 2
        narrow_total = piece[per : per + 1, middle : middle + 1]
        factor = jnp.exp(jnp.where(upper_rows, wide_total, narrow_total))
        running = factor * running + piece
    answers = exchange(answer, carried, answer_sent, answer_got)
    routing_tables(devices, cap, tall, flat, choice, share)

    for load in loads[2:]:
        load.wait()
    for copy in answers:
        copy.wait_recv()
    gather.pass_on(1)
    entering = carried[...].astype(jnp.float32).reshape(devices * STATE_ROWS, width)

    def head(inside, asked, size, kind, mix, opened, gain):
        result = inside + quick_dot(asked, entering)[:, :size]
        result = (result + tall[:, 4 + kind : 5 + kind] * mix) * opened
        mean = jnp.sum(result * result, axis=-1, keepdims=True) * (1.0 / size)
        return (result * lax.rsqrt(mean + NORM_EPS) * gain[...]).astype(jnp.bfloat16)

    narrow = head(narrow_inside, narrow_query, narrow_size, 0, narrow_mix, narrow_open, narrow_gain)
    wide = head(wide_inside, wide_query, width, 1, wide_mix, wide_open, wide_gain)

    totals_of = [
        Summer(
            place, first, partial.at[u], relay.at[u], sums.at[u], half.at[u], last.at[u],
            sum_sent.at[u], sum_got.at[u],
        )
        for u, first in ((0, "x"), (1, "y"))
    ]
    unit = length // 2
    for i in range(SIDE):
        part = pl.ds(i * SIDE * width, SIDE * width)
        product = dot(narrow, narrow_rows[:, part]) + dot(wide, wide_rows[:, part])
        product = product.astype(jnp.bfloat16)
        for j in range(SIDE):
            for u in (0, 1):
                partial[u, i, j] = product[u * unit : (u + 1) * unit, j * width : (j + 1) * width]
    for move in ("open", "pass_on", "turn", "pass_again"):
        for total in totals_of:
            getattr(total, move)()
    mixed = jnp.concatenate([total.close() for total in totals_of], axis=0)
    hidden = resid[...].astype(jnp.float32) + mixed
    gather.pass_on(2)
    state[...] = hidden
    outgoing[...] = dot(choice[...], hidden.astype(jnp.bfloat16)).astype(jnp.bfloat16)
    order = chip_order(chips)
    spot = {d: k for k, d in enumerate(order)}
    row, column_own, core = place.at["b"], place.at["a"], place.core
    home = spot[0]
    inside = column_own == 2 * (home % 2) + core
    outside = column_own != 2 * (home % 2) + core
    waits = []

    def slot_rows(number):
        return pl.ds(pl.multiple_of(number * cap, cap), cap)

    def guarded(apart, act):
        if apart:
            pl.when(outside)(act)
        else:
            act()

    for s, d in enumerate(order):
        for other in (0, 1):
            aim = core if other == 0 else 1 - core
            target = ((place.z + chips - d) % chips) * CORES + aim
            across = place.pick(aim, place.at["x"], place.at["y"])
            along = place.pick(aim, place.at["y"], place.at["x"])
            device = (target, place.flat(aim, 2 * (s % 2) + core, along))
            rows = slot_rows(target)
            to = pl.ds((s // 2) * cap, cap)
            copy = remote(
                outgoing.at[rows],
                tokens.at[along, across, to],
                out_sent.at[s * 2 + other],
                out_got.at[s // 2, across],
                device,
            )
            apart = d == 0 and other == 0
            guarded(apart, copy.start)
            waits.append((apart, copy))
            if apart:

                @pl.when(inside)
                def _(rows=rows, to=to):
                    tokens[row, column_own, to, :] = outgoing[rows, :]

    units = chips // 2
    per = units // chunks
    size = per * cap
    parts = []

    def steps(k):
        rows = pl.ds(k * size, size)
        line = Line(
            place, tokens.at[:, :, rows], blocks.at[k], line_relay.at[k], line_sums.at[k],
            line_sent.at[k], line_got.at[k],
        )
        parts.append(line)

        def arrive():
            for u in range(k * per, (k + 1) * per):
                for side in range(SIDE):
                    column = (column_own + side) % SIDE
                    to = pl.ds(u * cap, cap)
                    copy = remote(
                        outgoing.at[pl.ds(0, cap)],
                        tokens.at[row, column, to],
                        out_sent.at[0],
                        out_got.at[u, column],
                        place.plane("b", 1),
                    )
                    guarded(side == 0 and u == home // 2, copy.wait_recv)
            line.open()

        def compute():
            line.arrived()
            if k == 0:
                gather.close()
            pairs_of = [(i, j) for i in range(SIDE) for j in range(SIDE)]
            pieces = [tokens[i, j, rows, :].astype(jnp.float32) for i, j in pairs_of]
            squared = sum(piece * piece for piece in pieces)
            mean = jnp.sum(squared, axis=-1, keepdims=True) * (1.0 / (plane * width))
            scale = lax.rsqrt(mean + NORM_EPS)
            gains = [
                last_gain[
                    :, pl.ds(pl.multiple_of(place.flat(core, j, i) * width, width), width)
                ]
                for i, j in pairs_of
            ]
            values = jnp.concatenate(
                [(piece * scale * gain).astype(jnp.bfloat16) for piece, gain in zip(pieces, gains)],
                axis=1,
            )
            both = dot(values, gate_up[...])
            hidden_units = both.shape[1] // 2
            gate = jnp.minimum(both[:, :hidden_units], CLAMP_LIMIT)
            up = jnp.clip(both[:, hidden_units:], -CLAMP_LIMIT, CLAMP_LIMIT)
            act = ((up + 1.0) * gate * jax.nn.sigmoid(SIGMOID_SCALE * gate)).astype(jnp.bfloat16)
            for i in range(SIDE):
                wide_part = dot(act, down[:, i * SIDE * width : (i + 1) * SIDE * width])
                for j in range(SIDE):
                    blocks[k, i, j] = wide_part[:, j * width : (j + 1) * width].astype(jnp.bfloat16)
            line.give()

        def close():
            result[k] = line.total().astype(jnp.bfloat16)
            for u in range(k * per, (k + 1) * per):
                d = order[2 * u] + (column_own // 2) * (order[2 * u + 1] - order[2 * u])
                source = ((place.z + d) % chips) * CORES + column_own % 2
                number = (2 * u + column_own // 2) * 2 + (column_own % 2 + core) % 2
                piece = pl.ds((u - k * per) * cap, cap)
                for side in range(SIDE):
                    column = (column_own + side) % SIDE
                    copy = remote(
                        result.at[k, column, piece],
                        back.at[slot_rows(place.sp)],
                        back_sent.at[u, side],
                        back_got.at[number],
                        (source, place.flat(core, column, row)),
                    )
                    apart = side == 0 and u == home // 2
                    guarded(apart, copy.start)
                    waits.append((apart, copy))
                    if apart:

                        @pl.when(inside)
                        def _(piece=piece):
                            back[slot_rows(place.sp), :] = result[k, column_own, piece, :]

        return [arrive, line.pass_on, compute, line.add, close]

    plans = [steps(k) for k in range(chunks)]
    depth = len(plans[0])
    turns = sorted((k + LAG * n, -n, k) for k in range(chunks) for n in range(depth))
    for _, n, k in turns:
        plans[k][-n]()
    for s in range(chips):
        for other in (0, 1):
            copy = remote(
                outgoing.at[pl.ds(0, cap)],
                back.at[pl.ds(0, cap)],
                out_sent.at[0],
                back_got.at[s * 2 + other],
                place.plane("b", 1),
            )
            guarded(s == home and other == 0, copy.wait_recv)
    combined = state[...] + dot(share[0], back[...]) + dot(share[1], back[...])
    out[...] = combined.astype(jnp.bfloat16)
    for apart, copy in waits:
        guarded(apart, copy.wait_send)
    for copy in gather.started.values():
        copy.wait_send()
    for line in parts:
        for copy in line.started:
            copy.wait_send()
    for copy in rims + tells + answers:
        copy.wait_send()
    for total in totals_of:
        for copy in total.started:
            copy.wait_send()


def layer_call(
    inputs, loose, chips, cap
):
    length, width = inputs[1].shape
    narrow_size = inputs[0].shape[0]
    narrow_rows, wide_rows, gate_hbm, down_hbm = loose[3], loose[4], loose[5], loose[7]
    devices = chips * CORES
    unit = length // 2
    chunks = CHUNKS
    slots = devices * cap
    rows = slots // SIDE
    size = rows // chunks
    features, hidden_units = gate_hbm.shape
    bf16, f32 = jnp.bfloat16, jnp.float32
    vmem, any_ = pl.BlockSpec(memory_space=pltpu.VMEM), pl.BlockSpec(memory_space=pl.ANY)
    dma = pltpu.SemaphoreType.DMA
    return pl.pallas_call(
        functools.partial(layer_kernel, chips, cap, chunks),
        out_shape=jax.ShapeDtypeStruct((length, width), bf16),
        in_specs=[vmem] * 12 + [any_] * 8,
        out_specs=vmem,
        scratch_shapes=[
            pltpu.VMEM((length, narrow_size), bf16),
            pltpu.VMEM((length, width), bf16),
            pltpu.VMEM((length, width), bf16),
            pltpu.VMEM((length, width), bf16),
            pltpu.VMEM(narrow_rows.shape, bf16),
            pltpu.VMEM(wide_rows.shape, bf16),
            pltpu.VMEM((RIM, narrow_size), bf16),
            pltpu.VMEM((RIM, width), bf16),
            pltpu.VMEM((RIM, width), bf16),
            pltpu.VMEM((RIM, width), bf16),
            pltpu.VMEM((RIM + length, width), f32),
            pltpu.VMEM((devices, STATE_ROWS, width), bf16),
            pltpu.VMEM((devices, STATE_ROWS, width), bf16),
            pltpu.VMEM((devices, STATE_ROWS, width), bf16),
            pltpu.VMEM((devices, STATE_ROWS, width), bf16),
            pltpu.VMEM((2, SIDE, SIDE, unit, width), bf16),
            pltpu.VMEM((2, 2, SIDE, unit // 2, width), bf16),
            pltpu.VMEM((2, 2, SIDE, unit, width), bf16),
            pltpu.VMEM((2, 2, unit // 2, width), bf16),
            pltpu.VMEM((2, 2, unit, width), bf16),
            dma((5,)),
            dma((4,)),
            dma((4,)),
            dma((devices,)),
            dma((devices,)),
            dma((devices,)),
            dma((devices,)),
            dma((2, 8)),
            dma((2, 8)),
            pltpu.VMEM((length, width), f32),
            pltpu.VMEM((slots, length), bf16),
            pltpu.VMEM((2, length, slots), bf16),
            pltpu.VMEM((slots, width), bf16),
            pltpu.VMEM((SIDE, SIDE, rows, width), bf16),
            pltpu.VMEM((features, 2 * SIDE * hidden_units), bf16),
            pltpu.VMEM((SIDE * hidden_units, features), bf16),
            pltpu.VMEM((chunks, SIDE, SIDE, size, width), bf16),
            pltpu.VMEM((chunks, 2, SIDE, size // 2, width), bf16),
            pltpu.VMEM((chunks, 2, SIDE, size, width), bf16),
            pltpu.VMEM((chunks, SIDE, size, width), bf16),
            pltpu.VMEM((slots, width), bf16),
            dma((3, SIDE * SIDE)),
            dma((3, 4)),
            dma((3, 4)),
            dma((devices,)),
            dma((chips // 2, SIDE)),
            dma((chunks, 8)),
            dma((chunks, 8)),
            dma((chips // 2, SIDE)),
            dma((devices,)),
        ],
        compiler_params=pltpu.CompilerParams(
            collective_id=0, has_side_effects=True, vmem_limit_bytes=56 * 1024 * 1024
        ),
    )(*inputs, *loose)


def local(
    resid,
    narrow_head_input,
    wide_head_input,
    key_group_input,
    query_group_input,
    narrow_output_gate,
    wide_output_gate,
    step_input_rows,
    head_decay_logarithm,
    position_log_decay,
    direct_input_weight,
    narrow_conv_taps,
    wide_conv_taps,
    key_conv_taps,
    query_conv_taps,
    narrow_norm_gain,
    wide_norm_gain,
    narrow_output_rows,
    wide_output_rows,
    feedforward_norm_gain,
    routes,
    routing_weight_values,
    expert_gate_matrix,
    expert_up_matrix,
    expert_down_matrix,
):
    chips = lax.axis_size(SP) // CORES
    steps = jax.nn.softplus(step_input_rows[:, :, 0].T.astype(jnp.float32))
    decays = -jnp.exp(head_decay_logarithm) * steps + position_log_decay[:, :, 0].T
    direct = jnp.broadcast_to(direct_input_weight, steps.shape)
    blank = jnp.zeros((2, steps.shape[1]), jnp.float32)
    lines = jnp.concatenate(
        [
            steps,
            decays,
            direct,
            blank,
            routing_weight_values.T,
            routes.T.astype(jnp.float32),
            blank,
        ],
        axis=0,
    )
    length, picks = routes.shape
    inputs = (
        narrow_head_input.T,
        wide_head_input,
        narrow_output_gate.T,
        wide_output_gate,
        lines,
        narrow_conv_taps,
        wide_conv_taps,
        key_conv_taps,
        query_conv_taps,
        narrow_norm_gain.reshape(1, -1),
        wide_norm_gain.reshape(1, -1),
        feedforward_norm_gain.reshape(1, -1),
    )
    loose = (
        key_group_input,
        query_group_input,
        resid,
        narrow_output_rows,
        wide_output_rows,
        expert_gate_matrix[0],
        expert_up_matrix[0],
        expert_down_matrix[0],
    )
    return layer_call(inputs, loose, chips, 4 * length * picks // (3 * chips * CORES))


def solution(mesh):
    return jax.shard_map(
        local,
        mesh=mesh,
        in_specs=(
            P(SP, None),
            P(SP, "tp"),
            P(SP, "tp"),
            P(SP, None),
            P(SP, None),
            P(SP, "tp"),
            P(SP, "tp"),
            P(SP, None, "tp"),
            P(None, "tp"),
            P(SP, None, "tp"),
            P(None, "tp"),
            P(None, "tp"),
            P(None, "tp"),
            P(),
            P(),
            P("tp"),
            P("tp"),
            P("tp", None),
            P("tp", None),
            P(),
            P(SP, None),
            P(SP, None),
            P(SP, None, "tp"),
            P(SP, None, "tp"),
            P(SP, "tp", None),
        ),
        out_specs=P(SP, "tp"),
        check_vma=False,
    )
```

```python
import functools

import jax
import jax.numpy as jnp
from jax import lax
from jax.experimental import pallas as pl
from jax.experimental.pallas import tpu as pltpu
from jax.sharding import PartitionSpec as P

HEADS = 16
NARROW_HEAD_DIM = 64
WIDE_HEAD_DIM = 128
GROUPS = 4
CONV = 4
SP = "sp"


NORM_EPS = 1e-06
CLAMP_LIMIT = 7.0
SIGMOID_SCALE = 1.702
FULL_PRECISION = lax.Precision.HIGHEST


MESH = pl.DeviceIdType.MESH
CORES = 2
SIDE = 4
LAG = 1
CHUNKS = 4
PICKS = 3


def remote(src, dst, send_sem, recv_sem, device):
    return pltpu.make_async_remote_copy(
        src_ref=src,
        dst_ref=dst,
        send_sem=send_sem,
        recv_sem=recv_sem,
        device_id=device,
        device_id_type=MESH,
    )


class Place:
    def __init__(self, chips):
        self.chips = chips
        self.sp = lax.axis_index("sp")
        self.tp = lax.axis_index("tp")
        self.z, self.core = self.sp // CORES, self.sp % CORES
        self.at = {"y": self.tp // SIDE, "x": self.tp % SIDE}

        self.at["a"] = self.pick(self.core, self.at["x"], self.at["y"])
        self.at["b"] = self.pick(self.core, self.at["y"], self.at["x"])

    def pick(self, core, first, second):
        return first + core * (second - first)

    def flat(self, core, a, b):
        return b * (SIDE - (SIDE - 1) * core) + a * (1 + (SIDE - 1) * core)

    def plane(self, axis, step):
        if axis == "a":
            return (self.sp, self.flat(self.core, self.index("a", step), self.at["b"]))
        if axis == "b":
            return (self.sp, self.flat(self.core, self.at["a"], self.index("b", step)))
        moved = (self.at[axis] + step + SIDE) % SIDE
        if axis == "x":
            return (self.sp, self.at["y"] * SIDE + moved)
        return (self.sp, moved * SIDE + self.at["x"])

    def index(self, axis, step):
        return (self.at[axis] + step + SIDE) % SIDE

    def along(self, step, core):
        return (((self.z + step + self.chips) % self.chips) * CORES + core, self.tp)


def chip_order(chips):
    if chips == 16:
        return [1, 15, 3, 13, 5, 11, 7, 9, 8, 6, 10, 4, 12, 2, 14, 0]
    return [d % chips for d in range(1, chips + 1)]


def greet(place):
    barrier = pltpu.get_barrier_semaphore()
    count = 0
    devices = place.chips * CORES

    def tell(sp, a, b):
        device = (sp, place.flat(place.core, a, b))
        pl.semaphore_signal(barrier, inc=1, device_id=device, device_id_type=MESH)

    own_a, own_b = place.at["a"], place.at["b"]
    for step in range(devices):
        for side in range(SIDE):
            if step or side:
                tell((place.sp + step) % devices, (own_a + side) % SIDE, own_b)
                count += 1
    for side in range(1, SIDE):
        for step in range(place.chips):
            other = ((place.z + step) % place.chips) * CORES + 1 - place.core
            tell(other, own_a, (own_b + side) % SIDE)
            count += 1
        tell(place.sp, own_a, (own_b + side) % SIDE)
        count += 1
    return barrier, count


class Gather:
    def __init__(self, place, gate_up, down, sent, got):
        self.place, self.gate_up, self.down = place, gate_up, down
        self.sent, self.got, self.started, self.loads = sent, got, {}, []
        self.width = down.shape[0] // SIDE

    def piece(self, kind, step, part=None):
        index = self.place.index("a", step)
        if kind == 2:
            ref = self.down.at[pl.ds(pl.multiple_of(index * self.width, self.width), self.width)]
        else:
            start = pl.multiple_of(index * self.width + kind * SIDE * self.width, self.width)
            ref = self.gate_up.at[:, pl.ds(start, self.width)]
        if part is None:
            return ref
        size = ref.shape[0] // 2
        return ref.at[pl.ds(part * size, size)]

    def load(self, gate_hbm, up_hbm, down_hbm, sem):
        for kind, src in enumerate((gate_hbm, up_hbm, down_hbm)):
            dst = self.piece(kind, 0)
            copies = []
            for i in range(SIDE):
                for j in range(SIDE):
                    number = i * SIDE + j
                    there = self.place.flat(self.place.core, j, i) * self.width
                    there = pl.ds(pl.multiple_of(there, self.width), self.width)
                    here = pl.ds(number * self.width, self.width)
                    if kind == 2:
                        copy = pltpu.make_async_copy(
                            src.at[:, there], dst.at[:, here], sem.at[kind, number]
                        )
                    else:
                        copy = pltpu.make_async_copy(
                            src.at[there], dst.at[here], sem.at[kind, number]
                        )
                    copy.start()
                    copies.append(copy)
            self.loads.append(copies)

    def send(self, ref, kind, number, step):
        copy = remote(
            ref, ref, self.sent.at[kind, number], self.got.at[kind, number],
            self.place.plane("a", step),
        )
        copy.start()
        self.started[(kind, number)] = copy

    def open(self):
        for kind in range(3):
            for copy in self.loads[kind]:
                copy.wait()
            self.send(self.piece(kind, 0), kind, 0, 1)
            self.send(self.piece(kind, 0), kind, 1, SIDE - 1)

    def pass_on(self, kind):
        self.started[(kind, 0)].wait_recv()
        self.send(self.piece(kind, SIDE - 1, 0), kind, 2, 1)
        self.started[(kind, 1)].wait_recv()
        self.send(self.piece(kind, 1, 1), kind, 3, SIDE - 1)

    def close(self):
        for kind in range(3):
            self.started[(kind, 2)].wait_recv()
            self.started[(kind, 3)].wait_recv()


class Line:
    def __init__(self, place, tokens, blocks, relay, sums, sent, got):
        self.place, self.tokens, self.blocks = place, tokens, blocks
        self.relay, self.sums, self.sent, self.got = relay, sums, sent, got
        self.started = []
        rows = tokens.shape[2]
        self.low, self.high = pl.ds(0, rows // 2), pl.ds(rows // 2, rows // 2)

    def send(self, src, dst, step):
        number = len(self.started)
        copy = remote(
            src, dst, self.sent.at[number], self.got.at[number], self.place.plane("b", step)
        )
        copy.start()
        self.started.append(copy)

    def open(self):
        own = self.tokens.at[self.place.at["b"]]
        self.send(own, own, 1)
        self.send(own, own, SIDE - 1)

    def pass_on(self):
        for side, step in ((0, SIDE - 1), (1, 1)):
            self.started[side].wait_recv()
            part = self.low if side == 0 else self.high
            ref = self.tokens.at[self.place.index("b", step)].at[:, part]
            self.send(ref, ref, SIDE - step)

    def arrived(self):
        self.started[2].wait_recv()
        self.started[3].wait_recv()

    def give(self):
        far = self.blocks.at[self.place.index("b", 2)]
        self.send(far.at[:, self.low], self.relay.at[0], 1)
        self.send(far.at[:, self.high], self.relay.at[1], SIDE - 1)

    def add(self):
        for side, step in ((0, 1), (1, SIDE - 1)):
            part = self.low if side == 0 else self.high
            self.started[4 + side].wait_recv()
            near = self.blocks.at[self.place.index("b", step)]
            piece = near.at[:, part]
            piece[...] = (
                piece[...].astype(jnp.float32) + self.relay[side].astype(jnp.float32)
            ).astype(jnp.bfloat16)
            self.send(near, self.sums.at[side], step)

    def total(self):
        self.started[6].wait_recv()
        self.started[7].wait_recv()
        return (
            self.blocks[self.place.at["b"]].astype(jnp.float32)
            + self.sums[0].astype(jnp.float32)
            + self.sums[1].astype(jnp.float32)
        )


def chunk_of(ref, axis, index):
    return ref.at[index] if axis == "y" else ref.at[:, index]


class Summer:
    def __init__(self, place, first, blocks, relay, sums, half, last, sent, got):
        self.place, self.first, self.second = place, first, "y" if first == "x" else "x"
        self.blocks, self.relay, self.sums = blocks, relay, sums
        self.half, self.last, self.sent, self.got = half, last, sent, got
        self.started = []
        rows = blocks.shape[2]
        self.low, self.high = pl.ds(0, rows // 2), pl.ds(rows // 2, rows // 2)

    def send(self, src, dst, axis, step, number):
        copy = remote(
            src, dst, self.sent.at[number], self.got.at[number], self.place.plane(axis, step)
        )
        copy.start()
        self.started.append(copy)

    def open(self):
        far = chunk_of(self.blocks, self.first, self.place.index(self.first, 2))
        self.send(far.at[:, self.low], self.relay.at[0], self.first, 1, 0)
        self.send(far.at[:, self.high], self.relay.at[1], self.first, SIDE - 1, 1)

    def pass_on(self):
        for side, step in ((0, 1), (1, SIDE - 1)):
            part = self.low if side == 0 else self.high
            self.started[side].wait_recv()
            near = chunk_of(self.blocks, self.first, self.place.index(self.first, step))
            piece = near.at[:, part]
            piece[...] = (
                piece[...].astype(jnp.float32) + self.relay[side].astype(jnp.float32)
            ).astype(jnp.bfloat16)
            self.send(near, self.sums.at[side], self.first, step, 2 + side)

    def turn(self):
        self.started[2].wait_recv()
        self.started[3].wait_recv()
        own = chunk_of(self.blocks, self.first, self.place.at[self.first])
        own[...] = (
            own[...].astype(jnp.float32)
            + self.sums[0].astype(jnp.float32)
            + self.sums[1].astype(jnp.float32)
        ).astype(jnp.bfloat16)
        far = own.at[self.place.index(self.second, 2)]
        self.send(far.at[self.low], self.half.at[0], self.second, 1, 4)
        self.send(far.at[self.high], self.half.at[1], self.second, SIDE - 1, 5)

    def pass_again(self):
        own = chunk_of(self.blocks, self.first, self.place.at[self.first])
        for side, step in ((0, 1), (1, SIDE - 1)):
            part = self.low if side == 0 else self.high
            self.started[4 + side].wait_recv()
            near = own.at[self.place.index(self.second, step)]
            piece = near.at[part]
            piece[...] = (
                piece[...].astype(jnp.float32) + self.half[side].astype(jnp.float32)
            ).astype(jnp.bfloat16)
            self.send(near, self.last.at[side], self.second, step, 6 + side)

    def close(self):
        self.started[6].wait_recv()
        self.started[7].wait_recv()
        own = chunk_of(self.blocks, self.first, self.place.at[self.first])
        mine = own.at[self.place.at[self.second]]
        return (
            mine[...].astype(jnp.float32)
            + self.last[0].astype(jnp.float32)
            + self.last[1].astype(jnp.float32)
        )


def iota(shape, dim):
    return lax.broadcasted_iota(jnp.int32, shape, dim)


def ones_where(mask):
    return jnp.where(mask, 1.0, 0.0).astype(jnp.bfloat16)


def dot(a, b):
    return jnp.dot(a, b, preferred_element_type=jnp.float32)


def in_two(x):
    high = x.astype(jnp.bfloat16)
    return high, (x - high.astype(jnp.float32)).astype(jnp.bfloat16)


def routing_tables(experts, cap, tall, flat, choice, share):
    tokens, picks = tall.shape[0], PICKS
    slots = experts * cap
    shift = cap.bit_length() - 1
    start = 8 + picks
    named = (tall[:, start : start + picks] + 0.5).astype(jnp.int32)
    turned = (flat[start : start + picks, :] + 0.5).astype(jnp.int32)
    amount = tall[:, 8 : 8 + picks]
    lines = iota((experts, tokens), 0)
    there = turned[0:1, :] == lines
    for k in range(1, picks):
        there = there | (turned[k : k + 1, :] == lines)
    before = ones_where(iota((tokens, tokens), 0) < iota((tokens, tokens), 1))
    rank = jnp.where(there, dot(ones_where(there), before), -1.0).astype(jnp.bfloat16)
    spread = ones_where((iota((slots, experts), 0) >> shift) == iota((slots, experts), 1))
    wide = dot(spread, rank)
    number = (iota((slots, tokens), 0) & (cap - 1)).astype(jnp.float32)
    choice[...] = ones_where(wide == number)

    columns = iota((tokens, experts), 1)
    hit = named[:, 0:1] == columns
    weight = jnp.where(hit, amount[:, 0:1], 0.0)
    for k in range(1, picks):
        now = named[:, k : k + 1] == columns
        hit = hit | now
        weight = weight + jnp.where(now, amount[:, k : k + 1], 0.0)
    after = ones_where(iota((tokens, tokens), 1) < iota((tokens, tokens), 0))
    rank = jnp.where(hit, dot(after, ones_where(hit)), -1.0).astype(jnp.bfloat16)
    spread = ones_where(iota((experts, slots), 0) == (iota((experts, slots), 1) >> shift))
    wide = dot(rank, spread)
    number = (iota((tokens, slots), 1) & (cap - 1)).astype(jnp.float32)
    mine = wide == number
    for part, piece in enumerate(in_two(weight)):
        share[part] = jnp.where(mine, dot(piece, spread), 0.0).astype(jnp.bfloat16)


def fine_dot(a, b, dims=(((1,), (0,)), ((), ()))):
    return lax.dot_general(
        a, b, dims, precision=FULL_PRECISION, preferred_element_type=jnp.float32
    )


def quick_dot(a, b, dims=(((1,), (0,)), ((), ()))):
    a, b = a.astype(jnp.bfloat16), b.astype(jnp.bfloat16)
    return lax.dot_general(a, b, dims, preferred_element_type=jnp.float32)


def in_three(x):
    high, rest = x.astype(jnp.bfloat16), None
    rest = x - high.astype(jnp.float32)
    middle = rest.astype(jnp.bfloat16)
    low = (rest - middle.astype(jnp.float32)).astype(jnp.bfloat16)
    return high, middle, low


def silu(x):
    return x * jax.nn.sigmoid(x)


RIM = 16
STATE_ROWS = 8


def layer_kernel(
    chips,
    cap,
    chunks,
    narrow_turned,
    wide_in,
    gate_turned,
    wide_gate,
    lines,
    narrow_taps,
    wide_taps,
    key_taps,
    query_taps,
    narrow_gain,
    wide_gain,
    last_gain,
    key_hbm,
    query_hbm,
    resid_hbm,
    narrow_rows_hbm,
    wide_rows_hbm,
    gate_hbm,
    up_hbm,
    down_hbm,
    out,
    narrow_in,
    keys,
    queries,
    resid,
    narrow_rows,
    wide_rows,
    narrow_rim,
    wide_rim,
    key_rim,
    query_rim,
    padded,
    told,
    heard,
    answer,
    carried,
    partial,
    relay,
    sums,
    half,
    last,
    load_sem,
    rim_sent,
    rim_got,
    told_sent,
    told_got,
    answer_sent,
    answer_got,
    sum_sent,
    sum_got,
    state,
    choice,
    share,
    outgoing,
    tokens,
    gate_up,
    down,
    blocks,
    line_relay,
    line_sums,
    result,
    back,
    weight_load,
    weight_sent,
    weight_got,
    out_sent,
    out_got,
    line_sent,
    line_got,
    back_sent,
    back_got,
):
    place = Place(chips)
    devices = chips * CORES
    length = narrow_in.shape[0]
    width = keys.shape[1]
    plane = SIDE * SIDE
    barrier, count = greet(place)
    group = pl.multiple_of((place.tp // (HEADS // GROUPS)) * width, width)
    mine = pl.ds(pl.multiple_of(place.tp * width, width), width)
    pairs = (
        (key_hbm.at[:, pl.ds(group, width)], keys),
        (query_hbm.at[:, pl.ds(group, width)], queries),
        (resid_hbm.at[:, mine], resid),
        (narrow_rows_hbm, narrow_rows),
        (wide_rows_hbm, wide_rows),
    )
    gather = Gather(place, gate_up, down, weight_sent, weight_got)
    gather.load(gate_hbm, up_hbm, down_hbm, weight_load)
    loads = [pltpu.make_async_copy(src, dst, load_sem.at[k]) for k, (src, dst) in enumerate(pairs)]
    for load in loads:
        load.start()

    upper = ones_where(iota((length, length), 0) <= iota((length, length), 1))
    causal = iota((length, length), 0) >= iota((length, length), 1)
    lower = ones_where(causal)
    same = iota((length, length), 0) == iota((length, length), 1)
    across = (((1,), (1,)), ((), ()))
    flat = lines[...]
    tall = fine_dot(jnp.where(same, 1.0, 0.0), flat, across)
    narrow_in[...] = quick_dot(ones_where(same), narrow_turned[...], across).astype(jnp.bfloat16)
    narrow_open = silu(quick_dot(ones_where(same), gate_turned[...], across))
    wide_open = silu(wide_gate[...].astype(jnp.float32))
    tall_sum = sum(dot(lower, piece) for piece in in_three(tall))
    flat_sum = sum(dot(piece, upper) for piece in in_three(flat))
    decay, tails, totals, steps = [], [], [], []
    for kind in (0, 1):
        down_column = tall_sum[:, 2 + kind : 3 + kind]
        across = flat_sum[2 + kind : 3 + kind, :]
        decay.append(jnp.exp(jnp.where(causal, down_column - across, -1e30)))
        total = down_column[length - 1 : length, :]
        totals.append(total)
        tails.append(jnp.exp(total - down_column))
        steps.append(tall[:, kind : kind + 1])
    fades = [jnp.exp(tall_sum[:, 2 + kind : 3 + kind]) for kind in (0, 1)]
    rows = iota((width, devices * STATE_ROWS), 0)
    spots = iota((width, devices * STATE_ROWS), 1)
    per = STATE_ROWS // 2
    owner_row = (spots >> 3) * per + (spots & (per - 1))
    wide_spread = jnp.where((owner_row == rows) & ((spots & 7) < per), 1.0, 0.0)
    narrow_spread = jnp.where((owner_row == rows) & ((spots & 7) >= per), 1.0, 0.0)

    loads[0].wait()
    loads[1].wait()
    pl.semaphore_wait(barrier, count)
    gather.open()
    following = ((place.sp + 1) % devices, place.tp)
    rims = []
    tail = pl.ds(length - RIM, RIM)
    for k, (src, dst) in enumerate(
        ((narrow_in, narrow_rim), (wide_in, wide_rim), (keys, key_rim), (queries, query_rim))
    ):
        copy = remote(src.at[tail], dst, rim_sent.at[k], rim_got.at[k], following)
        copy.start()
        rims.append(copy)
    for copy in rims:
        copy.wait_recv()

    inner = place.sp > 0

    def mixed_rows(values, rim, taps):
        size = values.shape[1]
        before = jnp.where(inner, rim[...].astype(jnp.float32), 0.0)
        padded[0:RIM, 0:size] = before
        padded[RIM : RIM + length, 0:size] = values[...].astype(jnp.float32)
        total = jnp.zeros((length, size), jnp.float32)
        for k in range(CONV):
            start = RIM - CONV + 1 + k
            total = total + taps[k : k + 1, :] * padded[start : start + length, 0:size]
        return silu(total)

    key = mixed_rows(keys, key_rim, key_taps[:, pl.ds(group, width)])
    query = mixed_rows(queries, query_rim, query_taps[:, pl.ds(group, width)])
    narrow_mix = mixed_rows(narrow_in, narrow_rim, narrow_taps[...])
    wide_mix = mixed_rows(wide_in, wide_rim, wide_taps[...])
    narrow_size = narrow_mix.shape[1]
    narrow_value, wide_value = narrow_mix * steps[0], wide_mix * steps[1]

    turned = (((0,), (0,)), ((), ()))
    wide_keys = quick_dot(key, wide_spread)
    narrow_keys = quick_dot(key, narrow_spread)
    wide_state = quick_dot(wide_keys, wide_value * tails[1], turned)
    narrow_state = quick_dot(
        narrow_keys,
        jnp.concatenate(
            [narrow_value * tails[0], jnp.zeros((length, width - narrow_size), jnp.float32)], axis=1
        ),
        turned,
    )
    tile = iota((devices * STATE_ROWS, width), 0) & 7
    lane = iota((devices * STATE_ROWS, width), 1)
    spare = jnp.where(lane < (narrow_size + width) // 2, totals[1], totals[0])
    message = wide_state + narrow_state
    message = jnp.where((tile >= per) & (lane >= narrow_size), spare, message)
    told[...] = message.reshape(devices, STATE_ROWS, width).astype(jnp.bfloat16)

    def exchange(src, dst, sent, got):
        copies = []
        dst[place.sp] = src[place.sp]
        for step in range(1, devices):
            other = (place.sp + step) % devices
            copy = remote(
                src.at[other], dst.at[place.sp], sent.at[step], got.at[step], (other, place.tp)
            )
            copy.start()
            copies.append(copy)
        return copies

    tells = exchange(told, heard, told_sent, told_got)

    scores = quick_dot(query, key, (((1,), (1,)), ((), ())))
    narrow_inside = quick_dot(scores * decay[0], narrow_value)
    wide_inside = quick_dot(scores * decay[1], wide_value)
    wide_query = quick_dot(query * fades[1], wide_spread)
    narrow_query = quick_dot(query * fades[0], narrow_spread)

    for copy in tells:
        copy.wait_recv()
    gather.pass_on(0)
    running = jnp.zeros((STATE_ROWS, width), jnp.float32)
    upper_rows = iota((STATE_ROWS, width), 0) < per
    for source in range(devices):
        answer[source] = running.astype(jnp.bfloat16)
        piece = heard[source].astype(jnp.float32)
        wide_total = piece[per : per + 1, narrow_size : narrow_size + 1]
        middle = (narrow_size + width) // 2
        narrow_total = piece[per : per + 1, middle : middle + 1]
        factor = jnp.exp(jnp.where(upper_rows, wide_total, narrow_total))
        running = factor * running + piece
    answers = exchange(answer, carried, answer_sent, answer_got)
    routing_tables(devices, cap, tall, flat, choice, share)

    for load in loads[2:]:
        load.wait()
    for copy in answers:
        copy.wait_recv()
    gather.pass_on(1)
    entering = carried[...].astype(jnp.float32).reshape(devices * STATE_ROWS, width)

    def head(inside, asked, size, kind, mix, opened, gain):
        result = inside + quick_dot(asked, entering)[:, :size]
        result = (result + tall[:, 4 + kind : 5 + kind] * mix) * opened
        mean = jnp.sum(result * result, axis=-1, keepdims=True) * (1.0 / size)
        return (result * lax.rsqrt(mean + NORM_EPS) * gain[...]).astype(jnp.bfloat16)

    narrow = head(narrow_inside, narrow_query, narrow_size, 0, narrow_mix, narrow_open, narrow_gain)
    wide = head(wide_inside, wide_query, width, 1, wide_mix, wide_open, wide_gain)

    totals_of = [
        Summer(
            place, first, partial.at[u], relay.at[u], sums.at[u], half.at[u], last.at[u],
            sum_sent.at[u], sum_got.at[u],
        )
        for u, first in ((0, "x"), (1, "y"))
    ]
    unit = length // 2
    for i in range(SIDE):
        part = pl.ds(i * SIDE * width, SIDE * width)
        product = dot(narrow, narrow_rows[:, part]) + dot(wide, wide_rows[:, part])
        product = product.astype(jnp.bfloat16)
        for j in range(SIDE):
            for u in (0, 1):
                partial[u, i, j] = product[u * unit : (u + 1) * unit, j * width : (j + 1) * width]
    for move in ("open", "pass_on", "turn", "pass_again"):
        for total in totals_of:
            getattr(total, move)()
    mixed = jnp.concatenate([total.close() for total in totals_of], axis=0)
    hidden = resid[...].astype(jnp.float32) + mixed
    gather.pass_on(2)
    state[...] = hidden
    outgoing[...] = dot(choice[...], hidden.astype(jnp.bfloat16)).astype(jnp.bfloat16)
    order = chip_order(chips)
    spot = {d: k for k, d in enumerate(order)}
    row, column_own, core = place.at["b"], place.at["a"], place.core
    home = spot[0]
    inside = column_own == 2 * (home % 2) + core
    outside = column_own != 2 * (home % 2) + core
    waits = []

    def slot_rows(number):
        return pl.ds(pl.multiple_of(number * cap, cap), cap)

    def guarded(apart, act):
        if apart:
            pl.when(outside)(act)
        else:
            act()

    for s, d in enumerate(order):
        for other in (0, 1):
            aim = core if other == 0 else 1 - core
            target = ((place.z + chips - d) % chips) * CORES + aim
            across = place.pick(aim, place.at["x"], place.at["y"])
            along = place.pick(aim, place.at["y"], place.at["x"])
            device = (target, place.flat(aim, 2 * (s % 2) + core, along))
            rows = slot_rows(target)
            to = pl.ds((s // 2) * cap, cap)
            copy = remote(
                outgoing.at[rows],
                tokens.at[along, across, to],
                out_sent.at[s * 2 + other],
                out_got.at[s // 2, across],
                device,
            )
            apart = d == 0 and other == 0
            guarded(apart, copy.start)
            waits.append((apart, copy))
            if apart:

                @pl.when(inside)
                def _(rows=rows, to=to):
                    tokens[row, column_own, to, :] = outgoing[rows, :]

    units = chips // 2
    per = units // chunks
    size = per * cap
    parts = []

    def steps(k):
        rows = pl.ds(k * size, size)
        line = Line(
            place, tokens.at[:, :, rows], blocks.at[k], line_relay.at[k], line_sums.at[k],
            line_sent.at[k], line_got.at[k],
        )
        parts.append(line)

        def arrive():
            for u in range(k * per, (k + 1) * per):
                for side in range(SIDE):
                    column = (column_own + side) % SIDE
                    to = pl.ds(u * cap, cap)
                    copy = remote(
                        outgoing.at[pl.ds(0, cap)],
                        tokens.at[row, column, to],
                        out_sent.at[0],
                        out_got.at[u, column],
                        place.plane("b", 1),
                    )
                    guarded(side == 0 and u == home // 2, copy.wait_recv)
            line.open()

        def compute():
            line.arrived()
            if k == 0:
                gather.close()
            pairs_of = [(i, j) for i in range(SIDE) for j in range(SIDE)]
            pieces = [tokens[i, j, rows, :].astype(jnp.float32) for i, j in pairs_of]
            squared = sum(piece * piece for piece in pieces)
            mean = jnp.sum(squared, axis=-1, keepdims=True) * (1.0 / (plane * width))
            scale = lax.rsqrt(mean + NORM_EPS)
            gains = [
                last_gain[
                    :, pl.ds(pl.multiple_of(place.flat(core, j, i) * width, width), width)
                ]
                for i, j in pairs_of
            ]
            values = jnp.concatenate(
                [(piece * scale * gain).astype(jnp.bfloat16) for piece, gain in zip(pieces, gains)],
                axis=1,
            )
            both = dot(values, gate_up[...])
            hidden_units = both.shape[1] // 2
            gate = jnp.minimum(both[:, :hidden_units], CLAMP_LIMIT)
            up = jnp.clip(both[:, hidden_units:], -CLAMP_LIMIT, CLAMP_LIMIT)
            act = ((up + 1.0) * gate * jax.nn.sigmoid(SIGMOID_SCALE * gate)).astype(jnp.bfloat16)
            for i in range(SIDE):
                wide_part = dot(act, down[:, i * SIDE * width : (i + 1) * SIDE * width])
                for j in range(SIDE):
                    blocks[k, i, j] = wide_part[:, j * width : (j + 1) * width].astype(jnp.bfloat16)
            line.give()

        def close():
            result[k] = line.total().astype(jnp.bfloat16)
            for u in range(k * per, (k + 1) * per):
                d = order[2 * u] + (column_own // 2) * (order[2 * u + 1] - order[2 * u])
                source = ((place.z + d) % chips) * CORES + column_own % 2
                number = (2 * u + column_own // 2) * 2 + (column_own % 2 + core) % 2
                piece = pl.ds((u - k * per) * cap, cap)
                for side in range(SIDE):
                    column = (column_own + side) % SIDE
                    copy = remote(
                        result.at[k, column, piece],
                        back.at[slot_rows(place.sp)],
                        back_sent.at[u, side],
                        back_got.at[number],
                        (source, place.flat(core, column, row)),
                    )
                    apart = side == 0 and u == home // 2
                    guarded(apart, copy.start)
                    waits.append((apart, copy))
                    if apart:

                        @pl.when(inside)
                        def _(piece=piece):
                            back[slot_rows(place.sp), :] = result[k, column_own, piece, :]

        return [arrive, line.pass_on, compute, line.add, close]

    plans = [steps(k) for k in range(chunks)]
    depth = len(plans[0])
    turns = sorted((k + LAG * n, -n, k) for k in range(chunks) for n in range(depth))
    for _, n, k in turns:
        plans[k][-n]()
    for s in range(chips):
        for other in (0, 1):
            copy = remote(
                outgoing.at[pl.ds(0, cap)],
                back.at[pl.ds(0, cap)],
                out_sent.at[0],
                back_got.at[s * 2 + other],
                place.plane("b", 1),
            )
            guarded(s == home and other == 0, copy.wait_recv)
    combined = state[...] + dot(share[0], back[...]) + dot(share[1], back[...])
    out[...] = combined.astype(jnp.bfloat16)
    for apart, copy in waits:
        guarded(apart, copy.wait_send)
    for copy in gather.started.values():
        copy.wait_send()
    for line in parts:
        for copy in line.started:
            copy.wait_send()
    for copy in rims + tells + answers:
        copy.wait_send()
    for total in totals_of:
        for copy in total.started:
            copy.wait_send()


def layer_call(
    inputs, loose, chips, cap
):
    length, width = inputs[1].shape
    narrow_size = inputs[0].shape[0]
    narrow_rows, wide_rows, gate_hbm, down_hbm = loose[3], loose[4], loose[5], loose[7]
    devices = chips * CORES
    unit = length // 2
    chunks = CHUNKS
    slots = devices * cap
    rows = slots // SIDE
    size = rows // chunks
    features, hidden_units = gate_hbm.shape
    bf16, f32 = jnp.bfloat16, jnp.float32
    vmem, any_ = pl.BlockSpec(memory_space=pltpu.VMEM), pl.BlockSpec(memory_space=pl.ANY)
    dma = pltpu.SemaphoreType.DMA
    return pl.pallas_call(
        functools.partial(layer_kernel, chips, cap, chunks),
        out_shape=jax.ShapeDtypeStruct((length, width), bf16),
        in_specs=[vmem] * 12 + [any_] * 8,
        out_specs=vmem,
        scratch_shapes=[
            pltpu.VMEM((length, narrow_size), bf16),
            pltpu.VMEM((length, width), bf16),
            pltpu.VMEM((length, width), bf16),
            pltpu.VMEM((length, width), bf16),
            pltpu.VMEM(narrow_rows.shape, bf16),
            pltpu.VMEM(wide_rows.shape, bf16),
            pltpu.VMEM((RIM, narrow_size), bf16),
            pltpu.VMEM((RIM, width), bf16),
            pltpu.VMEM((RIM, width), bf16),
            pltpu.VMEM((RIM, width), bf16),
            pltpu.VMEM((RIM + length, width), f32),
            pltpu.VMEM((devices, STATE_ROWS, width), bf16),
            pltpu.VMEM((devices, STATE_ROWS, width), bf16),
            pltpu.VMEM((devices, STATE_ROWS, width), bf16),
            pltpu.VMEM((devices, STATE_ROWS, width), bf16),
            pltpu.VMEM((2, SIDE, SIDE, unit, width), bf16),
            pltpu.VMEM((2, 2, SIDE, unit // 2, width), bf16),
            pltpu.VMEM((2, 2, SIDE, unit, width), bf16),
            pltpu.VMEM((2, 2, unit // 2, width), bf16),
            pltpu.VMEM((2, 2, unit, width), bf16),
            dma((5,)),
            dma((4,)),
            dma((4,)),
            dma((devices,)),
            dma((devices,)),
            dma((devices,)),
            dma((devices,)),
            dma((2, 8)),
            dma((2, 8)),
            pltpu.VMEM((length, width), f32),
            pltpu.VMEM((slots, length), bf16),
            pltpu.VMEM((2, length, slots), bf16),
            pltpu.VMEM((slots, width), bf16),
            pltpu.VMEM((SIDE, SIDE, rows, width), bf16),
            pltpu.VMEM((features, 2 * SIDE * hidden_units), bf16),
            pltpu.VMEM((SIDE * hidden_units, features), bf16),
            pltpu.VMEM((chunks, SIDE, SIDE, size, width), bf16),
            pltpu.VMEM((chunks, 2, SIDE, size // 2, width), bf16),
            pltpu.VMEM((chunks, 2, SIDE, size, width), bf16),
            pltpu.VMEM((chunks, SIDE, size, width), bf16),
            pltpu.VMEM((slots, width), bf16),
            dma((3, SIDE * SIDE)),
            dma((3, 4)),
            dma((3, 4)),
            dma((devices,)),
            dma((chips // 2, SIDE)),
            dma((chunks, 8)),
            dma((chunks, 8)),
            dma((chips // 2, SIDE)),
            dma((devices,)),
        ],
        compiler_params=pltpu.CompilerParams(
            collective_id=0, has_side_effects=True, vmem_limit_bytes=56 * 1024 * 1024
        ),
    )(*inputs, *loose)


def local(
    resid,
    narrow_head_input,
    wide_head_input,
    key_group_input,
    query_group_input,
    narrow_output_gate,
    wide_output_gate,
    step_input_rows,
    head_decay_logarithm,
    position_log_decay,
    direct_input_weight,
    narrow_conv_taps,
    wide_conv_taps,
    key_conv_taps,
    query_conv_taps,
    narrow_norm_gain,
    wide_norm_gain,
    narrow_output_rows,
    wide_output_rows,
    feedforward_norm_gain,
    routes,
    routing_weight_values,
    expert_gate_matrix,
    expert_up_matrix,
    expert_down_matrix,
):
    chips = lax.axis_size(SP) // CORES
    steps = jax.nn.softplus(step_input_rows[:, :, 0].T.astype(jnp.float32))
    decays = -jnp.exp(head_decay_logarithm) * steps + position_log_decay[:, :, 0].T
    direct = jnp.broadcast_to(direct_input_weight, steps.shape)
    blank = jnp.zeros((2, steps.shape[1]), jnp.float32)
    lines = jnp.concatenate(
        [
            steps,
            decays,
            direct,
            blank,
            routing_weight_values.T,
            routes.T.astype(jnp.float32),
            blank,
        ],
        axis=0,
    )
    length, picks = routes.shape
    inputs = (
        narrow_head_input.T,
        wide_head_input,
        narrow_output_gate.T,
        wide_output_gate,
        lines,
        narrow_conv_taps,
        wide_conv_taps,
        key_conv_taps,
        query_conv_taps,
        narrow_norm_gain.reshape(1, -1),
        wide_norm_gain.reshape(1, -1),
        feedforward_norm_gain.reshape(1, -1),
    )
    loose = (
        key_group_input,
        query_group_input,
        resid,
        narrow_output_rows,
        wide_output_rows,
        expert_gate_matrix[0],
        expert_up_matrix[0],
        expert_down_matrix[0],
    )
    return layer_call(inputs, loose, chips, 4 * length * picks // (3 * chips * CORES))


def solution(mesh):
    return jax.shard_map(
        local,
        mesh=mesh,
        in_specs=(
            P(SP, None),
            P(SP, "tp"),
            P(SP, "tp"),
            P(SP, None),
            P(SP, None),
            P(SP, "tp"),
            P(SP, "tp"),
            P(SP, None, "tp"),
            P(None, "tp"),
            P(SP, None, "tp"),
            P(None, "tp"),
            P(None, "tp"),
            P(None, "tp"),
            P(),
            P(),
            P("tp"),
            P("tp"),
            P("tp", None),
            P("tp", None),
            P(),
            P(SP, None),
            P(SP, None),
            P(SP, None, "tp"),
            P(SP, None, "tp"),
            P(SP, "tp", None),
        ),
        out_specs=P(SP, "tp"),
        check_vma=False,
    )
```
